32 devices in a mesh: grp: 2 (over y), sp: 4 (over z), tp: 4 (over x, core).
Axes of the slice: x: 2, y: 2, z: 4, core: 2. Of those that a mesh axis runs over, the one named last changes fastest.
Arguments:
- stream: bfloat16 [2048, 2048], P(('grp', 'sp'), 'tp'), parts along dimension 0, may hold values from -1.5 to 1.5
- layer_norm_gain: float32 [2, 2048], replicated, may hold values from 0.1 to 1.9
- convolution_in_weight: bfloat16 [2, 2048, 1536], P(None, 'sp', 'tp'), may hold values from -0.125 to 0.125
- gating_in_weight: bfloat16 [2, 2048, 1536], P(None, 'sp', 'tp'), may hold values from -0.125 to 0.125
- output_weight: bfloat16 [2, 1536, 2048], P(None, 'tp', 'sp'), may hold values from -0.15625 to 0.15625
- convolution_kernel_taps: float32 [2, 4, 1536], P(None, None, 'tp'), may hold values from -12 to 12
- recurrent_gate_blocks: bfloat16 [2, 2, 2, 12, 128, 128], P(None, None, None, 'tp'), may hold values from -0.5 to 0.5
- channel_decay_logit: float32 [2, 2, 1536], P(None, None, 'tp')
- position_decay_boost: float32 [2, 2, 2048], P(None, None, ('grp', 'sp')), parts along dimension 2, may hold values from -1.4 to 0, as said below
Outputs:
- new_stream: bfloat16 [2048, 2048], P(('grp', 'sp'), 'tp'), parts along dimension 0
The draws below stay inside these ranges and needn't reach their ends.
There are 2 independent parts, one for each index of `grp`. The reference program is written for one: setup_inputs(seed, part) draws one part's arguments, and reference() takes and returns one part's arrays. A program takes and returns all parts, laid end to end along the dimension named above; an argument that names none is the same for every part. Nothing has to cross between parts.
Inputs may be any that keep to these rules, and one draw needn't show every extreme that they name: `position_decay_boost`: zero at all but a few positions.
All inputs are finite; a program needn't handle non-finite values.
Results may differ from the reference program's by a relative error of at most 0.025.
Values may be sent and summed in bfloat16 or wider, within the bound.
A program may use at most 128 MiB of HBM per device.

```python
import jax
import jax.numpy as jnp
from jax import lax

D = 2048
LRU = 1536
BW = 128
LAYERS = 2
TOKENS = 1024
N_TP = 4


def draw_channel_decay_logit(key, part):
    key_pick, key_slow, key_fast = jax.random.split(jax.random.fold_in(key, 11), 3)
    shape = (LAYERS, 2, LRU)
    share = 0.5
    slow = jax.random.uniform(key_pick, shape, jnp.float32) < share
    slow_rate = jax.random.uniform(key_slow, shape, jnp.float32, 0.03, 0.1) / TOKENS
    fast_rate = jnp.exp(jax.random.uniform(key_fast, shape, jnp.float32, jnp.log(0.004), jnp.log(0.0125)))
    return -jnp.log(jnp.where(slow, slow_rate, fast_rate))


def draw_position_decay_boost(key, part):
    key_spot, key_loss = jax.random.split(jax.random.fold_in(key, 23), 2)
    spots = jax.random.randint(key_spot, (LAYERS, 2, 2), 0, TOKENS)
    losses = jnp.log(jax.random.uniform(key_loss, (LAYERS, 2, 2), jnp.float32, 0.5, 0.8))
    positions = jnp.arange(TOKENS)
    return jnp.sum(jnp.where(positions[None, None, None, :] == spots[..., None], losses[..., None], 0.0), axis=2)


def draw_convolution_kernel_taps(key, part):
    noise = jax.random.normal(jax.random.fold_in(key, 37), (LAYERS, 4, LRU), jnp.float32)
    spread = jnp.array([3.0, 1.0, 1.0, 1.0], jnp.float32)
    return jnp.clip(noise * spread[None, :, None], -12.0, 12.0)


def block_levels(stream_key, extent, pieces, low, top_value):
    def one(position, blocks):
        steps = jax.random.uniform(jax.random.fold_in(jax.random.fold_in(stream_key, 6), position), (blocks,), jnp.float32, low / len(pieces), top_value / len(pieces))
        return jnp.repeat(jnp.exp(steps), extent[position] // blocks).reshape((-1,) + (1,) * (len(extent) - position - 1))

    loudness = one(*pieces[0])
    for cut in pieces[1:]:
        loudness = loudness * one(*cut)
    return loudness


def centred(own_key, extent, deviation, reach, shards=(), kind=jnp.bfloat16):
    result = deviation * jax.random.normal(own_key, extent, jnp.float32)
    if shards:
        result = result * block_levels(own_key, extent, shards, -0.22, 0.18)
    return jnp.clip(result, -reach, reach).astype(kind)


def setup_inputs(seed: int = 0, part: int = 0) -> dict:
    key_of = jax.random.split(jax.random.key(seed), 10)
    own_keys = jax.random.split(jax.random.fold_in(key_of[9], part), 10)
    stream = centred(own_keys[0], (TOKENS, D), 0.25, 1.5, ((0, 4), (1, 4)))
    layer_norm_gain = jnp.clip(1.0 + 0.18 * jax.random.normal(key_of[1], (LAYERS, D), jnp.float32), 0.1, 1.9)
    convolution_in_weight = centred(key_of[2], (LAYERS, D, LRU), D ** -0.5, 0.125, ((1, 4), (2, 4)))
    gating_in_weight = centred(key_of[3], (LAYERS, D, LRU), D ** -0.5, 0.125, ((1, 4), (2, 4)))
    output_weight = centred(key_of[4], (LAYERS, LRU, D), LRU ** -0.5, 0.15625, ((1, 4), (2, 4)))
    convolution_kernel_taps = draw_convolution_kernel_taps(jax.random.fold_in(key_of[9], 71), part)
    recurrent_gate_blocks = centred(key_of[6], (LAYERS, 2, 2, LRU // BW, BW, BW), BW ** -0.5, 0.5, ((3, 4),))
    channel_decay_logit = draw_channel_decay_logit(jax.random.fold_in(key_of[9], 71), part)
    position_decay_boost = draw_position_decay_boost(jax.random.fold_in(jax.random.fold_in(key_of[9], part), 71), part)
    return {"stream": stream, "layer_norm_gain": layer_norm_gain, "convolution_in_weight": convolution_in_weight, "gating_in_weight": gating_in_weight, "output_weight": output_weight, "convolution_kernel_taps": convolution_kernel_taps, "recurrent_gate_blocks": recurrent_gate_blocks, "channel_decay_logit": channel_decay_logit, "position_decay_boost": position_decay_boost}


EPS = 1e-06
RECURRENT_WIDTH = 8.0

def rms_norm(values, gain_row):
    floats = values.astype(jnp.float32)
    inverse = lax.rsqrt(lax.optimization_barrier(jnp.mean(floats * floats, axis=-1, keepdims=True)) + EPS)
    return (floats * inverse * gain_row.astype(jnp.float32)).astype(jnp.bfloat16)

def combine_pairs(earlier, latter):
    return (earlier[0] * latter[0], latter[0] * earlier[1] + latter[1])

def linear_recurrence(convolution_output, gate_matrix_pair, decay_logit_row, boost_row):
    seq_len = convolution_output.shape[0]
    block_width = gate_matrix_pair.shape[-1]
    conv_float = convolution_output.astype(jnp.float32)
    grouped = conv_float.reshape(seq_len, -1, block_width)
    recurrent_branch = jax.nn.sigmoid(jnp.einsum('tnc,ncd->tnd', grouped, gate_matrix_pair[0].astype(jnp.float32)).reshape(seq_len, -1))
    input_gate = jax.nn.sigmoid(jnp.einsum('tnc,ncd->tnd', grouped, gate_matrix_pair[1].astype(jnp.float32)).reshape(seq_len, -1))
    decay_logarithm = -RECURRENT_WIDTH * jax.nn.softplus(-decay_logit_row) * recurrent_branch + boost_row[:, None]
    is_start = (jnp.arange(seq_len) == 0)[:, None]
    multiplier = jnp.where(is_start, 1.0, jnp.sqrt(-jnp.expm1(2.0 * decay_logarithm)))
    driven = multiplier * input_gate * conv_float
    _, states = lax.associative_scan(combine_pairs, (jnp.exp(decay_logarithm), driven), axis=0)
    return states

def reference(stream, layer_norm_gain, convolution_in_weight, gating_in_weight, output_weight, convolution_kernel_taps, recurrent_gate_blocks, channel_decay_logit, position_decay_boost):
    seq_len = stream.shape[0]
    group_width = convolution_in_weight.shape[2] // N_TP
    for layer_index in range(LAYERS):
        normed = rms_norm(stream, layer_norm_gain[layer_index])
        proj_x = jnp.dot(normed, convolution_in_weight[layer_index], preferred_element_type=jnp.float32).astype(jnp.bfloat16)
        proj_y = jnp.dot(normed, gating_in_weight[layer_index], preferred_element_type=jnp.float32).astype(jnp.bfloat16)
        padded = jnp.pad(proj_x.astype(jnp.float32), ((1, 2), (0, 0)))
        taps_now = convolution_kernel_taps[layer_index]
        conv_mixed = taps_now[0] * padded[0:seq_len] + taps_now[1] * padded[1:seq_len + 1] + taps_now[2] * padded[2:seq_len + 2] + taps_now[3] * padded[3:seq_len + 3]
        convolution_output = conv_mixed.astype(jnp.bfloat16)
        forward_pass = linear_recurrence(convolution_output, recurrent_gate_blocks[layer_index, 0], channel_decay_logit[layer_index, 0], position_decay_boost[layer_index, 0])
        reverse_pass = jnp.flip(linear_recurrence(jnp.flip(convolution_output, 0), recurrent_gate_blocks[layer_index, 1], channel_decay_logit[layer_index, 1], jnp.flip(position_decay_boost[layer_index, 1], 0)), 0)
        gated = ((forward_pass + reverse_pass) * jax.nn.gelu(proj_y.astype(jnp.float32))).astype(jnp.bfloat16)
        branch = jnp.zeros((seq_len, stream.shape[1]), jnp.float32)
        for group in range(N_TP):
            lower = group * group_width
            partial_out = jnp.dot(gated[:, lower:lower + group_width], output_weight[layer_index, lower:lower + group_width, :], preferred_element_type=jnp.float32).astype(jnp.bfloat16)
            branch = branch + partial_out.astype(jnp.float32)
        stream = (stream.astype(jnp.float32) + branch).astype(jnp.bfloat16)
    return stream
```

```python
import functools

import jax
import jax.numpy as jnp
from jax import lax
from jax.experimental import pallas as pl
from jax.experimental.pallas import tpu as pltpu
from jax.sharding import PartitionSpec as P

EPS = 1e-06
RECURRENT_WIDTH = 8.0
TILE = 16
HALO = 8
MESH = pl.DeviceIdType.MESH


def own_share(rows, n_grp):
    if n_grp != 2:
        return rows
    return min(rows, -(-rows * 11 // (20 * TILE)) * TILE)


def one_minus_square(log_decay, decay):
    y = 2.0 * log_decay
    series = y * (1 / 720) + 1 / 120
    series = series * y + 1 / 24
    series = series * y + 1 / 6
    series = series * y + 0.5
    series = series * y + 1.0
    return jnp.where(y > -0.25, -y * series, 1.0 - decay * decay)


def scanned(a, b, reverse):
    count = a.shape[0]
    row = lax.broadcasted_iota(jnp.int32, a.shape, 0)
    step = 1
    while step < count:
        inside = row < count - step if reverse else row >= step
        shift = count - step if reverse else step
        a_near = jnp.where(inside, pltpu.roll(a, shift, 0), 1.0)
        b_near = jnp.where(inside, pltpu.roll(b, shift, 0), 0.0)
        b = a * b_near + b
        a = a * a_near
        step *= 2
    return a, b


def kernel(
    n_grp, n_sp, n_tp,
    stream, gain, conv_w, gate_w, out_w, taps, blocks, rate, boost,
    out,
    full, normed, g_in, g_out, xpad, y_act, cum, loc, ends, gated, parts, sums,
    z_send, z_recv, y_send, y_recv, f_send, f_recv, r_send, r_recv,
    h_send, h_recv, e_send, e_recv,
):
    g, s, t = lax.axis_index("grp"), lax.axis_index("sp"), lax.axis_index("tp")
    layers = conv_w.shape[0]
    rows, ds = stream.shape
    cs, channels = conv_w.shape[1], conv_w.shape[2]
    width = blocks.shape[-1]
    weights = 3 * layers

    def remote(src, dst, send, recv, axis, place):
        return pltpu.make_async_remote_copy(
            src_ref=src, dst_ref=dst, send_sem=send, recv_sem=recv,
            device_id={axis: place}, device_id_type=MESH,
        )

    barrier = pltpu.get_barrier_semaphore()
    total = 0
    for axis, me, count in (("sp", s, n_sp), ("tp", t, n_tp), ("grp", g, n_grp)):
        for d in range(1, count):
            pl.semaphore_signal(
                barrier, inc=1, device_id={axis: lax.rem(me + d, count)}, device_id_type=MESH
            )
            total += 1
    pl.semaphore_wait(barrier, total)

    def mine(w):
        return (conv_w, gate_w, out_w)[w % 3].at[w // 3]

    def hold(w, c):
        return g_out.at[w // 3, c] if w % 3 == 2 else g_in.at[w // 3 * 2 + w % 3, c]

    def depth(w):
        return channels if w % 3 == 2 else cs

    def z_rows(w):
        share = own_share(depth(w), n_grp)
        if share == depth(w):
            return pl.ds(0, share)
        return pl.ds(pl.multiple_of(g * (depth(w) - share), TILE), share)

    def y_rows(w, place):
        share = own_share(depth(w), n_grp)
        return pl.ds(pl.multiple_of(place * share, TILE), depth(w) - share)

    def z_copy(w, c, src, to, slot):
        return remote(
            src.at[z_rows(w)], hold(w, c).at[z_rows(w)],
            z_send.at[w, slot], z_recv.at[w, c], "sp", to,
        )

    shared = n_grp == 2

    def y_copy(w, c, place):
        return remote(
            hold(w, c).at[y_rows(w, place)], hold(w, c).at[y_rows(w, place)],
            y_send.at[w, c], y_recv.at[w, c], "grp", 1 - g,
        )

    def has_y(w):
        return shared and own_share(depth(w), n_grp) < depth(w)

    def start_own(w):
        @pl.when(s < n_sp - 1)
        def _():
            z_copy(w, s, mine(w), s + 1, s).start()

        @pl.when(s > 0)
        def _():
            z_copy(w, s, mine(w), s - 1, n_sp).start()

    def pass_on(w, c, onward, to, back):
        z_copy(w, c, hold(w, c), back, c).wait_recv()

        @pl.when(onward)
        def _():
            z_copy(w, c, hold(w, c), to, c).start()

        if has_y(w):
            y_copy(w, c, g).start()

    def event(w, k):
        @pl.when(s - 1 - k >= 0)
        def _():
            pass_on(w, s - 1 - k, s < n_sp - 1, s + 1, s - 1)

        @pl.when(s + 1 + k <= n_sp - 1)
        def _():
            pass_on(w, s + 1 + k, s > 0, s - 1, s + 1)

        if k == 0 and w + 2 < weights:
            start_own(w + 2)

    queue = [(w, k) for w in range(weights) for k in range(n_sp - 1)]

    def serve(count):
        for _ in range(min(count, len(queue))):
            event(*queue.pop(0))

    def serve_until(w):
        while queue and queue[0][0] <= w:
            event(*queue.pop(0))

    def landed(w):
        if has_y(w):
            for c in range(n_sp):
                @pl.when(c != s)
                def _():
                    y_copy(w, c, 1 - g).wait_recv()

    def f_copy(layer, src, source, d, to):
        return remote(
            src, full.at[layer, source], f_send.at[layer, d], f_recv.at[layer, source], "tp", to
        )

    tp_order = [d for d in range(1, n_tp)]

    def send_features(layer, src):
        for d in tp_order:
            f_copy(layer, src, t, d, lax.rem(t + d, n_tp)).start()

    send_features(0, stream)
    for w in range(min(2, weights)):
        start_own(w)
    full[0, t] = stream[...]
    for w in range(weights):
        if w % 3 == 2:
            g_out[w // 3, s] = out_w[w // 3]
        else:
            g_in[w // 3 * 2 + w % 3, s] = (conv_w, gate_w)[w % 3][w // 3]

    row = lax.broadcasted_iota(jnp.int32, (rows, 1), 0)

    for layer in range(layers):
        if layer == 0:
            serve(1)
        for d in tp_order:
            source = lax.rem(t + d, n_tp)
            f_copy(layer, full.at[layer, source], source, d, source).wait_recv()
        square = jnp.zeros((rows, 1), jnp.float32)
        for j in range(n_tp):
            x = full[layer, j].astype(jnp.float32)
            square += jnp.sum(x * x, axis=-1, keepdims=True)
        inverse = lax.rsqrt(square / (n_tp * ds) + EPS)
        piece = min(cs, ds)
        for p in range(n_tp * ds // piece):
            at = p * piece
            x = full[layer, at // ds, :, at % ds : at % ds + piece].astype(jnp.float32)
            x = x * inverse * gain[layer : layer + 1, at : at + piece]
            normed[at // cs, :, at % cs : at % cs + piece] = x.astype(jnp.bfloat16)

        def project(w):
            acc = None
            for c in range(n_sp):
                term = jnp.dot(
                    normed[c], g_in[w // 3 * 2 + w % 3, c], preferred_element_type=jnp.float32
                )
                acc = term if acc is None else acc + term
            return acc.astype(jnp.bfloat16).astype(jnp.float32)

        wx, wy, wo = 3 * layer, 3 * layer + 1, 3 * layer + 2
        serve_until(wx)
        if layer == 0:
            serve(1)
        landed(wx)
        xpad[layer, HALO : HALO + rows] = project(wx)

        def halo_right():
            return remote(
                xpad.at[layer, pl.ds(rows, HALO)], xpad.at[layer, pl.ds(0, HALO)],
                h_send.at[layer, 0], h_recv.at[layer, 0], "sp", lax.rem(s + 1, n_sp),
            )

        def halo_left():
            return remote(
                xpad.at[layer, pl.ds(HALO, HALO)], xpad.at[layer, pl.ds(HALO + rows, HALO)],
                h_send.at[layer, 1], h_recv.at[layer, 1], "sp", lax.rem(s + n_sp - 1, n_sp),
            )

        @pl.when(s < n_sp - 1)
        def _():
            halo_right().start()

        @pl.when(s > 0)
        def _():
            halo_left().start()

        serve_until(wy)
        landed(wy)
        y_act[...] = jax.nn.gelu(project(wy))

        @pl.when(s > 0)
        def _():
            halo_right().wait_recv()

        @pl.when(s == 0)
        def _():
            xpad[layer, 0:HALO] = jnp.zeros((HALO, channels), jnp.float32)

        @pl.when(s < n_sp - 1)
        def _():
            halo_left().wait_recv()

        @pl.when(s == n_sp - 1)
        def _():
            xpad[layer, HALO + rows : 2 * HALO + rows] = jnp.zeros((HALO, channels), jnp.float32)

        for n in range(channels // width):
            lanes = slice(n * width, (n + 1) * width)
            conv = None
            for k in range(taps.shape[1]):
                term = taps[layer, k : k + 1, lanes] * xpad[
                    layer, HALO - 1 + k : HALO - 1 + k + rows, lanes
                ]
                conv = term if conv is None else conv + term
            conv_half = conv.astype(jnp.bfloat16)
            conv = conv_half.astype(jnp.float32)
            for d in range(2):
                recur = jax.nn.sigmoid(
                    jnp.dot(conv_half, blocks[layer, d, 0, n], preferred_element_type=jnp.float32)
                )
                inject = jax.nn.sigmoid(
                    jnp.dot(conv_half, blocks[layer, d, 1, n], preferred_element_type=jnp.float32)
                )
                at = 2 * layer + d
                log_decay = rate[at : at + 1, lanes] * recur + boost[:, at : at + 1]
                decay = jnp.exp(log_decay)
                first = (row == 0) & (s == 0) if d == 0 else (row == rows - 1) & (s == n_sp - 1)
                m = jnp.where(first, 1.0, jnp.sqrt(one_minus_square(log_decay, decay)))
                a, b = scanned(decay, m * inject * conv, d == 1)
                cum[d, :, lanes] = a
                loc[d, :, lanes] = b
                edge = rows - 1 if d == 0 else 0
                ends[layer, s, 2 * d : 2 * d + 1, lanes] = a[edge : edge + 1]
                ends[layer, s, 2 * d + 1 : 2 * d + 2, lanes] = b[edge : edge + 1]
            serve(1)

        def e_copy(source, d, to):
            return remote(
                ends.at[layer, source], ends.at[layer, source],
                e_send.at[layer, d], e_recv.at[layer, source], "sp", to,
            )

        for d in range(1, n_sp):
            e_copy(s, d, lax.rem(s + d, n_sp)).start()
        serve_until(wo)
        for d in range(1, n_sp):
            source = lax.rem(s + d, n_sp)
            e_copy(source, d, source).wait_recv()
        forward = jnp.zeros((1, channels), jnp.float32)
        backward = forward
        for step in range(n_sp - 1):
            forward = jnp.where(
                step < s, ends[layer, step, 0:1] * forward + ends[layer, step, 1:2], forward
            )
            back = n_sp - 1 - step
            backward = jnp.where(
                back > s, ends[layer, back, 2:3] * backward + ends[layer, back, 3:4], backward
            )
        state = loc[0] + cum[0] * forward + loc[1] + cum[1] * backward
        gated[...] = (state * y_act[...]).astype(jnp.bfloat16)

        def r_copy(source, slot, to):
            return remote(
                parts.at[layer, to], sums.at[layer, source],
                r_send.at[layer, slot], r_recv.at[layer, source], "tp", to,
            )

        landed(wo)
        for c in range(n_sp):
            partial = jnp.dot(gated[...], g_out[layer, c], preferred_element_type=jnp.float32)
            partial = partial.astype(jnp.bfloat16)
            for q in range(cs // piece):
                at = c * cs + q * piece
                j = at // ds
                parts[layer, j, :, at % ds : at % ds + piece] = partial[
                    :, q * piece : (q + 1) * piece
                ]
                if (at + piece) % ds == 0:
                    @pl.when(j != t)
                    def _():
                        r_copy(t, j, j).start()

        if layer == 0:
            serve(n_sp - 1)
        new = full[layer, t].astype(jnp.float32) + parts[layer, t].astype(jnp.float32)
        for d in tp_order:
            source = lax.rem(t + d, n_tp)
            r_copy(source, source, source).wait_recv()
            new = new + sums[layer, source].astype(jnp.float32)
        new = new.astype(jnp.bfloat16)
        if layer + 1 < layers:
            full[layer + 1, t] = new
            send_features(layer + 1, full.at[layer + 1, t])
        else:
            out[...] = new

    for w in range(weights):
        @pl.when(s < n_sp - 1)
        def _():
            z_copy(w, s, mine(w), s + 1, s).wait_send()

        @pl.when(s > 0)
        def _():
            z_copy(w, s, mine(w), s - 1, n_sp).wait_send()

        for c in range(n_sp):
            @pl.when(((c < s) & (s < n_sp - 1)) | ((c > s) & (s > 0)))
            def _():
                z_copy(w, c, hold(w, c), lax.rem(s + 1, n_sp), c).wait_send()

            if has_y(w):
                @pl.when(c != s)
                def _():
                    y_copy(w, c, g).wait_send()

    for layer in range(layers):
        for d in tp_order:
            f_copy(layer, full.at[layer, t], t, d, lax.rem(t + d, n_tp)).wait_send()
        for j in range(n_tp):
            @pl.when(j != t)
            def _():
                remote(
                    parts.at[layer, j], sums.at[layer, t],
                    r_send.at[layer, j], r_recv.at[layer, t], "tp", j,
                ).wait_send()

        for d in range(1, n_sp):
            remote(
                ends.at[layer, s], ends.at[layer, s],
                e_send.at[layer, d], e_recv.at[layer, s], "sp", lax.rem(s + d, n_sp),
            ).wait_send()

        @pl.when(s < n_sp - 1)
        def _():
            remote(
                xpad.at[layer, pl.ds(rows, HALO)], xpad.at[layer, pl.ds(0, HALO)],
                h_send.at[layer, 0], h_recv.at[layer, 0], "sp", lax.rem(s + 1, n_sp),
            ).wait_send()

        @pl.when(s > 0)
        def _():
            remote(
                xpad.at[layer, pl.ds(HALO, HALO)], xpad.at[layer, pl.ds(HALO + rows, HALO)],
                h_send.at[layer, 1], h_recv.at[layer, 1], "sp", lax.rem(s + n_sp - 1, n_sp),
            ).wait_send()


def folded_kernel(
    n_grp, n_sp, n_tp,
    stream, gain, conv_w, gate_w, out_w, taps, blocks, rate, boost,
    out,
    full, normed, g_in, g_out, xpad, p_out, p_in, y_act, cum, loc, ends, gated,
    a_out, a_in, own, b_out, b_in,
    own_send, mid_send, in_send, out_send, y_send, w_recv,
    s_send, s_recv, x_send, x_recv, c_send, c_recv, p_send, p_recv,
    h_send, h_recv, e_send, e_recv, a_send, a_recv, b_send, b_recv,
):
    g, s, t = lax.axis_index("grp"), lax.axis_index("sp"), lax.axis_index("tp")
    layers = conv_w.shape[0]
    rows, ds = stream.shape
    cs, channels = conv_w.shape[1], conv_w.shape[2]
    width = blocks.shape[-1]
    groups = channels // width
    weights = 3 * layers
    last = n_sp - 1
    half = s // 2
    end, mid = last * half, 1 + half
    far_mid, far_end = last - mid, last - end
    is_end = s == end
    is_mid = s == mid
    near = end + mid - s
    chip, core = t // 2, t % 2
    across, partner = lax.rem(t + 2, n_tp), t + 1 - 2 * core
    guest = layers
    slots = (near, far_mid, far_end)

    def remote(src, dst, send, recv, axis, place):
        return pltpu.make_async_remote_copy(
            src_ref=src, dst_ref=dst, send_sem=send, recv_sem=recv,
            device_id={axis: place}, device_id_type=MESH,
        )

    started = []

    def launch(copy, cond=None):
        started.append((copy, cond))
        if cond is None:
            copy.start()
        else:
            @pl.when(cond)
            def _():
                copy.start()

    barrier = pltpu.get_barrier_semaphore()
    total = 0
    for axis, me, count in (("sp", s, n_sp), ("tp", t, n_tp), ("grp", g, n_grp)):
        for d in range(1, count):
            pl.semaphore_signal(
                barrier, inc=1, device_id={axis: lax.rem(me + d, count)}, device_id_type=MESH
            )
            total += 1
    pl.semaphore_wait(barrier, total)

    def mine(w):
        return (conv_w, gate_w, out_w)[w % 3].at[w // 3]

    def place(w, slot, chunk):
        return g_out.at[w // 3, chunk] if w % 3 == 2 else g_in.at[w // 3 * 2 + w % 3, slot]

    def quarter(w, i):
        size = (channels if w % 3 == 2 else cs) // 4
        index = 2 * g + i if i < 2 else 2 * (1 - g) + i - 2
        return pl.ds(pl.multiple_of(index * size, TILE), size)

    def whole(w):
        return w >= 1

    def own_to_near(w, i):
        q = quarter(w, i)
        return remote(
            mine(w).at[q], place(w, 0, s).at[q],
            own_send.at[w, i], w_recv.at[w, 0, i], "sp", near,
        )

    def own_to_mid(w, i):
        q = quarter(w, i)
        return remote(
            mine(w).at[q], place(w, 1, s).at[q],
            mid_send.at[w, i], w_recv.at[w, 1, i], "sp", far_mid,
        )

    def pass_in(w, i):
        q = quarter(w, i)
        return remote(
            place(w, 0, near).at[q], place(w, 2, near).at[q],
            in_send.at[w, i], w_recv.at[w, 2, i], "sp", far_mid,
        )

    def pass_out(w, slot, i):
        here = place(w, slot, slots[slot]).at[quarter(w, i)]
        return remote(
            here, here, out_send.at[w, slot - 1, i], w_recv.at[w, slot, i], "sp", near
        )

    def share(w, slot, i):
        here = place(w, slot, slots[slot]).at[quarter(w, i)]
        return remote(
            here, here, y_send.at[w, slot, i], w_recv.at[w, slot, 2 + i], "grp", 1 - g
        )

    def arrived(w, slot, i):
        here = place(w, slot, slots[slot]).at[quarter(w, i)]
        remote(
            here, here, y_send.at[w, slot, 0], w_recv.at[w, slot, i], "grp", 1 - g
        ).wait_recv()

    outgoing = [(w, i) for w in range(weights) for i in range(4 if whole(w) else 2)]

    def send_outgoing(count):
        for _ in range(min(count, len(outgoing))):
            launch(own_to_near(*outgoing.pop(0)), is_end)

    early = 2 * (weights - 2)

    def tick(n):
        w, i = n // 4, n % 4
        slot, p = 1 + i // 2, i % 2

        if n < early:
            launch(own_to_near(2 + n // 2, n % 2), is_mid)

        if i < 2 and w + 2 < weights:
            launch(own_to_mid(w + 2, i), is_mid)

        @pl.when(is_mid)
        def _():
            arrived(w, slot, p)

        launch(share(w, slot, p), is_mid)
        if w >= 2:
            launch(pass_out(w, slot, p), is_mid)
        if i < 2:
            @pl.when(is_mid)
            def _():
                arrived(w, 0, p)

            launch(pass_in(w, p), is_mid)
            if not whole(w):
                launch(share(w, 0, p), is_mid)

        send_outgoing(1)
        if n < early:
            @pl.when(is_end)
            def _():
                arrived(2 + n // 2, 0, n % 2)

            launch(share(2 + n // 2, 0, n % 2), is_end)
        if w >= 2:
            @pl.when(is_end)
            def _():
                arrived(w, slot, p)

            launch(share(w, slot, p), is_end)

    ticks = list(range(4 * weights))

    def serve_to(n):
        while ticks and ticks[0] < n:
            tick(ticks.pop(0))

    def landed(w):
        serve_to(4 * w + 4)

        def wait_all():
            for slot in range(3):
                for i in (2, 3):
                    arrived(w, slot, i)

        if w < 2:
            pl.when(is_mid)(wait_all)
        else:
            wait_all()

    pieces = 2
    part = rows // pieces

    def strip(p):
        return pl.ds(p * part, part)

    def guest_copy(p):
        return remote(
            stream.at[strip(p)], full.at[guest, t, strip(p)],
            s_send.at[p], s_recv.at[p], "sp", mid,
        )

    def across_copy(k, p, src):
        return remote(
            src.at[strip(p)], full.at[k, t, strip(p)],
            x_send.at[k, p], x_recv.at[k, p], "tp", across,
        )

    def core_copy(k, p, src):
        return remote(
            src.at[strip(p)], full.at[k, t, strip(p)],
            c_send.at[k, p, 0], c_recv.at[k, p, 0], "tp", partner,
        )

    def hand_copy(k, p):
        here = full.at[k, across, strip(p)]
        return remote(here, here, c_send.at[k, p, 1], c_recv.at[k, p, 1], "tp", partner)

    def spread(k, p, src, cond=None):
        launch(across_copy(k, p, src), cond)
        launch(core_copy(k, p, src), cond)

    def hand_on(k, p, cond=None):
        copy = across_copy(k, p, full.at[k, t])
        if cond is None:
            copy.wait_recv()
        else:
            @pl.when(cond)
            def _():
                copy.wait_recv()

        launch(hand_copy(k, p), cond)

    def gathered(k):
        for p in range(pieces):
            core_copy(k, p, full.at[k, t]).wait_recv()
            hand_copy(k, p).wait_recv()

    def normalise(layer, k, slot):
        square = jnp.zeros((rows, 1), jnp.float32)
        for j in range(n_tp):
            x = full[k, j].astype(jnp.float32)
            square += jnp.sum(x * x, axis=-1, keepdims=True)
        inverse = lax.rsqrt(square / (n_tp * ds) + EPS)
        for j in range(n_tp):
            x = full[k, j].astype(jnp.float32)
            x = x * inverse * gain[layer : layer + 1, j * ds : (j + 1) * ds]
            normed[slot, j] = x.astype(jnp.bfloat16)

    def project(w, slot):
        acc = jnp.dot(
            normed[slot, s], mine(w)[...], preferred_element_type=jnp.float32
        )
        for k in range(3):
            acc += jnp.dot(
                normed[slot, slots[k]], g_in[w // 3 * 2 + w % 3, k],
                preferred_element_type=jnp.float32,
            )
        return acc.astype(jnp.bfloat16)

    def p_copy(j, n):
        return remote(
            p_out.at[j, n], p_in.at[j, n], p_send.at[j, n], p_recv.at[j, n], "sp", near
        )

    def halo_right(layer):
        return remote(
            xpad.at[layer, pl.ds(rows, HALO)], xpad.at[layer, pl.ds(0, HALO)],
            h_send.at[layer, 0], h_recv.at[layer, 0], "sp", lax.rem(s + 1, n_sp),
        )

    def halo_left(layer):
        return remote(
            xpad.at[layer, pl.ds(HALO, HALO)], xpad.at[layer, pl.ds(HALO + rows, HALO)],
            h_send.at[layer, 1], h_recv.at[layer, 1], "sp", lax.rem(s + n_sp - 1, n_sp),
        )

    row = lax.broadcasted_iota(jnp.int32, (rows, 1), 0)
    diagonal = lax.broadcasted_iota(jnp.int32, (rows, rows), 0) == lax.broadcasted_iota(
        jnp.int32, (rows, rows), 1
    )

    def recurrences(layer, n):
        lanes = slice(n * width, (n + 1) * width)
        conv = None
        for k in range(taps.shape[1]):
            term = taps[layer, k : k + 1, lanes] * xpad[
                layer, HALO - 1 + k : HALO - 1 + k + rows, lanes
            ]
            conv = term if conv is None else conv + term
        conv_half = conv.astype(jnp.bfloat16)
        conv = conv_half.astype(jnp.float32)
        for d in range(2):
            recur = jax.nn.sigmoid(
                jnp.dot(conv_half, blocks[layer, d, 0, n], preferred_element_type=jnp.float32)
            )
            inject = jax.nn.sigmoid(
                jnp.dot(conv_half, blocks[layer, d, 1, n], preferred_element_type=jnp.float32)
            )
            lift = jnp.sum(
                jnp.where(diagonal, boost[layer, d : d + 1], 0.0), axis=1, keepdims=True
            )
            log_decay = rate[layer, d : d + 1, lanes] * recur + lift
            decay = jnp.exp(log_decay)
            first = (row == 0) & (s == 0) if d == 0 else (row == rows - 1) & (s == last)
            m = jnp.where(first, 1.0, jnp.sqrt(one_minus_square(log_decay, decay)))
            a, b = scanned(decay, m * inject * conv, d == 1)
            cum[d, :, lanes] = a
            loc[d, :, lanes] = b
            edge = rows - 1 if d == 0 else 0
            ends[layer, s, 2 * d : 2 * d + 1, lanes] = a[edge : edge + 1]
            ends[layer, s, 2 * d + 1 : 2 * d + 2, lanes] = b[edge : edge + 1]

    def e_copy(layer, source, d, to):
        return remote(
            ends.at[layer, source], ends.at[layer, source],
            e_send.at[layer, d], e_recv.at[layer, source], "sp", to,
        )

    def send_ends(layer):
        for d in range(1, n_sp):
            launch(e_copy(layer, s, d, lax.rem(s + d, n_sp)))

    def states(layer):
        for d in range(1, n_sp):
            source = lax.rem(s + d, n_sp)
            e_copy(layer, source, d, source).wait_recv()
        forward = jnp.zeros((1, channels), jnp.float32)
        backward = forward
        for step in range(n_sp - 1):
            forward = jnp.where(
                step < s, ends[layer, step, 0:1] * forward + ends[layer, step, 1:2], forward
            )
            back = n_sp - 1 - step
            backward = jnp.where(
                back > s, ends[layer, back, 2:3] * backward + ends[layer, back, 3:4], backward
            )
        state = loc[0] + cum[0] * forward + loc[1] + cum[1] * backward
        gated[...] = (state * y_act[...]).astype(jnp.bfloat16)

    def a_copy(layer, k):
        return remote(
            a_out.at[layer, k], a_in.at[layer, k],
            a_send.at[layer, k], a_recv.at[layer, k], "tp", partner,
        )

    def b_copy(layer, p):
        return remote(
            b_out.at[layer, strip(p)], b_in.at[layer, strip(p)],
            b_send.at[layer, p], b_recv.at[layer, p], "tp", across,
        )

    def branch(layer, j):
        return jnp.dot(gated[...], g_out[layer, j], preferred_element_type=jnp.float32)

    def project_out(layer):
        chips = (1 - chip, chip)
        for k in range(2):
            a_out[layer, k] = branch(layer, 2 * chips[k] + 1 - core).astype(jnp.bfloat16)
            launch(a_copy(layer, k))
        for k in range(2):
            own[k] = branch(layer, 2 * chips[k] + core)
        a_copy(layer, 0).wait_recv()
        for p in range(pieces):
            here = slice(p * part, (p + 1) * part)
            b_out[layer, here] = (
                own[0, here] + a_in[layer, 0, here].astype(jnp.float32)
            ).astype(jnp.bfloat16)
            launch(b_copy(layer, p))
        a_copy(layer, 1).wait_recv()
        own[1] += a_in[layer, 1].astype(jnp.float32)

    def finish(layer, p, old):
        here = slice(p * part, (p + 1) * part)
        b_copy(layer, p).wait_recv()
        new = old[here].astype(jnp.float32) + own[1, here]
        return (new + b_in[layer, here].astype(jnp.float32)).astype(jnp.bfloat16)

    send_outgoing(2)
    for p in range(pieces):
        launch(guest_copy(p), is_end)
        spread(0, p, stream, is_mid)
    send_outgoing(1)
    for w in range(min(2, weights)):
        for i in range(2):
            launch(own_to_mid(w, i), is_mid)
    full[0, t] = stream[...]
    for layer in range(layers):
        g_out[layer, s] = out_w[layer]

    serve_to(2)
    for p in range(pieces):
        hand_on(0, p, is_mid)
    for p in range(pieces):
        serve_to(3 + p)

        @pl.when(is_mid)
        def _():
            guest_copy(p).wait_recv()

        spread(guest, p, full.at[guest, t], is_mid)

    @pl.when(is_mid)
    def _():
        gathered(0)
        normalise(0, 0, 0)

    serve_to(5)
    landed(0)

    @pl.when(is_mid)
    def _():
        xpad[0, HALO : HALO + rows] = project(0, 0).astype(jnp.float32)

    launch(halo_right(0), is_mid)
    launch(halo_left(0), is_mid)
    serve_to(6)
    for p in range(pieces):
        hand_on(guest, p, is_mid)

    @pl.when(is_mid)
    def _():
        gathered(guest)
        normalise(0, guest, 1)
        x = project(0, 1)
        for n in range(groups):
            p_out[0, n] = x[:, n * width : (n + 1) * width]

        @pl.when(half == 0)
        def _():
            xpad[0, 0:HALO] = x[rows - HALO :].astype(jnp.float32)

        @pl.when(half == 1)
        def _():
            xpad[0, HALO + rows : 2 * HALO + rows] = x[:HALO].astype(jnp.float32)

    for n in range(groups):
        launch(p_copy(0, n), is_mid)
    serve_to(8)

    @pl.when(is_end)
    def _():
        for n in range(groups):
            p_copy(0, n).wait_recv()
            xpad[0, HALO : HALO + rows, n * width : (n + 1) * width] = p_in[0, n].astype(
                jnp.float32
            )

    for layer in range(layers):
        wx, wy, wo = 3 * layer, 3 * layer + 1, 3 * layer + 2
        if layer > 0:
            for p in range(pieces):
                hand_on(layer, p)
            gathered(layer)
            normalise(layer, layer, 0)
            landed(wx)
            xpad[layer, HALO : HALO + rows] = project(wx, 0).astype(jnp.float32)
            launch(halo_right(layer), s < last)
            launch(halo_left(layer), s > 0)

        @pl.when((s > 0) if layer > 0 else (s >= 2))
        def _():
            halo_right(layer).wait_recv()

        @pl.when(s == 0)
        def _():
            xpad[layer, 0:HALO] = jnp.zeros((HALO, channels), jnp.float32)

        @pl.when((s < last) if layer > 0 else (s < 2))
        def _():
            halo_left(layer).wait_recv()

        @pl.when(s == last)
        def _():
            xpad[layer, HALO + rows : 2 * HALO + rows] = jnp.zeros((HALO, channels), jnp.float32)

        for n in range(groups):
            recurrences(layer, n)
            serve_to(4 * wy + 2 + n)
        send_ends(layer)
        landed(wy)
        if layer == 0:
            @pl.when(is_mid)
            def _():
                y = project(wy, 1)
                for n in range(groups):
                    p_out[1, n] = y[:, n * width : (n + 1) * width]

            for n in range(groups):
                launch(p_copy(1, n), is_mid)

            @pl.when(is_mid)
            def _():
                y_act[...] = jax.nn.gelu(project(wy, 0).astype(jnp.float32))

            serve_to(4 * wo + 2)

            @pl.when(is_end)
            def _():
                for n in range(groups):
                    p_copy(1, n).wait_recv()
                    y_act[:, n * width : (n + 1) * width] = jax.nn.gelu(
                        p_in[1, n].astype(jnp.float32)
                    )
        else:
            y_act[...] = jax.nn.gelu(project(wy, 0).astype(jnp.float32))
        states(layer)
        landed(wo)
        project_out(layer)
        if layer + 1 < layers:
            serve_to(4 * wo + 6)
            for p in range(pieces):
                full[layer + 1, t, p * part : (p + 1) * part] = finish(
                    layer, p, stream if layer == 0 else full.at[layer, t]
                )
                spread(layer + 1, p, full.at[layer + 1, t])
            serve_to(4 * wo + 8)
        else:
            for p in range(pieces):
                out[p * part : (p + 1) * part] = finish(layer, p, full.at[layer, t])

    for copy, cond in started:
        if cond is None:
            copy.wait_send()
        else:
            @pl.when(cond)
            def _():
                copy.wait_send()


def folds(n_grp, n_sp, n_tp, layers, rows, ds, cs, channels):
    return (
        n_grp == 2 and n_sp == 4 and n_tp == n_sp and cs == ds
        and rows % (2 * TILE) == 0 and cs % (4 * TILE) == 0 and channels % (4 * TILE) == 0
    )


def solution(mesh):
    n_grp, n_sp, n_tp = mesh.shape["grp"], mesh.shape["sp"], mesh.shape["tp"]

    def local(stream, gain, conv_w, gate_w, out_w, taps, blocks, logit, boost):
        layers, cs, channels = conv_w.shape
        rows, ds = stream.shape
        width = blocks.shape[-1]
        bf, f32, dma = jnp.bfloat16, jnp.float32, pltpu.SemaphoreType.DMA
        vmem = pltpu.VMEM
        rate = -RECURRENT_WIDTH * jax.nn.softplus(-logit)
        if folds(n_grp, n_sp, n_tp, layers, rows, ds, cs, channels):
            weights, groups = 3 * layers, channels // width
            return pl.pallas_call(
                functools.partial(folded_kernel, n_grp, n_sp, n_tp),
                out_shape=jax.ShapeDtypeStruct((rows, ds), bf),
                in_specs=[pl.BlockSpec(memory_space=vmem)] * 9,
                out_specs=pl.BlockSpec(memory_space=vmem),
                scratch_shapes=[
                    vmem((layers + 1, n_tp, rows, ds), bf),
                    vmem((2, n_sp, rows, cs), bf),
                    vmem((2 * layers, 3, cs, channels), bf),
                    vmem((layers, n_sp, channels, cs), bf),
                    vmem((layers, rows + 2 * HALO, channels), f32),
                    vmem((2, groups, rows, width), bf),
                    vmem((2, groups, rows, width), bf),
                    vmem((rows, channels), f32),
                    vmem((2, rows, channels), f32),
                    vmem((2, rows, channels), f32),
                    vmem((layers, n_sp, 8, channels), f32),
                    vmem((rows, channels), bf),
                    vmem((layers, 2, rows, ds), bf),
                    vmem((layers, 2, rows, ds), bf),
                    vmem((2, rows, ds), f32),
                    vmem((layers, rows, ds), bf),
                    vmem((layers, rows, ds), bf),
                    dma((weights, 4)),
                    dma((weights, 2)),
                    dma((weights, 2)),
                    dma((weights, 2, 2)),
                    dma((weights, 3, 2)),
                    dma((weights, 3, 4)),
                    dma((2,)),
                    dma((2,)),
                    dma((layers + 1, 2)),
                    dma((layers + 1, 2)),
                    dma((layers + 1, 2, 2)),
                    dma((layers + 1, 2, 2)),
                    dma((2, groups)),
                    dma((2, groups)),
                    dma((layers, 2)),
                    dma((layers, 2)),
                    dma((layers, n_sp)),
                    dma((layers, n_sp)),
                    dma((layers, 2)),
                    dma((layers, 2)),
                    dma((layers, 2)),
                    dma((layers, 2)),
                ],
                compiler_params=pltpu.CompilerParams(
                    collective_id=0, has_side_effects=True, vmem_limit_bytes=60 * 1024 * 1024
                ),
            )(stream, gain, conv_w, gate_w, out_w, taps, blocks, rate, boost)
        rate = rate.reshape(-1, channels)
        boost = boost.reshape(-1, rows).T
        return pl.pallas_call(
            functools.partial(kernel, n_grp, n_sp, n_tp),
            out_shape=jax.ShapeDtypeStruct((rows, ds), bf),
            in_specs=[pl.BlockSpec(memory_space=vmem)] * 9,
            out_specs=pl.BlockSpec(memory_space=vmem),
            scratch_shapes=[
                vmem((layers, n_tp, rows, ds), bf),
                vmem((n_sp, rows, cs), bf),
                vmem((2 * layers, n_sp, cs, channels), bf),
                vmem((layers, n_sp, channels, cs), bf),
                vmem((layers, rows + 2 * HALO, channels), f32),
                vmem((rows, channels), f32),
                vmem((2, rows, channels), f32),
                vmem((2, rows, channels), f32),
                vmem((layers, n_sp, 8, channels), f32),
                vmem((rows, channels), bf),
                vmem((layers, n_tp, rows, ds), bf),
                vmem((layers, n_tp, rows, ds), bf),
                dma((3 * layers, n_sp + 1)),
                dma((3 * layers, n_sp)),
                dma((3 * layers, n_sp)),
                dma((3 * layers, n_sp)),
                dma((layers, n_tp)),
                dma((layers, n_tp)),
                dma((layers, n_tp)),
                dma((layers, n_tp)),
                dma((layers, 2)),
                dma((layers, 2)),
                dma((layers, n_sp)),
                dma((layers, n_sp)),
            ],
            compiler_params=pltpu.CompilerParams(
                collective_id=0, has_side_effects=True, vmem_limit_bytes=60 * 1024 * 1024
            ),
        )(stream, gain, conv_w, gate_w, out_w, taps, blocks, rate, boost)

    return jax.shard_map(
        local,
        mesh=mesh,
        in_specs=(
            P(("grp", "sp"), "tp"),
            P(),
            P(None, "sp", "tp"),
            P(None, "sp", "tp"),
            P(None, "tp", "sp"),
            P(None, None, "tp"),
            P(None, None, None, "tp", None, None),
            P(None, None, "tp"),
            P(None, None, ("grp", "sp")),
        ),
        out_specs=P(("grp", "sp"), "tp"),
        check_vma=False,
    )
```

```python
import functools

import jax
import jax.numpy as jnp
from jax import lax
from jax.experimental import pallas as pl
from jax.experimental.pallas import tpu as pltpu
from jax.sharding import PartitionSpec as P

EPS = 1e-06
RECURRENT_WIDTH = 8.0
TILE = 16
HALO = 8
LAG = 0
END_LAG = 0
PIECES = 4
MESH = pl.DeviceIdType.MESH


def own_share(rows, n_grp):
    if n_grp != 2:
        return rows
    return min(rows, -(-rows * 11 // (20 * TILE)) * TILE)


def one_minus_square(log_decay, decay):
    y = 2.0 * log_decay
    series = y * (1 / 720) + 1 / 120
    series = series * y + 1 / 24
    series = series * y + 1 / 6
    series = series * y + 0.5
    series = series * y + 1.0
    return jnp.where(y > -0.25, -y * series, 1.0 - decay * decay)


def scanned(a, b, reverse):
    count = a.shape[0]
    row = lax.broadcasted_iota(jnp.int32, a.shape, 0)
    step = 1
    while step < count:
        inside = row < count - step if reverse else row >= step
        shift = count - step if reverse else step
        a_near = jnp.where(inside, pltpu.roll(a, shift, 0), 1.0)
        b_near = jnp.where(inside, pltpu.roll(b, shift, 0), 0.0)
        b = a * b_near + b
        a = a * a_near
        step *= 2
    return a, b


def kernel(
    n_grp, n_sp, n_tp,
    stream, gain, conv_w, gate_w, out_w, taps, blocks, rate, boost,
    out,
    full, normed, g_in, g_out, xpad, y_act, cum, loc, ends, gated, parts, sums,
    z_send, z_recv, y_send, y_recv, f_send, f_recv, r_send, r_recv,
    h_send, h_recv, e_send, e_recv,
):
    g, s, t = lax.axis_index("grp"), lax.axis_index("sp"), lax.axis_index("tp")
    layers = conv_w.shape[0]
    rows, ds = stream.shape
    cs, channels = conv_w.shape[1], conv_w.shape[2]
    width = blocks.shape[-1]
    weights = 3 * layers

    def remote(src, dst, send, recv, axis, place):
        return pltpu.make_async_remote_copy(
            src_ref=src, dst_ref=dst, send_sem=send, recv_sem=recv,
            device_id={axis: place}, device_id_type=MESH,
        )

    barrier = pltpu.get_barrier_semaphore()
    total = 0
    for axis, me, count in (("sp", s, n_sp), ("tp", t, n_tp), ("grp", g, n_grp)):
        for d in range(1, count):
            pl.semaphore_signal(
                barrier, inc=1, device_id={axis: lax.rem(me + d, count)}, device_id_type=MESH
            )
            total += 1
    pl.semaphore_wait(barrier, total)

    def mine(w):
        return (conv_w, gate_w, out_w)[w % 3].at[w // 3]

    def hold(w, c):
        return g_out.at[w // 3, c] if w % 3 == 2 else g_in.at[w // 3 * 2 + w % 3, c]

    def depth(w):
        return channels if w % 3 == 2 else cs

    def z_rows(w):
        share = own_share(depth(w), n_grp)
        if share == depth(w):
            return pl.ds(0, share)
        return pl.ds(pl.multiple_of(g * (depth(w) - share), TILE), share)

    def y_rows(w, place):
        share = own_share(depth(w), n_grp)
        return pl.ds(pl.multiple_of(place * share, TILE), depth(w) - share)

    def z_copy(w, c, src, to, slot):
        return remote(
            src.at[z_rows(w)], hold(w, c).at[z_rows(w)],
            z_send.at[w, slot], z_recv.at[w, c], "sp", to,
        )

    shared = n_grp == 2

    def y_copy(w, c, place):
        return remote(
            hold(w, c).at[y_rows(w, place)], hold(w, c).at[y_rows(w, place)],
            y_send.at[w, c], y_recv.at[w, c], "grp", 1 - g,
        )

    def has_y(w):
        return shared and own_share(depth(w), n_grp) < depth(w)

    def start_own(w):
        @pl.when(s < n_sp - 1)
        def _():
            z_copy(w, s, mine(w), s + 1, s).start()

        @pl.when(s > 0)
        def _():
            z_copy(w, s, mine(w), s - 1, n_sp).start()

    def pass_on(w, c, onward, to, back):
        z_copy(w, c, hold(w, c), back, c).wait_recv()

        @pl.when(onward)
        def _():
            z_copy(w, c, hold(w, c), to, c).start()

        if has_y(w):
            y_copy(w, c, g).start()

    def event(w, k):
        @pl.when(s - 1 - k >= 0)
        def _():
            pass_on(w, s - 1 - k, s < n_sp - 1, s + 1, s - 1)

        @pl.when(s + 1 + k <= n_sp - 1)
        def _():
            pass_on(w, s + 1 + k, s > 0, s - 1, s + 1)

        if k == 0 and w + 2 < weights:
            start_own(w + 2)

    queue = [(w, k) for w in range(weights) for k in range(n_sp - 1)]

    def serve(count):
        for _ in range(min(count, len(queue))):
            event(*queue.pop(0))

    def serve_until(w):
        while queue and queue[0][0] <= w:
            event(*queue.pop(0))

    def landed(w):
        if has_y(w):
            for c in range(n_sp):
                @pl.when(c != s)
                def _():
                    y_copy(w, c, 1 - g).wait_recv()

    def f_copy(layer, src, source, d, to):
        return remote(
            src, full.at[layer, source], f_send.at[layer, d], f_recv.at[layer, source], "tp", to
        )

    tp_order = [d for d in range(1, n_tp)]

    def send_features(layer, src):
        for d in tp_order:
            f_copy(layer, src, t, d, lax.rem(t + d, n_tp)).start()

    send_features(0, stream)
    for w in range(min(2, weights)):
        start_own(w)
    full[0, t] = stream[...]
    for w in range(weights):
        if w % 3 == 2:
            g_out[w // 3, s] = out_w[w // 3]
        else:
            g_in[w // 3 * 2 + w % 3, s] = (conv_w, gate_w)[w % 3][w // 3]

    row = lax.broadcasted_iota(jnp.int32, (rows, 1), 0)

    for layer in range(layers):
        if layer == 0:
            serve(1)
        for d in tp_order:
            source = lax.rem(t + d, n_tp)
            f_copy(layer, full.at[layer, source], source, d, source).wait_recv()
        square = jnp.zeros((rows, 1), jnp.float32)
        for j in range(n_tp):
            x = full[layer, j].astype(jnp.float32)
            square += jnp.sum(x * x, axis=-1, keepdims=True)
        inverse = lax.rsqrt(square / (n_tp * ds) + EPS)
        piece = min(cs, ds)
        for p in range(n_tp * ds // piece):
            at = p * piece
            x = full[layer, at // ds, :, at % ds : at % ds + piece].astype(jnp.float32)
            x = x * inverse * gain[layer : layer + 1, at : at + piece]
            normed[at // cs, :, at % cs : at % cs + piece] = x.astype(jnp.bfloat16)

        def project(w):
            acc = None
            for c in range(n_sp):
                term = jnp.dot(
                    normed[c], g_in[w // 3 * 2 + w % 3, c], preferred_element_type=jnp.float32
                )
                acc = term if acc is None else acc + term
            return acc.astype(jnp.bfloat16).astype(jnp.float32)

        wx, wy, wo = 3 * layer, 3 * layer + 1, 3 * layer + 2
        serve_until(wx)
        if layer == 0:
            serve(1)
        landed(wx)
        xpad[layer, HALO : HALO + rows] = project(wx)

        def halo_right():
            return remote(
                xpad.at[layer, pl.ds(rows, HALO)], xpad.at[layer, pl.ds(0, HALO)],
                h_send.at[layer, 0], h_recv.at[layer, 0], "sp", lax.rem(s + 1, n_sp),
            )

        def halo_left():
            return remote(
                xpad.at[layer, pl.ds(HALO, HALO)], xpad.at[layer, pl.ds(HALO + rows, HALO)],
                h_send.at[layer, 1], h_recv.at[layer, 1], "sp", lax.rem(s + n_sp - 1, n_sp),
            )

        @pl.when(s < n_sp - 1)
        def _():
            halo_right().start()

        @pl.when(s > 0)
        def _():
            halo_left().start()

        serve_until(wy)
        landed(wy)
        y_act[...] = jax.nn.gelu(project(wy))

        @pl.when(s > 0)
        def _():
            halo_right().wait_recv()

        @pl.when(s == 0)
        def _():
            xpad[layer, 0:HALO] = jnp.zeros((HALO, channels), jnp.float32)

        @pl.when(s < n_sp - 1)
        def _():
            halo_left().wait_recv()

        @pl.when(s == n_sp - 1)
        def _():
            xpad[layer, HALO + rows : 2 * HALO + rows] = jnp.zeros((HALO, channels), jnp.float32)

        for n in range(channels // width):
            lanes = slice(n * width, (n + 1) * width)
            conv = None
            for k in range(taps.shape[1]):
                term = taps[layer, k : k + 1, lanes] * xpad[
                    layer, HALO - 1 + k : HALO - 1 + k + rows, lanes
                ]
                conv = term if conv is None else conv + term
            conv_half = conv.astype(jnp.bfloat16)
            conv = conv_half.astype(jnp.float32)
            for d in range(2):
                recur = jax.nn.sigmoid(
                    jnp.dot(conv_half, blocks[layer, d, 0, n], preferred_element_type=jnp.float32)
                )
                inject = jax.nn.sigmoid(
                    jnp.dot(conv_half, blocks[layer, d, 1, n], preferred_element_type=jnp.float32)
                )
                at = 2 * layer + d
                log_decay = rate[at : at + 1, lanes] * recur + boost[:, at : at + 1]
                decay = jnp.exp(log_decay)
                first = (row == 0) & (s == 0) if d == 0 else (row == rows - 1) & (s == n_sp - 1)
                m = jnp.where(first, 1.0, jnp.sqrt(one_minus_square(log_decay, decay)))
                a, b = scanned(decay, m * inject * conv, d == 1)
                cum[d, :, lanes] = a
                loc[d, :, lanes] = b
                edge = rows - 1 if d == 0 else 0
                ends[layer, s, 2 * d : 2 * d + 1, lanes] = a[edge : edge + 1]
                ends[layer, s, 2 * d + 1 : 2 * d + 2, lanes] = b[edge : edge + 1]
            serve(1)

        def e_copy(source, d, to):
            return remote(
                ends.at[layer, source], ends.at[layer, source],
                e_send.at[layer, d], e_recv.at[layer, source], "sp", to,
            )

        for d in range(1, n_sp):
            e_copy(s, d, lax.rem(s + d, n_sp)).start()
        serve_until(wo)
        for d in range(1, n_sp):
            source = lax.rem(s + d, n_sp)
            e_copy(source, d, source).wait_recv()
        forward = jnp.zeros((1, channels), jnp.float32)
        backward = forward
        for step in range(n_sp - 1):
            forward = jnp.where(
                step < s, ends[layer, step, 0:1] * forward + ends[layer, step, 1:2], forward
            )
            back = n_sp - 1 - step
            backward = jnp.where(
                back > s, ends[layer, back, 2:3] * backward + ends[layer, back, 3:4], backward
            )
        state = loc[0] + cum[0] * forward + loc[1] + cum[1] * backward
        gated[...] = (state * y_act[...]).astype(jnp.bfloat16)

        def r_copy(source, slot, to):
            return remote(
                parts.at[layer, to], sums.at[layer, source],
                r_send.at[layer, slot], r_recv.at[layer, source], "tp", to,
            )

        landed(wo)
        for c in range(n_sp):
            partial = jnp.dot(gated[...], g_out[layer, c], preferred_element_type=jnp.float32)
            partial = partial.astype(jnp.bfloat16)
            for q in range(cs // piece):
                at = c * cs + q * piece
                j = at // ds
                parts[layer, j, :, at % ds : at % ds + piece] = partial[
                    :, q * piece : (q + 1) * piece
                ]
                if (at + piece) % ds == 0:
                    @pl.when(j != t)
                    def _():
                        r_copy(t, j, j).start()

        if layer == 0:
            serve(n_sp - 1)
        new = full[layer, t].astype(jnp.float32) + parts[layer, t].astype(jnp.float32)
        for d in tp_order:
            source = lax.rem(t + d, n_tp)
            r_copy(source, source, source).wait_recv()
            new = new + sums[layer, source].astype(jnp.float32)
        new = new.astype(jnp.bfloat16)
        if layer + 1 < layers:
            full[layer + 1, t] = new
            send_features(layer + 1, full.at[layer + 1, t])
        else:
            out[...] = new

    for w in range(weights):
        @pl.when(s < n_sp - 1)
        def _():
            z_copy(w, s, mine(w), s + 1, s).wait_send()

        @pl.when(s > 0)
        def _():
            z_copy(w, s, mine(w), s - 1, n_sp).wait_send()

        for c in range(n_sp):
            @pl.when(((c < s) & (s < n_sp - 1)) | ((c > s) & (s > 0)))
            def _():
                z_copy(w, c, hold(w, c), lax.rem(s + 1, n_sp), c).wait_send()

            if has_y(w):
                @pl.when(c != s)
                def _():
                    y_copy(w, c, g).wait_send()

    for layer in range(layers):
        for d in tp_order:
            f_copy(layer, full.at[layer, t], t, d, lax.rem(t + d, n_tp)).wait_send()
        for j in range(n_tp):
            @pl.when(j != t)
            def _():
                remote(
                    parts.at[layer, j], sums.at[layer, t],
                    r_send.at[layer, j], r_recv.at[layer, t], "tp", j,
                ).wait_send()

        for d in range(1, n_sp):
            remote(
                ends.at[layer, s], ends.at[layer, s],
                e_send.at[layer, d], e_recv.at[layer, s], "sp", lax.rem(s + d, n_sp),
            ).wait_send()

        @pl.when(s < n_sp - 1)
        def _():
            remote(
                xpad.at[layer, pl.ds(rows, HALO)], xpad.at[layer, pl.ds(0, HALO)],
                h_send.at[layer, 0], h_recv.at[layer, 0], "sp", lax.rem(s + 1, n_sp),
            ).wait_send()

        @pl.when(s > 0)
        def _():
            remote(
                xpad.at[layer, pl.ds(HALO, HALO)], xpad.at[layer, pl.ds(HALO + rows, HALO)],
                h_send.at[layer, 1], h_recv.at[layer, 1], "sp", lax.rem(s + n_sp - 1, n_sp),
            ).wait_send()


def folded_kernel(
    n_grp, n_sp, n_tp,
    stream, gain, conv_w, gate_w, out_w, taps, blocks, rate, boost,
    out,
    full, normed, g_in, g_out, xpad, p_out, p_in, y_act, cum, loc, ends, gated,
    a_out, a_in, own, b_out, b_in,
    own_send, mid_send, in_send, out_send, y_send, w_recv,
    s_send, s_recv, x_send, x_recv, c_send, c_recv, p_send, p_recv,
    h_send, h_recv, e_send, e_recv, a_send, a_recv, b_send, b_recv,
):
    g, s, t = lax.axis_index("grp"), lax.axis_index("sp"), lax.axis_index("tp")
    layers = conv_w.shape[0]
    rows, ds = stream.shape
    cs, channels = conv_w.shape[1], conv_w.shape[2]
    width = blocks.shape[-1]
    groups = channels // width
    weights = 3 * layers
    last = n_sp - 1
    half = s // 2
    end, mid = last * half, 1 + half
    far_mid, far_end = last - mid, last - end
    is_end = s == end
    is_mid = s == mid
    near = end + mid - s
    chip, core = t // 2, t % 2
    across, partner = lax.rem(t + 2, n_tp), t + 1 - 2 * core
    guest = layers
    slots = (near, far_mid, far_end)

    def remote(src, dst, send, recv, axis, place):
        return pltpu.make_async_remote_copy(
            src_ref=src, dst_ref=dst, send_sem=send, recv_sem=recv,
            device_id={axis: place}, device_id_type=MESH,
        )

    started = []

    def launch(copy, cond=None):
        started.append((copy, cond))
        if cond is None:
            copy.start()
        else:
            @pl.when(cond)
            def _():
                copy.start()

    barrier = pltpu.get_barrier_semaphore()
    total = 0
    for axis, me, count in (("sp", s, n_sp), ("tp", t, n_tp), ("grp", g, n_grp)):
        for d in range(1, count):
            pl.semaphore_signal(
                barrier, inc=1, device_id={axis: lax.rem(me + d, count)}, device_id_type=MESH
            )
            total += 1
    pl.semaphore_wait(barrier, total)

    def mine(w):
        return (conv_w, gate_w, out_w)[w % 3].at[w // 3]

    def place(w, slot, chunk):
        return g_out.at[w // 3, chunk] if w % 3 == 2 else g_in.at[w // 3 * 2 + w % 3, slot]

    def quarter(w, i):
        size = (channels if w % 3 == 2 else cs) // 4
        index = 2 * g + i if i < 2 else 2 * (1 - g) + i - 2
        return pl.ds(pl.multiple_of(index * size, TILE), size)

    def whole(w):
        return w >= 1

    def own_to_near(w, i):
        q = quarter(w, i)
        return remote(
            mine(w).at[q], place(w, 0, s).at[q],
            own_send.at[w, i], w_recv.at[w, 0, i], "sp", near,
        )

    def own_to_mid(w, i):
        q = quarter(w, i)
        return remote(
            mine(w).at[q], place(w, 1, s).at[q],
            mid_send.at[w, i], w_recv.at[w, 1, i], "sp", far_mid,
        )

    def pass_in(w, i):
        q = quarter(w, i)
        return remote(
            place(w, 0, near).at[q], place(w, 2, near).at[q],
            in_send.at[w, i], w_recv.at[w, 2, i], "sp", far_mid,
        )

    def pass_out(w, slot, i):
        here = place(w, slot, slots[slot]).at[quarter(w, i)]
        return remote(
            here, here, out_send.at[w, slot - 1, i], w_recv.at[w, slot, i], "sp", near
        )

    def share(w, slot, i):
        here = place(w, slot, slots[slot]).at[quarter(w, i)]
        return remote(
            here, here, y_send.at[w, slot, i], w_recv.at[w, slot, 2 + i], "grp", 1 - g
        )

    def arrived(w, slot, i):
        here = place(w, slot, slots[slot]).at[quarter(w, i)]
        remote(
            here, here, y_send.at[w, slot, 0], w_recv.at[w, slot, i], "grp", 1 - g
        ).wait_recv()

    outgoing = [(w, i) for w in range(weights) for i in range(4 if whole(w) else 2)]

    def send_outgoing(count):
        for _ in range(min(count, len(outgoing))):
            launch(own_to_near(*outgoing.pop(0)), is_end)

    inward = [(w, i) for w in range(weights) for i in range(2)]

    def send_inward(count):
        for _ in range(min(count, len(inward))):
            launch(own_to_mid(*inward.pop(0)), is_mid)

    early = 2 * (weights - 2)

    def mid_tick(n):
        w, i = n // 4, n % 4
        slot, p = 1 + i // 2, i % 2

        @pl.when(is_mid)
        def _():
            arrived(w, slot, p)

        launch(share(w, slot, p), is_mid)
        if w >= 2:
            launch(pass_out(w, slot, p), is_mid)
        if i < 2:
            @pl.when(is_mid)
            def _():
                arrived(w, 0, p)

            launch(pass_in(w, p), is_mid)
            if not whole(w):
                launch(share(w, 0, p), is_mid)
            if i == 1:
                send_inward(2)

    def end_tick(n):
        w, i = n // 4, n % 4
        slot, p = 1 + i // 2, i % 2
        if n >= 2:
            send_outgoing(1)
        if n < early:
            @pl.when(is_end)
            def _():
                arrived(2 + n // 2, 0, n % 2)

            launch(share(2 + n // 2, 0, n % 2), is_end)
        if w >= 2:
            @pl.when(is_end)
            def _():
                arrived(w, slot, p)

            launch(share(w, slot, p), is_end)

    mid_ticks = list(range(4 * weights))
    end_ticks = list(range(4 * weights))

    def serve(mid=0, end=0):
        while mid_ticks and mid_ticks[0] < mid:
            mid_tick(mid_ticks.pop(0))
        while end_ticks and end_ticks[0] < end:
            end_tick(end_ticks.pop(0))

    def landed(w):
        serve(4 * w + 4 + LAG, 4 * w + 4 + END_LAG if w >= 2 else 0)

        def wait_all():
            for slot in range(3):
                for i in (2, 3):
                    arrived(w, slot, i)

        if w < 2:
            pl.when(is_mid)(wait_all)
        else:
            wait_all()

    pieces = PIECES
    part = rows // pieces

    def strip(p):
        return pl.ds(p * part, part)

    def guest_copy(p):
        return remote(
            stream.at[strip(p)], full.at[guest, t, strip(p)],
            s_send.at[p], s_recv.at[p], "sp", mid,
        )

    def across_copy(k, p, src):
        return remote(
            src.at[strip(p)], full.at[k, t, strip(p)],
            x_send.at[k, p], x_recv.at[k, p], "tp", across,
        )

    def core_copy(k, p, src):
        return remote(
            src.at[strip(p)], full.at[k, t, strip(p)],
            c_send.at[k, p, 0], c_recv.at[k, p, 0], "tp", partner,
        )

    def hand_copy(k, p):
        here = full.at[k, across, strip(p)]
        return remote(here, here, c_send.at[k, p, 1], c_recv.at[k, p, 1], "tp", partner)

    def spread(k, p, src, cond=None):
        launch(across_copy(k, p, src), cond)
        launch(core_copy(k, p, src), cond)

    def hand_on(k, p, cond=None):
        copy = across_copy(k, p, full.at[k, t])
        if cond is None:
            copy.wait_recv()
        else:
            @pl.when(cond)
            def _():
                copy.wait_recv()

        launch(hand_copy(k, p), cond)

    def gathered(k):
        for p in range(pieces):
            core_copy(k, p, full.at[k, t]).wait_recv()
            hand_copy(k, p).wait_recv()

    def normalise(layer, k, slot):
        square = jnp.zeros((rows, 1), jnp.float32)
        for j in range(n_tp):
            x = full[k, j].astype(jnp.float32)
            square += jnp.sum(x * x, axis=-1, keepdims=True)
        inverse = lax.rsqrt(square / (n_tp * ds) + EPS)
        for j in range(n_tp):
            x = full[k, j].astype(jnp.float32)
            x = x * inverse * gain[layer : layer + 1, j * ds : (j + 1) * ds]
            normed[slot, j] = x.astype(jnp.bfloat16)

    def project(w, slot):
        acc = jnp.dot(
            normed[slot, s], mine(w)[...], preferred_element_type=jnp.float32
        )
        for k in range(3):
            acc += jnp.dot(
                normed[slot, slots[k]], g_in[w // 3 * 2 + w % 3, k],
                preferred_element_type=jnp.float32,
            )
        return acc.astype(jnp.bfloat16)

    def p_copy(j, n):
        return remote(
            p_out.at[j, n], p_in.at[j, n], p_send.at[j, n], p_recv.at[j, n], "sp", near
        )

    def halo_right(layer):
        return remote(
            xpad.at[layer, pl.ds(rows, HALO)], xpad.at[layer, pl.ds(0, HALO)],
            h_send.at[layer, 0], h_recv.at[layer, 0], "sp", lax.rem(s + 1, n_sp),
        )

    def halo_left(layer):
        return remote(
            xpad.at[layer, pl.ds(HALO, HALO)], xpad.at[layer, pl.ds(HALO + rows, HALO)],
            h_send.at[layer, 1], h_recv.at[layer, 1], "sp", lax.rem(s + n_sp - 1, n_sp),
        )

    row = lax.broadcasted_iota(jnp.int32, (rows, 1), 0)
    diagonal = lax.broadcasted_iota(jnp.int32, (rows, rows), 0) == lax.broadcasted_iota(
        jnp.int32, (rows, rows), 1
    )

    def recurrences(layer, n):
        lanes = slice(n * width, (n + 1) * width)
        conv = None
        for k in range(taps.shape[1]):
            term = taps[layer, k : k + 1, lanes] * xpad[
                layer, HALO - 1 + k : HALO - 1 + k + rows, lanes
            ]
            conv = term if conv is None else conv + term
        conv_half = conv.astype(jnp.bfloat16)
        conv = conv_half.astype(jnp.float32)
        for d in range(2):
            recur = jax.nn.sigmoid(
                jnp.dot(conv_half, blocks[layer, d, 0, n], preferred_element_type=jnp.float32)
            )
            inject = jax.nn.sigmoid(
                jnp.dot(conv_half, blocks[layer, d, 1, n], preferred_element_type=jnp.float32)
            )
            lift = jnp.sum(
                jnp.where(diagonal, boost[layer, d : d + 1], 0.0), axis=1, keepdims=True
            )
            log_decay = rate[layer, d : d + 1, lanes] * recur + lift
            decay = jnp.exp(log_decay)
            first = (row == 0) & (s == 0) if d == 0 else (row == rows - 1) & (s == last)
            m = jnp.where(first, 1.0, jnp.sqrt(one_minus_square(log_decay, decay)))
            a, b = scanned(decay, m * inject * conv, d == 1)
            cum[d, :, lanes] = a
            loc[d, :, lanes] = b
            edge = rows - 1 if d == 0 else 0
            ends[layer, s, 2 * d : 2 * d + 1, lanes] = a[edge : edge + 1]
            ends[layer, s, 2 * d + 1 : 2 * d + 2, lanes] = b[edge : edge + 1]

    def e_copy(layer, source, d, to):
        return remote(
            ends.at[layer, source], ends.at[layer, source],
            e_send.at[layer, d], e_recv.at[layer, source], "sp", to,
        )

    def send_ends(layer):
        for d in range(1, n_sp):
            launch(e_copy(layer, s, d, lax.rem(s + d, n_sp)))

    def states(layer):
        for d in range(1, n_sp):
            source = lax.rem(s + d, n_sp)
            e_copy(layer, source, d, source).wait_recv()
        forward = jnp.zeros((1, channels), jnp.float32)
        backward = forward
        for step in range(n_sp - 1):
            forward = jnp.where(
                step < s, ends[layer, step, 0:1] * forward + ends[layer, step, 1:2], forward
            )
            back = n_sp - 1 - step
            backward = jnp.where(
                back > s, ends[layer, back, 2:3] * backward + ends[layer, back, 3:4], backward
            )
        state = loc[0] + cum[0] * forward + loc[1] + cum[1] * backward
        gated[...] = (state * y_act[...]).astype(jnp.bfloat16)

    def a_copy(layer, k):
        return remote(
            a_out.at[layer, k], a_in.at[layer, k],
            a_send.at[layer, k], a_recv.at[layer, k], "tp", partner,
        )

    def b_copy(layer, p):
        return remote(
            b_out.at[layer, strip(p)], b_in.at[layer, strip(p)],
            b_send.at[layer, p], b_recv.at[layer, p], "tp", across,
        )

    def branch(layer, j):
        return jnp.dot(gated[...], g_out[layer, j], preferred_element_type=jnp.float32)

    def project_out(layer):
        chips = (1 - chip, chip)
        for k in range(2):
            a_out[layer, k] = branch(layer, 2 * chips[k] + 1 - core).astype(jnp.bfloat16)
            launch(a_copy(layer, k))
        for k in range(2):
            own[k] = branch(layer, 2 * chips[k] + core)
        a_copy(layer, 0).wait_recv()
        for p in range(pieces):
            here = slice(p * part, (p + 1) * part)
            b_out[layer, here] = (
                own[0, here] + a_in[layer, 0, here].astype(jnp.float32)
            ).astype(jnp.bfloat16)
            launch(b_copy(layer, p))
        a_copy(layer, 1).wait_recv()
        own[1] += a_in[layer, 1].astype(jnp.float32)

    def finish(layer, p, old):
        here = slice(p * part, (p + 1) * part)
        b_copy(layer, p).wait_recv()
        new = old[here].astype(jnp.float32) + own[1, here]
        return (new + b_in[layer, here].astype(jnp.float32)).astype(jnp.bfloat16)

    send_outgoing(2)
    for p in range(pieces):
        launch(guest_copy(p), is_end)
        spread(0, p, stream, is_mid)
    send_outgoing(0)
    send_inward(2)
    for n in range(early):
        launch(own_to_near(2 + n // 2, n % 2), is_mid)
    full[0, t] = stream[...]
    for layer in range(layers):
        g_out[layer, s] = out_w[layer]

    serve(2, 4)
    for p in range(pieces):
        hand_on(0, p, is_mid)
    for p in range(pieces):
        serve(2 + (2 * p + 1) // pieces)

        @pl.when(is_mid)
        def _():
            guest_copy(p).wait_recv()

        spread(guest, p, full.at[guest, t], is_mid)
    serve(4)

    @pl.when(is_mid)
    def _():
        gathered(0)
        normalise(0, 0, 0)

    for p in range(pieces):
        hand_on(guest, p, is_mid)
    serve(6)

    @pl.when(is_mid)
    def _():
        gathered(guest)
        normalise(0, guest, 1)

    landed(0)

    @pl.when(is_mid)
    def _():
        x = project(0, 1)
        for n in range(groups):
            p_out[0, n] = x[:, n * width : (n + 1) * width]

        @pl.when(half == 0)
        def _():
            xpad[0, 0:HALO] = x[rows - HALO :].astype(jnp.float32)

        @pl.when(half == 1)
        def _():
            xpad[0, HALO + rows : 2 * HALO + rows] = x[:HALO].astype(jnp.float32)

    for n in range(groups):
        launch(p_copy(0, n), is_mid)

    @pl.when(is_mid)
    def _():
        xpad[0, HALO : HALO + rows] = project(0, 0).astype(jnp.float32)

    launch(halo_right(0), is_mid)
    launch(halo_left(0), is_mid)
    serve(8, 8)
    send_outgoing(4)

    @pl.when(is_end)
    def _():
        for n in range(groups):
            p_copy(0, n).wait_recv()
            xpad[0, HALO : HALO + rows, n * width : (n + 1) * width] = p_in[0, n].astype(
                jnp.float32
            )

    for layer in range(layers):
        wx, wy, wo = 3 * layer, 3 * layer + 1, 3 * layer + 2
        if layer > 0:
            for p in range(pieces):
                hand_on(layer, p)
                serve(4 * wx + 6 + 2 * p // pieces, 4 * wx + 6 + 2 * p // pieces)
            gathered(layer)
            normalise(layer, layer, 0)
            landed(wx)
            xpad[layer, HALO : HALO + rows] = project(wx, 0).astype(jnp.float32)
            launch(halo_right(layer), s < last)
            launch(halo_left(layer), s > 0)
            serve(4 * wx + 11, 4 * wx + 9)

        @pl.when((s > 0) if layer > 0 else (s >= 2))
        def _():
            halo_right(layer).wait_recv()

        @pl.when(s == 0)
        def _():
            xpad[layer, 0:HALO] = jnp.zeros((HALO, channels), jnp.float32)

        @pl.when((s < last) if layer > 0 else (s < 2))
        def _():
            halo_left(layer).wait_recv()

        @pl.when(s == last)
        def _():
            xpad[layer, HALO + rows : 2 * HALO + rows] = jnp.zeros((HALO, channels), jnp.float32)

        for n in range(groups):
            recurrences(layer, n)
            if layer == 0:
                serve(4 * wo + n)
            else:
                serve(4 * wx + 12)
        send_ends(layer)
        if layer == 0:
            send_outgoing(4)
            serve(4 * wo + 4, 4 * wo + 2)
        if layer == layers - 1:
            serve(4 * weights, 24)
        landed(wy)
        if layer == 0:
            @pl.when(is_mid)
            def _():
                y = project(wy, 1)
                for n in range(groups):
                    p_out[1, n] = y[:, n * width : (n + 1) * width]

            for n in range(groups):
                launch(p_copy(1, n), is_mid)

            @pl.when(is_mid)
            def _():
                y_act[...] = jax.nn.gelu(project(wy, 0).astype(jnp.float32))

            serve(4 * wo + 4, 4 * wo + 4)

            @pl.when(is_end)
            def _():
                for n in range(groups):
                    p_copy(1, n).wait_recv()
                    y_act[:, n * width : (n + 1) * width] = jax.nn.gelu(
                        p_in[1, n].astype(jnp.float32)
                    )
        else:
            y_act[...] = jax.nn.gelu(project(wy, 0).astype(jnp.float32))
        states(layer)
        landed(wo)
        project_out(layer)
        if layer + 1 < layers:
            for p in range(pieces):
                serve(4 * wo + 7 + 3 * p // pieces, 4 * wo + 6 + 4 * p // pieces)
                full[layer + 1, t, p * part : (p + 1) * part] = finish(
                    layer, p, stream if layer == 0 else full.at[layer, t]
                )
                spread(layer + 1, p, full.at[layer + 1, t])
        else:
            for p in range(pieces):
                out[p * part : (p + 1) * part] = finish(layer, p, full.at[layer, t])

    for copy, cond in started:
        if cond is None:
            copy.wait_send()
        else:
            @pl.when(cond)
            def _():
                copy.wait_send()


def folds(n_grp, n_sp, n_tp, layers, rows, ds, cs, channels):
    return (
        n_grp == 2 and n_sp == 4 and n_tp == n_sp and cs == ds
        and rows % (PIECES * TILE) == 0 and cs % (4 * TILE) == 0 and channels % (4 * TILE) == 0
    )


def solution(mesh):
    n_grp, n_sp, n_tp = mesh.shape["grp"], mesh.shape["sp"], mesh.shape["tp"]

    def local(stream, gain, conv_w, gate_w, out_w, taps, blocks, logit, boost):
        layers, cs, channels = conv_w.shape
        rows, ds = stream.shape
        width = blocks.shape[-1]
        bf, f32, dma = jnp.bfloat16, jnp.float32, pltpu.SemaphoreType.DMA
        vmem = pltpu.VMEM
        rate = -RECURRENT_WIDTH * jax.nn.softplus(-logit)
        if folds(n_grp, n_sp, n_tp, layers, rows, ds, cs, channels):
            weights, groups = 3 * layers, channels // width
            return pl.pallas_call(
                functools.partial(folded_kernel, n_grp, n_sp, n_tp),
                out_shape=jax.ShapeDtypeStruct((rows, ds), bf),
                in_specs=[pl.BlockSpec(memory_space=vmem)] * 9,
                out_specs=pl.BlockSpec(memory_space=vmem),
                scratch_shapes=[
                    vmem((layers + 1, n_tp, rows, ds), bf),
                    vmem((2, n_sp, rows, cs), bf),
                    vmem((2 * layers, 3, cs, channels), bf),
                    vmem((layers, n_sp, channels, cs), bf),
                    vmem((layers, rows + 2 * HALO, channels), f32),
                    vmem((2, groups, rows, width), bf),
                    vmem((2, groups, rows, width), bf),
                    vmem((rows, channels), f32),
                    vmem((2, rows, channels), f32),
                    vmem((2, rows, channels), f32),
                    vmem((layers, n_sp, 8, channels), f32),
                    vmem((rows, channels), bf),
                    vmem((layers, 2, rows, ds), bf),
                    vmem((layers, 2, rows, ds), bf),
                    vmem((2, rows, ds), f32),
                    vmem((layers, rows, ds), bf),
                    vmem((layers, rows, ds), bf),
                    dma((weights, 4)),
                    dma((weights, 2)),
                    dma((weights, 2)),
                    dma((weights, 2, 2)),
                    dma((weights, 3, 2)),
                    dma((weights, 3, 4)),
                    dma((PIECES,)),
                    dma((PIECES,)),
                    dma((layers + 1, PIECES)),
                    dma((layers + 1, PIECES)),
                    dma((layers + 1, PIECES, 2)),
                    dma((layers + 1, PIECES, 2)),
                    dma((2, groups)),
                    dma((2, groups)),
                    dma((layers, 2)),
                    dma((layers, 2)),
                    dma((layers, n_sp)),
                    dma((layers, n_sp)),
                    dma((layers, 2)),
                    dma((layers, 2)),
                    dma((layers, PIECES)),
                    dma((layers, PIECES)),
                ],
                compiler_params=pltpu.CompilerParams(
                    collective_id=0, has_side_effects=True, vmem_limit_bytes=60 * 1024 * 1024
                ),
            )(stream, gain, conv_w, gate_w, out_w, taps, blocks, rate, boost)
        rate = rate.reshape(-1, channels)
        boost = boost.reshape(-1, rows).T
        return pl.pallas_call(
            functools.partial(kernel, n_grp, n_sp, n_tp),
            out_shape=jax.ShapeDtypeStruct((rows, ds), bf),
            in_specs=[pl.BlockSpec(memory_space=vmem)] * 9,
            out_specs=pl.BlockSpec(memory_space=vmem),
            scratch_shapes=[
                vmem((layers, n_tp, rows, ds), bf),
                vmem((n_sp, rows, cs), bf),
                vmem((2 * layers, n_sp, cs, channels), bf),
                vmem((layers, n_sp, channels, cs), bf),
                vmem((layers, rows + 2 * HALO, channels), f32),
                vmem((rows, channels), f32),
                vmem((2, rows, channels), f32),
                vmem((2, rows, channels), f32),
                vmem((layers, n_sp, 8, channels), f32),
                vmem((rows, channels), bf),
                vmem((layers, n_tp, rows, ds), bf),
                vmem((layers, n_tp, rows, ds), bf),
                dma((3 * layers, n_sp + 1)),
                dma((3 * layers, n_sp)),
                dma((3 * layers, n_sp)),
                dma((3 * layers, n_sp)),
                dma((layers, n_tp)),
                dma((layers, n_tp)),
                dma((layers, n_tp)),
                dma((layers, n_tp)),
                dma((layers, 2)),
                dma((layers, 2)),
                dma((layers, n_sp)),
                dma((layers, n_sp)),
            ],
            compiler_params=pltpu.CompilerParams(
                collective_id=0, has_side_effects=True, vmem_limit_bytes=60 * 1024 * 1024
            ),
        )(stream, gain, conv_w, gate_w, out_w, taps, blocks, rate, boost)

    return jax.shard_map(
        local,
        mesh=mesh,
        in_specs=(
            P(("grp", "sp"), "tp"),
            P(),
            P(None, "sp", "tp"),
            P(None, "sp", "tp"),
            P(None, "tp", "sp"),
            P(None, None, "tp"),
            P(None, None, None, "tp", None, None),
            P(None, None, "tp"),
            P(None, None, ("grp", "sp")),
        ),
        out_specs=P(("grp", "sp"), "tp"),
        check_vma=False,
    )
```

```python
import functools

import jax
import jax.numpy as jnp
from jax import lax
from jax.experimental import pallas as pl
from jax.experimental.pallas import tpu as pltpu
from jax.sharding import PartitionSpec as P

EPS = 1e-06
RECURRENT_WIDTH = 8.0
TILE = 16
HALO = 8
LAG = 0
END_LAG = 0
PIECES = 4
MESH = pl.DeviceIdType.MESH


def own_share(rows, n_grp):
    if n_grp != 2:
        return rows
    return min(rows, -(-rows * 11 // (20 * TILE)) * TILE)


def one_minus_square(log_decay, decay):
    y = 2.0 * log_decay
    series = y * (1 / 720) + 1 / 120
    series = series * y + 1 / 24
    series = series * y + 1 / 6
    series = series * y + 0.5
    series = series * y + 1.0
    return jnp.where(y > -0.25, -y * series, 1.0 - decay * decay)


def scanned(a, b, reverse):
    count = a.shape[0]
    row = lax.broadcasted_iota(jnp.int32, a.shape, 0)
    step = 1
    while step < count:
        inside = row < count - step if reverse else row >= step
        shift = count - step if reverse else step
        a_near = jnp.where(inside, pltpu.roll(a, shift, 0), 1.0)
        b_near = jnp.where(inside, pltpu.roll(b, shift, 0), 0.0)
        b = a * b_near + b
        a = a * a_near
        step *= 2
    return a, b


def kernel(
    n_grp, n_sp, n_tp,
    stream, gain, conv_w, gate_w, out_w, taps, blocks, rate, boost,
    out,
    full, normed, g_in, g_out, xpad, y_act, cum, loc, ends, gated, parts, sums,
    z_send, z_recv, y_send, y_recv, f_send, f_recv, r_send, r_recv,
    h_send, h_recv, e_send, e_recv,
):
    g, s, t = lax.axis_index("grp"), lax.axis_index("sp"), lax.axis_index("tp")
    layers = conv_w.shape[0]
    rows, ds = stream.shape
    cs, channels = conv_w.shape[1], conv_w.shape[2]
    width = blocks.shape[-1]
    weights = 3 * layers

    def remote(src, dst, send, recv, axis, place):
        return pltpu.make_async_remote_copy(
            src_ref=src, dst_ref=dst, send_sem=send, recv_sem=recv,
            device_id={axis: place}, device_id_type=MESH,
        )

    barrier = pltpu.get_barrier_semaphore()
    total = 0
    for axis, me, count in (("sp", s, n_sp), ("tp", t, n_tp), ("grp", g, n_grp)):
        for d in range(1, count):
            pl.semaphore_signal(
                barrier, inc=1, device_id={axis: lax.rem(me + d, count)}, device_id_type=MESH
            )
            total += 1
    pl.semaphore_wait(barrier, total)

    def mine(w):
        return (conv_w, gate_w, out_w)[w % 3].at[w // 3]

    def hold(w, c):
        return g_out.at[w // 3, c] if w % 3 == 2 else g_in.at[w // 3 * 2 + w % 3, c]

    def depth(w):
        return channels if w % 3 == 2 else cs

    def z_rows(w):
        share = own_share(depth(w), n_grp)
        if share == depth(w):
            return pl.ds(0, share)
        return pl.ds(pl.multiple_of(g * (depth(w) - share), TILE), share)

    def y_rows(w, place):
        share = own_share(depth(w), n_grp)
        return pl.ds(pl.multiple_of(place * share, TILE), depth(w) - share)

    def z_copy(w, c, src, to, slot):
        return remote(
            src.at[z_rows(w)], hold(w, c).at[z_rows(w)],
            z_send.at[w, slot], z_recv.at[w, c], "sp", to,
        )

    shared = n_grp == 2

    def y_copy(w, c, place):
        return remote(
            hold(w, c).at[y_rows(w, place)], hold(w, c).at[y_rows(w, place)],
            y_send.at[w, c], y_recv.at[w, c], "grp", 1 - g,
        )

    def has_y(w):
        return shared and own_share(depth(w), n_grp) < depth(w)

    def start_own(w):
        @pl.when(s < n_sp - 1)
        def _():
            z_copy(w, s, mine(w), s + 1, s).start()

        @pl.when(s > 0)
        def _():
            z_copy(w, s, mine(w), s - 1, n_sp).start()

    def pass_on(w, c, onward, to, back):
        z_copy(w, c, hold(w, c), back, c).wait_recv()

        @pl.when(onward)
        def _():
            z_copy(w, c, hold(w, c), to, c).start()

        if has_y(w):
            y_copy(w, c, g).start()

    def event(w, k):
        @pl.when(s - 1 - k >= 0)
        def _():
            pass_on(w, s - 1 - k, s < n_sp - 1, s + 1, s - 1)

        @pl.when(s + 1 + k <= n_sp - 1)
        def _():
            pass_on(w, s + 1 + k, s > 0, s - 1, s + 1)

        if k == 0 and w + 2 < weights:
            start_own(w + 2)

    queue = [(w, k) for w in range(weights) for k in range(n_sp - 1)]

    def serve(count):
        for _ in range(min(count, len(queue))):
            event(*queue.pop(0))

    def serve_until(w):
        while queue and queue[0][0] <= w:
            event(*queue.pop(0))

    def landed(w):
        if has_y(w):
            for c in range(n_sp):
                @pl.when(c != s)
                def _():
                    y_copy(w, c, 1 - g).wait_recv()

    def f_copy(layer, src, source, d, to):
        return remote(
            src, full.at[layer, source], f_send.at[layer, d], f_recv.at[layer, source], "tp", to
        )

    tp_order = [d for d in range(1, n_tp)]

    def send_features(layer, src):
        for d in tp_order:
            f_copy(layer, src, t, d, lax.rem(t + d, n_tp)).start()

    send_features(0, stream)
    for w in range(min(2, weights)):
        start_own(w)
    full[0, t] = stream[...]
    for w in range(weights):
        if w % 3 == 2:
            g_out[w // 3, s] = out_w[w // 3]
        else:
            g_in[w // 3 * 2 + w % 3, s] = (conv_w, gate_w)[w % 3][w // 3]

    row = lax.broadcasted_iota(jnp.int32, (rows, 1), 0)

    for layer in range(layers):
        if layer == 0:
            serve(1)
        for d in tp_order:
            source = lax.rem(t + d, n_tp)
            f_copy(layer, full.at[layer, source], source, d, source).wait_recv()
        square = jnp.zeros((rows, 1), jnp.float32)
        for j in range(n_tp):
            x = full[layer, j].astype(jnp.float32)
            square += jnp.sum(x * x, axis=-1, keepdims=True)
        inverse = lax.rsqrt(square / (n_tp * ds) + EPS)
        piece = min(cs, ds)
        for p in range(n_tp * ds // piece):
            at = p * piece
            x = full[layer, at // ds, :, at % ds : at % ds + piece].astype(jnp.float32)
            x = x * inverse * gain[layer : layer + 1, at : at + piece]
            normed[at // cs, :, at % cs : at % cs + piece] = x.astype(jnp.bfloat16)

        def project(w):
            acc = None
            for c in range(n_sp):
                term = jnp.dot(
                    normed[c], g_in[w // 3 * 2 + w % 3, c], preferred_element_type=jnp.float32
                )
                acc = term if acc is None else acc + term
            return acc.astype(jnp.bfloat16).astype(jnp.float32)

        wx, wy, wo = 3 * layer, 3 * layer + 1, 3 * layer + 2
        serve_until(wx)
        if layer == 0:
            serve(1)
        landed(wx)
        xpad[layer, HALO : HALO + rows] = project(wx)

        def halo_right():
            return remote(
                xpad.at[layer, pl.ds(rows, HALO)], xpad.at[layer, pl.ds(0, HALO)],
                h_send.at[layer, 0], h_recv.at[layer, 0], "sp", lax.rem(s + 1, n_sp),
            )

        def halo_left():
            return remote(
                xpad.at[layer, pl.ds(HALO, HALO)], xpad.at[layer, pl.ds(HALO + rows, HALO)],
                h_send.at[layer, 1], h_recv.at[layer, 1], "sp", lax.rem(s + n_sp - 1, n_sp),
            )

        @pl.when(s < n_sp - 1)
        def _():
            halo_right().start()

        @pl.when(s > 0)
        def _():
            halo_left().start()

        serve_until(wy)
        landed(wy)
        y_act[...] = jax.nn.gelu(project(wy))

        @pl.when(s > 0)
        def _():
            halo_right().wait_recv()

        @pl.when(s == 0)
        def _():
            xpad[layer, 0:HALO] = jnp.zeros((HALO, channels), jnp.float32)

        @pl.when(s < n_sp - 1)
        def _():
            halo_left().wait_recv()

        @pl.when(s == n_sp - 1)
        def _():
            xpad[layer, HALO + rows : 2 * HALO + rows] = jnp.zeros((HALO, channels), jnp.float32)

        for n in range(channels // width):
            lanes = slice(n * width, (n + 1) * width)
            conv = None
            for k in range(taps.shape[1]):
                term = taps[layer, k : k + 1, lanes] * xpad[
                    layer, HALO - 1 + k : HALO - 1 + k + rows, lanes
                ]
                conv = term if conv is None else conv + term
            conv_half = conv.astype(jnp.bfloat16)
            conv = conv_half.astype(jnp.float32)
            for d in range(2):
                recur = jax.nn.sigmoid(
                    jnp.dot(conv_half, blocks[layer, d, 0, n], preferred_element_type=jnp.float32)
                )
                inject = jax.nn.sigmoid(
                    jnp.dot(conv_half, blocks[layer, d, 1, n], preferred_element_type=jnp.float32)
                )
                at = 2 * layer + d
                log_decay = rate[at : at + 1, lanes] * recur + boost[:, at : at + 1]
                decay = jnp.exp(log_decay)
                first = (row == 0) & (s == 0) if d == 0 else (row == rows - 1) & (s == n_sp - 1)
                m = jnp.where(first, 1.0, jnp.sqrt(one_minus_square(log_decay, decay)))
                a, b = scanned(decay, m * inject * conv, d == 1)
                cum[d, :, lanes] = a
                loc[d, :, lanes] = b
                edge = rows - 1 if d == 0 else 0
                ends[layer, s, 2 * d : 2 * d + 1, lanes] = a[edge : edge + 1]
                ends[layer, s, 2 * d + 1 : 2 * d + 2, lanes] = b[edge : edge + 1]
            serve(1)

        def e_copy(source, d, to):
            return remote(
                ends.at[layer, source], ends.at[layer, source],
                e_send.at[layer, d], e_recv.at[layer, source], "sp", to,
            )

        for d in range(1, n_sp):
            e_copy(s, d, lax.rem(s + d, n_sp)).start()
        serve_until(wo)
        for d in range(1, n_sp):
            source = lax.rem(s + d, n_sp)
            e_copy(source, d, source).wait_recv()
        forward = jnp.zeros((1, channels), jnp.float32)
        backward = forward
        for step in range(n_sp - 1):
            forward = jnp.where(
                step < s, ends[layer, step, 0:1] * forward + ends[layer, step, 1:2], forward
            )
            back = n_sp - 1 - step
            backward = jnp.where(
                back > s, ends[layer, back, 2:3] * backward + ends[layer, back, 3:4], backward
            )
        state = loc[0] + cum[0] * forward + loc[1] + cum[1] * backward
        gated[...] = (state * y_act[...]).astype(jnp.bfloat16)

        def r_copy(source, slot, to):
            return remote(
                parts.at[layer, to], sums.at[layer, source],
                r_send.at[layer, slot], r_recv.at[layer, source], "tp", to,
            )

        landed(wo)
        for c in range(n_sp):
            partial = jnp.dot(gated[...], g_out[layer, c], preferred_element_type=jnp.float32)
            partial = partial.astype(jnp.bfloat16)
            for q in range(cs // piece):
                at = c * cs + q * piece
                j = at // ds
                parts[layer, j, :, at % ds : at % ds + piece] = partial[
                    :, q * piece : (q + 1) * piece
                ]
                if (at + piece) % ds == 0:
                    @pl.when(j != t)
                    def _():
                        r_copy(t, j, j).start()

        if layer == 0:
            serve(n_sp - 1)
        new = full[layer, t].astype(jnp.float32) + parts[layer, t].astype(jnp.float32)
        for d in tp_order:
            source = lax.rem(t + d, n_tp)
            r_copy(source, source, source).wait_recv()
            new = new + sums[layer, source].astype(jnp.float32)
        new = new.astype(jnp.bfloat16)
        if layer + 1 < layers:
            full[layer + 1, t] = new
            send_features(layer + 1, full.at[layer + 1, t])
        else:
            out[...] = new

    for w in range(weights):
        @pl.when(s < n_sp - 1)
        def _():
            z_copy(w, s, mine(w), s + 1, s).wait_send()

        @pl.when(s > 0)
        def _():
            z_copy(w, s, mine(w), s - 1, n_sp).wait_send()

        for c in range(n_sp):
            @pl.when(((c < s) & (s < n_sp - 1)) | ((c > s) & (s > 0)))
            def _():
                z_copy(w, c, hold(w, c), lax.rem(s + 1, n_sp), c).wait_send()

            if has_y(w):
                @pl.when(c != s)
                def _():
                    y_copy(w, c, g).wait_send()

    for layer in range(layers):
        for d in tp_order:
            f_copy(layer, full.at[layer, t], t, d, lax.rem(t + d, n_tp)).wait_send()
        for j in range(n_tp):
            @pl.when(j != t)
            def _():
                remote(
                    parts.at[layer, j], sums.at[layer, t],
                    r_send.at[layer, j], r_recv.at[layer, t], "tp", j,
                ).wait_send()

        for d in range(1, n_sp):
            remote(
                ends.at[layer, s], ends.at[layer, s],
                e_send.at[layer, d], e_recv.at[layer, s], "sp", lax.rem(s + d, n_sp),
            ).wait_send()

        @pl.when(s < n_sp - 1)
        def _():
            remote(
                xpad.at[layer, pl.ds(rows, HALO)], xpad.at[layer, pl.ds(0, HALO)],
                h_send.at[layer, 0], h_recv.at[layer, 0], "sp", lax.rem(s + 1, n_sp),
            ).wait_send()

        @pl.when(s > 0)
        def _():
            remote(
                xpad.at[layer, pl.ds(HALO, HALO)], xpad.at[layer, pl.ds(HALO + rows, HALO)],
                h_send.at[layer, 1], h_recv.at[layer, 1], "sp", lax.rem(s + n_sp - 1, n_sp),
            ).wait_send()


def softplus(x):
    u = jnp.exp(-jnp.abs(x))
    w = u / (u + 2.0)
    square = w * w
    series = jnp.full_like(x, 1 / 19)
    for k in range(17, 0, -2):
        series = series * square + 1 / k
    return jnp.maximum(x, 0.0) + 2.0 * w * series


def folded_kernel(
    n_grp, n_sp, n_tp,
    stream_in, gain_in, conv_in, gate_in, out_in, taps_in, blocks_in, logit_in, boost_in,
    out,
    gain, conv_w, gate_w, taps, blocks, logit, boost, rate, load_sem,
    full, normed, g_in, g_out, xpad, p_out, p_in, y_act, cum, loc, ends, gated,
    a_out, a_in, own, b_out, b_in,
    own_send, mid_send, in_send, out_send, y_send, w_recv,
    guest_boost, g_send, g_recv, s_send, s_recv, x_send, x_recv, c_send, c_recv, p_send, p_recv,
    h_send, h_recv, e_send, e_recv, a_send, a_recv, b_send, b_recv,
):
    g, s, t = lax.axis_index("grp"), lax.axis_index("sp"), lax.axis_index("tp")
    layers = conv_w.shape[0]
    rows, ds = stream_in.shape
    cs, channels = conv_w.shape[1], conv_w.shape[2]
    width = blocks.shape[-1]
    groups = channels // width
    weights = 3 * layers
    last = n_sp - 1
    half = s // 2
    end, mid = last * half, 1 + half
    far_mid, far_end = last - mid, last - end
    is_end = s == end
    is_mid = s == mid
    near = end + mid - s
    chip, core = t // 2, t % 2
    across, partner = lax.rem(t + 2, n_tp), t + 1 - 2 * core
    guest = layers
    slots = (near, far_mid, far_end)

    def remote(src, dst, send, recv, axis, place):
        return pltpu.make_async_remote_copy(
            src_ref=src, dst_ref=dst, send_sem=send, recv_sem=recv,
            device_id={axis: place}, device_id_type=MESH,
        )

    stream = full.at[0, t]
    loads = [
        (stream_in, stream), (conv_in, conv_w), (gate_in, gate_w),
        *((out_in.at[layer], g_out.at[layer, s]) for layer in range(layers)),
        (logit_in, logit), (gain_in, gain), (taps_in, taps), (boost_in, boost),
        (blocks_in, blocks),
    ]
    loads = [
        pltpu.make_async_copy(src, dst, load_sem.at[i]) for i, (src, dst) in enumerate(loads)
    ]
    for load in loads:
        load.start()

    started = []

    def launch(copy, cond=None):
        started.append((copy, cond))
        if cond is None:
            copy.start()
        else:
            @pl.when(cond)
            def _():
                copy.start()

    barrier = pltpu.get_barrier_semaphore()
    total = 0
    for axis, me, count in (("sp", s, n_sp), ("tp", t, n_tp), ("grp", g, n_grp)):
        for d in range(1, count):
            pl.semaphore_signal(
                barrier, inc=1, device_id={axis: lax.rem(me + d, count)}, device_id_type=MESH
            )
            total += 1
    pl.semaphore_wait(barrier, total)
    for load in loads:
        load.wait()

    def mine(w):
        if w % 3 == 2:
            return g_out.at[w // 3, s]
        return (conv_w, gate_w)[w % 3].at[w // 3]

    def place(w, slot, chunk):
        return g_out.at[w // 3, chunk] if w % 3 == 2 else g_in.at[w // 3 * 2 + w % 3, slot]

    def quarter(w, i):
        size = (channels if w % 3 == 2 else cs) // 4
        index = 2 * g + i if i < 2 else 2 * (1 - g) + i - 2
        return pl.ds(pl.multiple_of(index * size, TILE), size)

    def whole(w):
        return w >= 1

    def own_to_near(w, i):
        q = quarter(w, i)
        return remote(
            mine(w).at[q], place(w, 0, s).at[q],
            own_send.at[w, i], w_recv.at[w, 0, i], "sp", near,
        )

    def own_to_mid(w, i):
        q = quarter(w, i)
        return remote(
            mine(w).at[q], place(w, 1, s).at[q],
            mid_send.at[w, i], w_recv.at[w, 1, i], "sp", far_mid,
        )

    def pass_in(w, i):
        q = quarter(w, i)
        return remote(
            place(w, 0, near).at[q], place(w, 2, near).at[q],
            in_send.at[w, i], w_recv.at[w, 2, i], "sp", far_mid,
        )

    def pass_out(w, slot, i):
        here = place(w, slot, slots[slot]).at[quarter(w, i)]
        return remote(
            here, here, out_send.at[w, slot - 1, i], w_recv.at[w, slot, i], "sp", near
        )

    def share(w, slot, i):
        here = place(w, slot, slots[slot]).at[quarter(w, i)]
        return remote(
            here, here, y_send.at[w, slot, i], w_recv.at[w, slot, 2 + i], "grp", 1 - g
        )

    def arrived(w, slot, i):
        here = place(w, slot, slots[slot]).at[quarter(w, i)]
        remote(
            here, here, y_send.at[w, slot, 0], w_recv.at[w, slot, i], "grp", 1 - g
        ).wait_recv()

    outgoing = [(w, i) for w in range(weights) for i in range(4 if whole(w) else 2)]

    def send_outgoing(count):
        for _ in range(min(count, len(outgoing))):
            launch(own_to_near(*outgoing.pop(0)), is_end)

    inward = [(w, i) for w in range(weights) for i in range(2)]

    def send_inward(count):
        for _ in range(min(count, len(inward))):
            launch(own_to_mid(*inward.pop(0)), is_mid)

    early = 2 * (weights - 2)

    def mid_tick(n):
        w, i = n // 4, n % 4
        slot, p = 1 + i // 2, i % 2

        @pl.when(is_mid)
        def _():
            arrived(w, slot, p)

        launch(share(w, slot, p), is_mid)
        if w >= 2:
            launch(pass_out(w, slot, p), is_mid)
        if i < 2:
            @pl.when(is_mid)
            def _():
                arrived(w, 0, p)

            launch(pass_in(w, p), is_mid)
            if not whole(w):
                launch(share(w, 0, p), is_mid)
            if i == 1:
                send_inward(2)

    def end_tick(n):
        w, i = n // 4, n % 4
        slot, p = 1 + i // 2, i % 2
        if n >= 2:
            send_outgoing(1)
        if n < early:
            @pl.when(is_end)
            def _():
                arrived(2 + n // 2, 0, n % 2)

            launch(share(2 + n // 2, 0, n % 2), is_end)
        if w >= 2:
            @pl.when(is_end)
            def _():
                arrived(w, slot, p)

            launch(share(w, slot, p), is_end)

    mid_ticks = list(range(4 * weights))
    end_ticks = list(range(4 * weights))

    def serve(mid=0, end=0):
        while mid_ticks and mid_ticks[0] < mid:
            mid_tick(mid_ticks.pop(0))
        while end_ticks and end_ticks[0] < end:
            end_tick(end_ticks.pop(0))

    def landed(w):
        serve(4 * w + 4 + LAG, 4 * w + 4 + END_LAG if w >= 2 else 0)

        def wait_all():
            for slot in range(3):
                for i in (2, 3):
                    arrived(w, slot, i)

        if w < 2:
            pl.when(is_mid)(wait_all)
        else:
            wait_all()

    pieces = PIECES
    part = rows // pieces

    def strip(p):
        return pl.ds(p * part, part)

    def guest_copy(p):
        return remote(
            stream.at[strip(p)], full.at[guest, t, strip(p)],
            s_send.at[p], s_recv.at[p], "sp", mid,
        )

    def across_copy(k, p, src):
        return remote(
            src.at[strip(p)], full.at[k, t, strip(p)],
            x_send.at[k, p], x_recv.at[k, p], "tp", across,
        )

    def core_copy(k, p, src):
        return remote(
            src.at[strip(p)], full.at[k, t, strip(p)],
            c_send.at[k, p, 0], c_recv.at[k, p, 0], "tp", partner,
        )

    def hand_copy(k, p):
        here = full.at[k, across, strip(p)]
        return remote(here, here, c_send.at[k, p, 1], c_recv.at[k, p, 1], "tp", partner)

    def spread(k, p, src, cond=None):
        launch(across_copy(k, p, src), cond)
        launch(core_copy(k, p, src), cond)

    def hand_on(k, p, cond=None):
        copy = across_copy(k, p, full.at[k, t])
        if cond is None:
            copy.wait_recv()
        else:
            @pl.when(cond)
            def _():
                copy.wait_recv()

        launch(hand_copy(k, p), cond)

    def gathered(k):
        for p in range(pieces):
            core_copy(k, p, full.at[k, t]).wait_recv()
            hand_copy(k, p).wait_recv()

    def normalise(layer, k, slot):
        square = jnp.zeros((rows, 1), jnp.float32)
        for j in range(n_tp):
            x = full[k, j].astype(jnp.float32)
            square += jnp.sum(x * x, axis=-1, keepdims=True)
        inverse = lax.rsqrt(square / (n_tp * ds) + EPS)
        for j in range(n_tp):
            x = full[k, j].astype(jnp.float32)
            x = x * inverse * gain[layer : layer + 1, j * ds : (j + 1) * ds]
            normed[slot, j] = x.astype(jnp.bfloat16)

    def project(w, slot):
        acc = jnp.dot(
            normed[slot, s], mine(w)[...], preferred_element_type=jnp.float32
        )
        for k in range(3):
            acc += jnp.dot(
                normed[slot, slots[k]], g_in[w // 3 * 2 + w % 3, k],
                preferred_element_type=jnp.float32,
            )
        return acc.astype(jnp.bfloat16)

    def p_copy(n):
        return remote(p_out.at[n], p_in.at[n], p_send.at[n], p_recv.at[n], "sp", near)

    def boost_copy():
        return remote(
            boost.at[0], guest_boost, g_send.at[0], g_recv.at[0], "sp", mid
        )

    def halo_right(layer):
        return remote(
            xpad.at[layer, pl.ds(rows, HALO)], xpad.at[layer, pl.ds(0, HALO)],
            h_send.at[layer, 0], h_recv.at[layer, 0], "sp", lax.rem(s + 1, n_sp),
        )

    def halo_left(layer):
        return remote(
            xpad.at[layer, pl.ds(HALO, HALO)], xpad.at[layer, pl.ds(HALO + rows, HALO)],
            h_send.at[layer, 1], h_recv.at[layer, 1], "sp", lax.rem(s + n_sp - 1, n_sp),
        )

    row = lax.broadcasted_iota(jnp.int32, (rows, 1), 0)
    diagonal = lax.broadcasted_iota(jnp.int32, (rows, rows), 0) == lax.broadcasted_iota(
        jnp.int32, (rows, rows), 1
    )

    def recurrences(layer, n, k=0):
        pad = guest if k else layer
        block = end if k else s
        raised = guest_boost if k else boost.at[layer]
        lanes = slice(n * width, (n + 1) * width)
        conv = None
        for tap in range(taps.shape[1]):
            term = taps[layer, tap : tap + 1, lanes] * xpad[
                pad, HALO - 1 + tap : HALO - 1 + tap + rows, lanes
            ]
            conv = term if conv is None else conv + term
        conv_half = conv.astype(jnp.bfloat16)
        conv = conv_half.astype(jnp.float32)
        for d in range(2):
            recur = jax.nn.sigmoid(
                jnp.dot(conv_half, blocks[layer, d, 0, n], preferred_element_type=jnp.float32)
            )
            inject = jax.nn.sigmoid(
                jnp.dot(conv_half, blocks[layer, d, 1, n], preferred_element_type=jnp.float32)
            )
            lift = jnp.sum(
                jnp.where(diagonal, raised[d : d + 1], 0.0), axis=1, keepdims=True
            )
            log_decay = rate[layer, d : d + 1, lanes] * recur + lift
            decay = jnp.exp(log_decay)
            first = (row == 0) & (block == 0) if d == 0 else (row == rows - 1) & (block == last)
            m = jnp.where(first, 1.0, jnp.sqrt(one_minus_square(log_decay, decay)))
            a, b = scanned(decay, m * inject * conv, d == 1)
            cum[k, d, :, lanes] = a
            loc[k, d, :, lanes] = b
            edge = rows - 1 if d == 0 else 0
            ends[layer, block, 2 * d : 2 * d + 1, lanes] = a[edge : edge + 1]
            ends[layer, block, 2 * d + 1 : 2 * d + 2, lanes] = b[edge : edge + 1]

    def e_copy(layer, source, d, to):
        return remote(
            ends.at[layer, source], ends.at[layer, source],
            e_send.at[layer, d], e_recv.at[layer, source], "sp", to,
        )

    def send_ends(layer):
        for d in range(1, n_sp):
            launch(e_copy(layer, s, d, lax.rem(s + d, n_sp)))

    def ends_pair(to_half):
        here = ends.at[0, pl.ds(2 * to_half, 2)]
        return remote(here, here, e_send.at[0, 0], e_recv.at[0, 0], "sp", far_mid)

    def gather_ends(layer):
        for d in range(1, n_sp):
            source = lax.rem(s + d, n_sp)
            e_copy(layer, source, d, source).wait_recv()

    def states(layer, k=0):
        block = end if k else s
        forward = jnp.zeros((1, channels), jnp.float32)
        backward = forward
        for step in range(n_sp - 1):
            forward = jnp.where(
                step < block, ends[layer, step, 0:1] * forward + ends[layer, step, 1:2], forward
            )
            back = n_sp - 1 - step
            backward = jnp.where(
                back > block, ends[layer, back, 2:3] * backward + ends[layer, back, 3:4], backward
            )
        state = loc[k, 0] + cum[k, 0] * forward + loc[k, 1] + cum[k, 1] * backward
        return (state * y_act[k]).astype(jnp.bfloat16)

    def a_copy(layer, k):
        return remote(
            a_out.at[layer, k], a_in.at[layer, k],
            a_send.at[layer, k], a_recv.at[layer, k], "tp", partner,
        )

    def b_copy(layer, p):
        return remote(
            b_out.at[layer, strip(p)], b_in.at[layer, strip(p)],
            b_send.at[layer, p], b_recv.at[layer, p], "tp", across,
        )

    def branch(layer, j):
        return jnp.dot(gated[...], g_out[layer, j], preferred_element_type=jnp.float32)

    def project_out(layer):
        chips = (1 - chip, chip)
        for k in range(2):
            a_out[layer, k] = branch(layer, 2 * chips[k] + 1 - core).astype(jnp.bfloat16)
            launch(a_copy(layer, k))
        for k in range(2):
            own[k] = branch(layer, 2 * chips[k] + core)
        if layer == 0:
            serve(14, 13)
        a_copy(layer, 0).wait_recv()
        for p in range(pieces):
            here = slice(p * part, (p + 1) * part)
            b_out[layer, here] = (
                own[0, here] + a_in[layer, 0, here].astype(jnp.float32)
            ).astype(jnp.bfloat16)
            launch(b_copy(layer, p))
        a_copy(layer, 1).wait_recv()
        own[1] += a_in[layer, 1].astype(jnp.float32)

    def finish(layer, p, old):
        here = slice(p * part, (p + 1) * part)
        b_copy(layer, p).wait_recv()
        new = old[here].astype(jnp.float32) + own[1, here]
        return (new + b_in[layer, here].astype(jnp.float32)).astype(jnp.bfloat16)

    launch(boost_copy(), is_end)
    send_outgoing(2)
    for p in range(pieces):
        launch(guest_copy(p), is_end)
        spread(0, p, stream, is_mid)
    send_outgoing(0)
    send_inward(2)
    for n in range(early):
        launch(own_to_near(2 + n // 2, n % 2), is_mid)
    for layer in range(layers):
        rate[layer] = -RECURRENT_WIDTH * softplus(-logit[layer])

    serve(2, 4)
    for p in range(pieces):
        hand_on(0, p, is_mid)
    for p in range(pieces):
        serve(2 + (2 * p + 1) // pieces)

        @pl.when(is_mid)
        def _():
            guest_copy(p).wait_recv()

        spread(guest, p, full.at[guest, t], is_mid)
    serve(4)

    @pl.when(is_mid)
    def _():
        gathered(0)
        normalise(0, 0, 0)

    for p in range(pieces):
        hand_on(guest, p, is_mid)
    serve(6)

    @pl.when(is_mid)
    def _():
        gathered(guest)
        normalise(0, guest, 1)

    landed(0)

    @pl.when(is_mid)
    def _():
        x = project(0, 0).astype(jnp.float32)
        xpad[0, HALO : HALO + rows] = x
        edge = jnp.zeros((HALO, channels), jnp.float32)

        @pl.when(half == 0)
        def _():
            xpad[guest, 0:HALO] = edge
            xpad[guest, HALO + rows : 2 * HALO + rows] = x[:HALO]

        @pl.when(half == 1)
        def _():
            xpad[guest, 0:HALO] = x[rows - HALO :]
            xpad[guest, HALO + rows : 2 * HALO + rows] = edge

    launch(halo_right(0), s == 1)
    launch(halo_left(0), s == 2)

    @pl.when(is_mid)
    def _():
        x = project(0, 1).astype(jnp.float32)
        xpad[guest, HALO : HALO + rows] = x

        @pl.when(half == 0)
        def _():
            xpad[0, 0:HALO] = x[rows - HALO :]

        @pl.when(half == 1)
        def _():
            xpad[0, HALO + rows : 2 * HALO + rows] = x[:HALO]

        boost_copy().wait_recv()

    serve(8, 8)
    send_outgoing(4)
    for n in range(groups):
        pl.when(is_mid)(functools.partial(recurrences, 0, n, 1))
        serve(8 + (n + 2) // 3)

    @pl.when(s == 2)
    def _():
        halo_right(0).wait_recv()

    @pl.when(s == 1)
    def _():
        halo_left(0).wait_recv()

    for n in range(groups):
        serve((9, 10, 11)[n])
        pl.when(is_mid)(functools.partial(recurrences, 0, n))
    launch(ends_pair(half), is_mid)
    landed(1)

    @pl.when(is_mid)
    def _():
        y_act[1] = jax.nn.gelu(project(1, 1).astype(jnp.float32))

    serve(12, 8)

    @pl.when(is_mid)
    def _():
        y_act[0] = jax.nn.gelu(project(1, 0).astype(jnp.float32))
        ends_pair(1 - half).wait_recv()
        x = states(0, 1)
        for n in range(groups):
            p_out[n] = x[:, n * width : (n + 1) * width]

    for n in range(groups):
        launch(p_copy(n), is_mid)

    @pl.when(is_mid)
    def _():
        gated[...] = states(0)

    serve(12, 12)

    send_outgoing(len(outgoing))

    @pl.when(is_end)
    def _():
        for n in range(groups):
            p_copy(n).wait_recv()
            gated[:, n * width : (n + 1) * width] = p_in[n]

    for layer in range(layers):
        wx, wy, wo = 3 * layer, 3 * layer + 1, 3 * layer + 2
        final = layer + 1 == layers
        if layer > 0:
            for p in range(pieces):
                hand_on(layer, p)
                if layer == 1:
                    serve((20, 20, 21, 22)[4 * p // pieces], (17, 18, 19, 20)[4 * p // pieces])
            gathered(layer)
            normalise(layer, layer, 0)
            landed(wx)
            xpad[layer, HALO : HALO + rows] = project(wx, 0).astype(jnp.float32)
            launch(halo_right(layer), s < last)
            launch(halo_left(layer), s > 0)
            if final:
                serve((24, 22)[0], (24, 22)[1])

            @pl.when(s > 0)
            def _():
                halo_right(layer).wait_recv()

            @pl.when(s == 0)
            def _():
                xpad[layer, 0:HALO] = jnp.zeros((HALO, channels), jnp.float32)

            @pl.when(s < last)
            def _():
                halo_left(layer).wait_recv()

            @pl.when(s == last)
            def _():
                xpad[layer, HALO + rows : 2 * HALO + rows] = jnp.zeros(
                    (HALO, channels), jnp.float32
                )

            for n in range(groups):
                recurrences(layer, n)
            send_ends(layer)
            if final:
                serve(4 * weights, 24)
            landed(wy)
            y_act[0] = jax.nn.gelu(project(wy, 0).astype(jnp.float32))
            gather_ends(layer)
            gated[...] = states(layer)
        landed(wo)
        project_out(layer)
        for p in range(pieces):
            if layer == 0:
                serve((16, 17, 18, 19)[4 * p // pieces], (14, 15, 16, 17)[4 * p // pieces])
            new = finish(layer, p, full.at[layer, t])
            if final:
                out[p * part : (p + 1) * part] = new
            else:
                full[layer + 1, t, p * part : (p + 1) * part] = new
                spread(layer + 1, p, full.at[layer + 1, t])

    for copy, cond in started:
        if cond is None:
            copy.wait_send()
        else:
            @pl.when(cond)
            def _():
                copy.wait_send()


def folds(n_grp, n_sp, n_tp, layers, rows, ds, cs, channels):
    return (
        n_grp == 2 and n_sp == 4 and n_tp == n_sp and cs == ds
        and rows % (PIECES * TILE) == 0 and cs % (4 * TILE) == 0 and channels % (4 * TILE) == 0
    )


def solution(mesh):
    n_grp, n_sp, n_tp = mesh.shape["grp"], mesh.shape["sp"], mesh.shape["tp"]

    def local(stream, gain, conv_w, gate_w, out_w, taps, blocks, logit, boost):
        layers, cs, channels = conv_w.shape
        rows, ds = stream.shape
        width = blocks.shape[-1]
        bf, f32, dma = jnp.bfloat16, jnp.float32, pltpu.SemaphoreType.DMA
        vmem = pltpu.VMEM
        if folds(n_grp, n_sp, n_tp, layers, rows, ds, cs, channels):
            weights, groups = 3 * layers, channels // width
            return pl.pallas_call(
                functools.partial(folded_kernel, n_grp, n_sp, n_tp),
                out_shape=jax.ShapeDtypeStruct((rows, ds), bf),
                in_specs=[pl.BlockSpec(memory_space=pl.ANY)] * 9,
                out_specs=pl.BlockSpec(memory_space=vmem),
                scratch_shapes=[
                    vmem(gain.shape, f32),
                    vmem(conv_w.shape, bf),
                    vmem(gate_w.shape, bf),
                    vmem(taps.shape, f32),
                    vmem(blocks.shape, bf),
                    vmem(logit.shape, f32),
                    vmem(boost.shape, f32),
                    vmem(logit.shape, f32),
                    dma((8 + layers,)),
                    vmem((layers + 1, n_tp, rows, ds), bf),
                    vmem((2, n_sp, rows, cs), bf),
                    vmem((2 * layers, 3, cs, channels), bf),
                    vmem((layers, n_sp, channels, cs), bf),
                    vmem((layers + 1, rows + 2 * HALO, channels), f32),
                    vmem((groups, rows, width), bf),
                    vmem((groups, rows, width), bf),
                    vmem((2, rows, channels), f32),
                    vmem((2, 2, rows, channels), f32),
                    vmem((2, 2, rows, channels), f32),
                    vmem((layers, n_sp, 8, channels), f32),
                    vmem((rows, channels), bf),
                    vmem((layers, 2, rows, ds), bf),
                    vmem((layers, 2, rows, ds), bf),
                    vmem((2, rows, ds), f32),
                    vmem((layers, rows, ds), bf),
                    vmem((layers, rows, ds), bf),
                    dma((weights, 4)),
                    dma((weights, 2)),
                    dma((weights, 2)),
                    dma((weights, 2, 2)),
                    dma((weights, 3, 2)),
                    dma((weights, 3, 4)),
                    vmem((2, rows), f32),
                    dma((1,)),
                    dma((1,)),
                    dma((PIECES,)),
                    dma((PIECES,)),
                    dma((layers + 1, PIECES)),
                    dma((layers + 1, PIECES)),
                    dma((layers + 1, PIECES, 2)),
                    dma((layers + 1, PIECES, 2)),
                    dma((groups,)),
                    dma((groups,)),
                    dma((layers, 2)),
                    dma((layers, 2)),
                    dma((layers, n_sp)),
                    dma((layers, n_sp)),
                    dma((layers, 2)),
                    dma((layers, 2)),
                    dma((layers, PIECES)),
                    dma((layers, PIECES)),
                ],
                compiler_params=pltpu.CompilerParams(
                    collective_id=0, has_side_effects=True, vmem_limit_bytes=60 * 1024 * 1024
                ),
            )(stream, gain, conv_w, gate_w, out_w, taps, blocks, logit, boost)
        rate = (-RECURRENT_WIDTH * jax.nn.softplus(-logit)).reshape(-1, channels)
        boost = boost.reshape(-1, rows).T
        return pl.pallas_call(
            functools.partial(kernel, n_grp, n_sp, n_tp),
            out_shape=jax.ShapeDtypeStruct((rows, ds), bf),
            in_specs=[pl.BlockSpec(memory_space=vmem)] * 9,
            out_specs=pl.BlockSpec(memory_space=vmem),
            scratch_shapes=[
                vmem((layers, n_tp, rows, ds), bf),
                vmem((n_sp, rows, cs), bf),
                vmem((2 * layers, n_sp, cs, channels), bf),
                vmem((layers, n_sp, channels, cs), bf),
                vmem((layers, rows + 2 * HALO, channels), f32),
                vmem((rows, channels), f32),
                vmem((2, rows, channels), f32),
                vmem((2, rows, channels), f32),
                vmem((layers, n_sp, 8, channels), f32),
                vmem((rows, channels), bf),
                vmem((layers, n_tp, rows, ds), bf),
                vmem((layers, n_tp, rows, ds), bf),
                dma((3 * layers, n_sp + 1)),
                dma((3 * layers, n_sp)),
                dma((3 * layers, n_sp)),
                dma((3 * layers, n_sp)),
                dma((layers, n_tp)),
                dma((layers, n_tp)),
                dma((layers, n_tp)),
                dma((layers, n_tp)),
                dma((layers, 2)),
                dma((layers, 2)),
                dma((layers, n_sp)),
                dma((layers, n_sp)),
            ],
            compiler_params=pltpu.CompilerParams(
                collective_id=0, has_side_effects=True, vmem_limit_bytes=60 * 1024 * 1024
            ),
        )(stream, gain, conv_w, gate_w, out_w, taps, blocks, rate, boost)

    return jax.shard_map(
        local,
        mesh=mesh,
        in_specs=(
            P(("grp", "sp"), "tp"),
            P(),
            P(None, "sp", "tp"),
            P(None, "sp", "tp"),
            P(None, "tp", "sp"),
            P(None, None, "tp"),
            P(None, None, None, "tp", None, None),
            P(None, None, "tp"),
            P(None, None, ("grp", "sp")),
        ),
        out_specs=P(("grp", "sp"), "tp"),
        check_vma=False,
    )
```

```python
import functools

import jax
import jax.numpy as jnp
from jax import lax
from jax.experimental import pallas as pl
from jax.experimental.pallas import tpu as pltpu
from jax.sharding import PartitionSpec as P

EPS = 1e-06
RECURRENT_WIDTH = 8.0
TILE = 16
HALO = 8
LAG = 0
END_LAG = 0
PIECES = 4
MESH = pl.DeviceIdType.MESH


def own_share(rows, n_grp):
    if n_grp != 2:
        return rows
    return min(rows, -(-rows * 11 // (20 * TILE)) * TILE)


def one_minus_square(log_decay, decay):
    y = 2.0 * log_decay
    series = y * (1 / 720) + 1 / 120
    series = series * y + 1 / 24
    series = series * y + 1 / 6
    series = series * y + 0.5
    series = series * y + 1.0
    return jnp.where(y > -0.25, -y * series, 1.0 - decay * decay)


def scanned(a, b, reverse):
    count = a.shape[0]
    row = lax.broadcasted_iota(jnp.int32, a.shape, 0)
    step = 1
    while step < count:
        inside = row < count - step if reverse else row >= step
        shift = count - step if reverse else step
        a_near = jnp.where(inside, pltpu.roll(a, shift, 0), 1.0)
        b_near = jnp.where(inside, pltpu.roll(b, shift, 0), 0.0)
        b = a * b_near + b
        a = a * a_near
        step *= 2
    return a, b


def kernel(
    n_grp, n_sp, n_tp,
    stream, gain, conv_w, gate_w, out_w, taps, blocks, rate, boost,
    out,
    full, normed, g_in, g_out, xpad, y_act, cum, loc, ends, gated, parts, sums,
    z_send, z_recv, y_send, y_recv, f_send, f_recv, r_send, r_recv,
    h_send, h_recv, e_send, e_recv,
):
    g, s, t = lax.axis_index("grp"), lax.axis_index("sp"), lax.axis_index("tp")
    layers = conv_w.shape[0]
    rows, ds = stream.shape
    cs, channels = conv_w.shape[1], conv_w.shape[2]
    width = blocks.shape[-1]
    weights = 3 * layers

    def remote(src, dst, send, recv, axis, place):
        return pltpu.make_async_remote_copy(
            src_ref=src, dst_ref=dst, send_sem=send, recv_sem=recv,
            device_id={axis: place}, device_id_type=MESH,
        )

    barrier = pltpu.get_barrier_semaphore()
    total = 0
    for axis, me, count in (("sp", s, n_sp), ("tp", t, n_tp), ("grp", g, n_grp)):
        for d in range(1, count):
            pl.semaphore_signal(
                barrier, inc=1, device_id={axis: lax.rem(me + d, count)}, device_id_type=MESH
            )
            total += 1
    pl.semaphore_wait(barrier, total)

    def mine(w):
        return (conv_w, gate_w, out_w)[w % 3].at[w // 3]

    def hold(w, c):
        return g_out.at[w // 3, c] if w % 3 == 2 else g_in.at[w // 3 * 2 + w % 3, c]

    def depth(w):
        return channels if w % 3 == 2 else cs

    def z_rows(w):
        share = own_share(depth(w), n_grp)
        if share == depth(w):
            return pl.ds(0, share)
        return pl.ds(pl.multiple_of(g * (depth(w) - share), TILE), share)

    def y_rows(w, place):
        share = own_share(depth(w), n_grp)
        return pl.ds(pl.multiple_of(place * share, TILE), depth(w) - share)

    def z_copy(w, c, src, to, slot):
        return remote(
            src.at[z_rows(w)], hold(w, c).at[z_rows(w)],
            z_send.at[w, slot], z_recv.at[w, c], "sp", to,
        )

    shared = n_grp == 2

    def y_copy(w, c, place):
        return remote(
            hold(w, c).at[y_rows(w, place)], hold(w, c).at[y_rows(w, place)],
            y_send.at[w, c], y_recv.at[w, c], "grp", 1 - g,
        )

    def has_y(w):
        return shared and own_share(depth(w), n_grp) < depth(w)

    def start_own(w):
        @pl.when(s < n_sp - 1)
        def _():
            z_copy(w, s, mine(w), s + 1, s).start()

        @pl.when(s > 0)
        def _():
            z_copy(w, s, mine(w), s - 1, n_sp).start()

    def pass_on(w, c, onward, to, back):
        z_copy(w, c, hold(w, c), back, c).wait_recv()

        @pl.when(onward)
        def _():
            z_copy(w, c, hold(w, c), to, c).start()

        if has_y(w):
            y_copy(w, c, g).start()

    def event(w, k):
        @pl.when(s - 1 - k >= 0)
        def _():
            pass_on(w, s - 1 - k, s < n_sp - 1, s + 1, s - 1)

        @pl.when(s + 1 + k <= n_sp - 1)
        def _():
            pass_on(w, s + 1 + k, s > 0, s - 1, s + 1)

        if k == 0 and w + 2 < weights:
            start_own(w + 2)

    queue = [(w, k) for w in range(weights) for k in range(n_sp - 1)]

    def serve(count):
        for _ in range(min(count, len(queue))):
            event(*queue.pop(0))

    def serve_until(w):
        while queue and queue[0][0] <= w:
            event(*queue.pop(0))

    def landed(w):
        if has_y(w):
            for c in range(n_sp):
                @pl.when(c != s)
                def _():
                    y_copy(w, c, 1 - g).wait_recv()

    def f_copy(layer, src, source, d, to):
        return remote(
            src, full.at[layer, source], f_send.at[layer, d], f_recv.at[layer, source], "tp", to
        )

    tp_order = [d for d in range(1, n_tp)]

    def send_features(layer, src):
        for d in tp_order:
            f_copy(layer, src, t, d, lax.rem(t + d, n_tp)).start()

    send_features(0, stream)
    for w in range(min(2, weights)):
        start_own(w)
    full[0, t] = stream[...]
    for w in range(weights):
        if w % 3 == 2:
            g_out[w // 3, s] = out_w[w // 3]
        else:
            g_in[w // 3 * 2 + w % 3, s] = (conv_w, gate_w)[w % 3][w // 3]

    row = lax.broadcasted_iota(jnp.int32, (rows, 1), 0)

    for layer in range(layers):
        if layer == 0:
            serve(1)
        for d in tp_order:
            source = lax.rem(t + d, n_tp)
            f_copy(layer, full.at[layer, source], source, d, source).wait_recv()
        square = jnp.zeros((rows, 1), jnp.float32)
        for j in range(n_tp):
            x = full[layer, j].astype(jnp.float32)
            square += jnp.sum(x * x, axis=-1, keepdims=True)
        inverse = lax.rsqrt(square / (n_tp * ds) + EPS)
        piece = min(cs, ds)
        for p in range(n_tp * ds // piece):
            at = p * piece
            x = full[layer, at // ds, :, at % ds : at % ds + piece].astype(jnp.float32)
            x = x * inverse * gain[layer : layer + 1, at : at + piece]
            normed[at // cs, :, at % cs : at % cs + piece] = x.astype(jnp.bfloat16)

        def project(w):
            acc = None
            for c in range(n_sp):
                term = jnp.dot(
                    normed[c], g_in[w // 3 * 2 + w % 3, c], preferred_element_type=jnp.float32
                )
                acc = term if acc is None else acc + term
            return acc.astype(jnp.bfloat16).astype(jnp.float32)

        wx, wy, wo = 3 * layer, 3 * layer + 1, 3 * layer + 2
        serve_until(wx)
        if layer == 0:
            serve(1)
        landed(wx)
        xpad[layer, HALO : HALO + rows] = project(wx)

        def halo_right():
            return remote(
                xpad.at[layer, pl.ds(rows, HALO)], xpad.at[layer, pl.ds(0, HALO)],
                h_send.at[layer, 0], h_recv.at[layer, 0], "sp", lax.rem(s + 1, n_sp),
            )

        def halo_left():
            return remote(
                xpad.at[layer, pl.ds(HALO, HALO)], xpad.at[layer, pl.ds(HALO + rows, HALO)],
                h_send.at[layer, 1], h_recv.at[layer, 1], "sp", lax.rem(s + n_sp - 1, n_sp),
            )

        @pl.when(s < n_sp - 1)
        def _():
            halo_right().start()

        @pl.when(s > 0)
        def _():
            halo_left().start()

        serve_until(wy)
        landed(wy)
        y_act[...] = jax.nn.gelu(project(wy))

        @pl.when(s > 0)
        def _():
            halo_right().wait_recv()

        @pl.when(s == 0)
        def _():
            xpad[layer, 0:HALO] = jnp.zeros((HALO, channels), jnp.float32)

        @pl.when(s < n_sp - 1)
        def _():
            halo_left().wait_recv()

        @pl.when(s == n_sp - 1)
        def _():
            xpad[layer, HALO + rows : 2 * HALO + rows] = jnp.zeros((HALO, channels), jnp.float32)

        for n in range(channels // width):
            lanes = slice(n * width, (n + 1) * width)
            conv = None
            for k in range(taps.shape[1]):
                term = taps[layer, k : k + 1, lanes] * xpad[
                    layer, HALO - 1 + k : HALO - 1 + k + rows, lanes
                ]
                conv = term if conv is None else conv + term
            conv_half = conv.astype(jnp.bfloat16)
            conv = conv_half.astype(jnp.float32)
            for d in range(2):
                recur = jax.nn.sigmoid(
                    jnp.dot(conv_half, blocks[layer, d, 0, n], preferred_element_type=jnp.float32)
                )
                inject = jax.nn.sigmoid(
                    jnp.dot(conv_half, blocks[layer, d, 1, n], preferred_element_type=jnp.float32)
                )
                at = 2 * layer + d
                log_decay = rate[at : at + 1, lanes] * recur + boost[:, at : at + 1]
                decay = jnp.exp(log_decay)
                first = (row == 0) & (s == 0) if d == 0 else (row == rows - 1) & (s == n_sp - 1)
                m = jnp.where(first, 1.0, jnp.sqrt(one_minus_square(log_decay, decay)))
                a, b = scanned(decay, m * inject * conv, d == 1)
                cum[d, :, lanes] = a
                loc[d, :, lanes] = b
                edge = rows - 1 if d == 0 else 0
                ends[layer, s, 2 * d : 2 * d + 1, lanes] = a[edge : edge + 1]
                ends[layer, s, 2 * d + 1 : 2 * d + 2, lanes] = b[edge : edge + 1]
            serve(1)

        def e_copy(source, d, to):
            return remote(
                ends.at[layer, source], ends.at[layer, source],
                e_send.at[layer, d], e_recv.at[layer, source], "sp", to,
            )

        for d in range(1, n_sp):
            e_copy(s, d, lax.rem(s + d, n_sp)).start()
        serve_until(wo)
        for d in range(1, n_sp):
            source = lax.rem(s + d, n_sp)
            e_copy(source, d, source).wait_recv()
        forward = jnp.zeros((1, channels), jnp.float32)
        backward = forward
        for step in range(n_sp - 1):
            forward = jnp.where(
                step < s, ends[layer, step, 0:1] * forward + ends[layer, step, 1:2], forward
            )
            back = n_sp - 1 - step
            backward = jnp.where(
                back > s, ends[layer, back, 2:3] * backward + ends[layer, back, 3:4], backward
            )
        state = loc[0] + cum[0] * forward + loc[1] + cum[1] * backward
        gated[...] = (state * y_act[...]).astype(jnp.bfloat16)

        def r_copy(source, slot, to):
            return remote(
                parts.at[layer, to], sums.at[layer, source],
                r_send.at[layer, slot], r_recv.at[layer, source], "tp", to,
            )

        landed(wo)
        for c in range(n_sp):
            partial = jnp.dot(gated[...], g_out[layer, c], preferred_element_type=jnp.float32)
            partial = partial.astype(jnp.bfloat16)
            for q in range(cs // piece):
                at = c * cs + q * piece
                j = at // ds
                parts[layer, j, :, at % ds : at % ds + piece] = partial[
                    :, q * piece : (q + 1) * piece
                ]
                if (at + piece) % ds == 0:
                    @pl.when(j != t)
                    def _():
                        r_copy(t, j, j).start()

        if layer == 0:
            serve(n_sp - 1)
        new = full[layer, t].astype(jnp.float32) + parts[layer, t].astype(jnp.float32)
        for d in tp_order:
            source = lax.rem(t + d, n_tp)
            r_copy(source, source, source).wait_recv()
            new = new + sums[layer, source].astype(jnp.float32)
        new = new.astype(jnp.bfloat16)
        if layer + 1 < layers:
            full[layer + 1, t] = new
            send_features(layer + 1, full.at[layer + 1, t])
        else:
            out[...] = new

    for w in range(weights):
        @pl.when(s < n_sp - 1)
        def _():
            z_copy(w, s, mine(w), s + 1, s).wait_send()

        @pl.when(s > 0)
        def _():
            z_copy(w, s, mine(w), s - 1, n_sp).wait_send()

        for c in range(n_sp):
            @pl.when(((c < s) & (s < n_sp - 1)) | ((c > s) & (s > 0)))
            def _():
                z_copy(w, c, hold(w, c), lax.rem(s + 1, n_sp), c).wait_send()

            if has_y(w):
                @pl.when(c != s)
                def _():
                    y_copy(w, c, g).wait_send()

    for layer in range(layers):
        for d in tp_order:
            f_copy(layer, full.at[layer, t], t, d, lax.rem(t + d, n_tp)).wait_send()
        for j in range(n_tp):
            @pl.when(j != t)
            def _():
                remote(
                    parts.at[layer, j], sums.at[layer, t],
                    r_send.at[layer, j], r_recv.at[layer, t], "tp", j,
                ).wait_send()

        for d in range(1, n_sp):
            remote(
                ends.at[layer, s], ends.at[layer, s],
                e_send.at[layer, d], e_recv.at[layer, s], "sp", lax.rem(s + d, n_sp),
            ).wait_send()

        @pl.when(s < n_sp - 1)
        def _():
            remote(
                xpad.at[layer, pl.ds(rows, HALO)], xpad.at[layer, pl.ds(0, HALO)],
                h_send.at[layer, 0], h_recv.at[layer, 0], "sp", lax.rem(s + 1, n_sp),
            ).wait_send()

        @pl.when(s > 0)
        def _():
            remote(
                xpad.at[layer, pl.ds(HALO, HALO)], xpad.at[layer, pl.ds(HALO + rows, HALO)],
                h_send.at[layer, 1], h_recv.at[layer, 1], "sp", lax.rem(s + n_sp - 1, n_sp),
            ).wait_send()


def softplus(x):
    u = jnp.exp(-jnp.abs(x))
    w = u / (u + 2.0)
    square = w * w
    series = jnp.full_like(x, 1 / 19)
    for k in range(17, 0, -2):
        series = series * square + 1 / k
    return jnp.maximum(x, 0.0) + 2.0 * w * series


def folded_kernel(
    n_grp, n_sp, n_tp,
    stream_in, gain_in, conv_in, gate_in, out_in, taps_in, blocks_in, logit_in, boost_in,
    out,
    gain, conv_w, gate_w, taps, blocks, logit, boost, rate, load_sem,
    full, normed, g_in, g_out, xpad, p_out, p_in, y_act, cum, loc, ends, gated,
    a_out, a_in, own, b_out, b_in,
    own_send, mid_send, in_send, out_send, y_send, w_recv,
    guest_boost, g_send, g_recv, s_send, s_recv, x_send, x_recv, c_send, c_recv, p_send, p_recv,
    h_send, h_recv, e_send, e_recv, a_send, a_recv, b_send, b_recv,
):
    g, s, t = lax.axis_index("grp"), lax.axis_index("sp"), lax.axis_index("tp")
    layers = conv_w.shape[0]
    rows, ds = stream_in.shape
    cs, channels = conv_w.shape[1], conv_w.shape[2]
    width = blocks.shape[-1]
    groups = channels // width
    weights = 3 * layers
    last = n_sp - 1
    half = s // 2
    end, mid = last * half, 1 + half
    far_mid, far_end = last - mid, last - end
    is_end = s == end
    is_mid = s == mid
    near = end + mid - s
    chip, core = t // 2, t % 2
    across, partner = lax.rem(t + 2, n_tp), t + 1 - 2 * core
    guest = layers
    slots = (near, far_mid, far_end)

    def remote(src, dst, send, recv, axis, place):
        return pltpu.make_async_remote_copy(
            src_ref=src, dst_ref=dst, send_sem=send, recv_sem=recv,
            device_id={axis: place}, device_id_type=MESH,
        )

    stream = full.at[0, t]
    loads = [
        (stream_in, stream), (conv_in, conv_w), (gate_in, gate_w),
        *((out_in.at[layer], g_out.at[layer, s]) for layer in range(layers)),
        (logit_in, logit), (gain_in, gain), (taps_in, taps), (boost_in, boost),
        (blocks_in, blocks),
    ]
    loads = [
        pltpu.make_async_copy(src, dst, load_sem.at[i]) for i, (src, dst) in enumerate(loads)
    ]
    for load in loads:
        load.start()

    started = []

    def launch(copy, cond=None):
        started.append((copy, cond))
        if cond is None:
            copy.start()
        else:
            @pl.when(cond)
            def _():
                copy.start()

    barrier = pltpu.get_barrier_semaphore()
    total = 0
    for axis, me, count in (("sp", s, n_sp), ("tp", t, n_tp), ("grp", g, n_grp)):
        for d in range(1, count):
            pl.semaphore_signal(
                barrier, inc=1, device_id={axis: lax.rem(me + d, count)}, device_id_type=MESH
            )
            total += 1
    pl.semaphore_wait(barrier, total)
    for load in loads:
        load.wait()

    def mine(w):
        if w % 3 == 2:
            return g_out.at[w // 3, s]
        return (conv_w, gate_w)[w % 3].at[w // 3]

    def place(w, slot, chunk):
        return g_out.at[w // 3, chunk] if w % 3 == 2 else g_in.at[w // 3 * 2 + w % 3, slot]

    def quarter(w, i):
        size = (channels if w % 3 == 2 else cs) // 4
        index = 2 * g + i if i < 2 else 2 * (1 - g) + i - 2
        return pl.ds(pl.multiple_of(index * size, TILE), size)

    def whole(w):
        return w >= 1

    def own_to_near(w, i):
        q = quarter(w, i)
        return remote(
            mine(w).at[q], place(w, 0, s).at[q],
            own_send.at[w, i], w_recv.at[w, 0, i], "sp", near,
        )

    def own_to_mid(w, i):
        q = quarter(w, i)
        return remote(
            mine(w).at[q], place(w, 1, s).at[q],
            mid_send.at[w, i], w_recv.at[w, 1, i], "sp", far_mid,
        )

    def pass_in(w, i):
        q = quarter(w, i)
        return remote(
            place(w, 0, near).at[q], place(w, 2, near).at[q],
            in_send.at[w, i], w_recv.at[w, 2, i], "sp", far_mid,
        )

    def pass_out(w, slot, i):
        here = place(w, slot, slots[slot]).at[quarter(w, i)]
        return remote(
            here, here, out_send.at[w, slot - 1, i], w_recv.at[w, slot, i], "sp", near
        )

    def share(w, slot, i):
        here = place(w, slot, slots[slot]).at[quarter(w, i)]
        return remote(
            here, here, y_send.at[w, slot, i], w_recv.at[w, slot, 2 + i], "grp", 1 - g
        )

    def arrived(w, slot, i):
        here = place(w, slot, slots[slot]).at[quarter(w, i)]
        remote(
            here, here, y_send.at[w, slot, 0], w_recv.at[w, slot, i], "grp", 1 - g
        ).wait_recv()

    outgoing = [(w, i) for w in range(weights) for i in range(4 if whole(w) else 2)]

    def send_outgoing(count):
        for _ in range(min(count, len(outgoing))):
            launch(own_to_near(*outgoing.pop(0)), is_end)

    inward = [(w, i) for w in range(weights) for i in range(2)]

    def send_inward(count):
        for _ in range(min(count, len(inward))):
            launch(own_to_mid(*inward.pop(0)), is_mid)

    early = 2 * (weights - 2)

    def mid_tick(n):
        w, i = n // 4, n % 4
        slot, p = 1 + i // 2, i % 2

        @pl.when(is_mid)
        def _():
            arrived(w, slot, p)

        launch(share(w, slot, p), is_mid)
        if w >= 2:
            launch(pass_out(w, slot, p), is_mid)
        if i < 2:
            @pl.when(is_mid)
            def _():
                arrived(w, 0, p)

            launch(pass_in(w, p), is_mid)
            if not whole(w):
                launch(share(w, 0, p), is_mid)
            if i == 1:
                send_inward(2)

    def end_tick(n):
        w, i = n // 4, n % 4
        slot, p = 1 + i // 2, i % 2
        if n >= 2:
            send_outgoing(1)
        if n < early:
            @pl.when(is_end)
            def _():
                arrived(2 + n // 2, 0, n % 2)

            launch(share(2 + n // 2, 0, n % 2), is_end)
        if w >= 2:
            @pl.when(is_end)
            def _():
                arrived(w, slot, p)

            launch(share(w, slot, p), is_end)

    mid_ticks = list(range(4 * weights))
    end_ticks = list(range(4 * weights))

    def serve(mid=0, end=0):
        while mid_ticks and mid_ticks[0] < mid:
            mid_tick(mid_ticks.pop(0))
        while end_ticks and end_ticks[0] < end:
            end_tick(end_ticks.pop(0))

    def landed(w, chosen=range(3)):
        serve(4 * w + 4 + LAG, 4 * w + 4 + END_LAG if w >= 2 else 0)

        def wait_all():
            for slot in chosen:
                for i in (2, 3):
                    arrived(w, slot, i)

        if w < 2:
            pl.when(is_mid)(wait_all)
        else:
            wait_all()

    pieces = PIECES
    part = rows // pieces

    def strip(p):
        return pl.ds(p * part, part)

    def guest_copy(p):
        return remote(
            stream.at[strip(p)], full.at[guest, t, strip(p)],
            s_send.at[p], s_recv.at[p], "sp", mid,
        )

    def across_copy(k, p, src):
        return remote(
            src.at[strip(p)], full.at[k, t, strip(p)],
            x_send.at[k, p], x_recv.at[k, p], "tp", across,
        )

    def core_copy(k, p, src):
        return remote(
            src.at[strip(p)], full.at[k, t, strip(p)],
            c_send.at[k, p, 0], c_recv.at[k, p, 0], "tp", partner,
        )

    def hand_copy(k, p):
        here = full.at[k, across, strip(p)]
        return remote(here, here, c_send.at[k, p, 1], c_recv.at[k, p, 1], "tp", partner)

    def spread(k, p, src, cond=None):
        launch(across_copy(k, p, src), cond)
        launch(core_copy(k, p, src), cond)

    def hand_on(k, p, cond=None):
        copy = across_copy(k, p, full.at[k, t])
        if cond is None:
            copy.wait_recv()
        else:
            @pl.when(cond)
            def _():
                copy.wait_recv()

        launch(hand_copy(k, p), cond)

    def gathered(k):
        for p in range(pieces):
            core_copy(k, p, full.at[k, t]).wait_recv()
            hand_copy(k, p).wait_recv()

    def normalise(layer, k, slot):
        square = jnp.zeros((rows, 1), jnp.float32)
        for j in range(n_tp):
            x = full[k, j].astype(jnp.float32)
            square += jnp.sum(x * x, axis=-1, keepdims=True)
        inverse = lax.rsqrt(square / (n_tp * ds) + EPS)
        for j in range(n_tp):
            x = full[k, j].astype(jnp.float32)
            x = x * inverse * gain[layer : layer + 1, j * ds : (j + 1) * ds]
            normed[slot, j] = x.astype(jnp.bfloat16)

    def project(w, slot):
        acc = jnp.dot(
            normed[slot, s], mine(w)[...], preferred_element_type=jnp.float32
        )
        for k in range(3):
            acc += jnp.dot(
                normed[slot, slots[k]], g_in[w // 3 * 2 + w % 3, k],
                preferred_element_type=jnp.float32,
            )
        return acc.astype(jnp.bfloat16)

    def p_copy(n):
        return remote(p_out.at[n], p_in.at[n], p_send.at[n], p_recv.at[n], "sp", near)

    def boost_copy():
        return remote(
            boost.at[0], guest_boost, g_send.at[0], g_recv.at[0], "sp", mid
        )

    def halo_right(layer):
        return remote(
            xpad.at[layer, pl.ds(rows, HALO)], xpad.at[layer, pl.ds(0, HALO)],
            h_send.at[layer, 0], h_recv.at[layer, 0], "sp", lax.rem(s + 1, n_sp),
        )

    def halo_left(layer):
        return remote(
            xpad.at[layer, pl.ds(HALO, HALO)], xpad.at[layer, pl.ds(HALO + rows, HALO)],
            h_send.at[layer, 1], h_recv.at[layer, 1], "sp", lax.rem(s + n_sp - 1, n_sp),
        )

    row = lax.broadcasted_iota(jnp.int32, (rows, 1), 0)
    diagonal = lax.broadcasted_iota(jnp.int32, (rows, rows), 0) == lax.broadcasted_iota(
        jnp.int32, (rows, rows), 1
    )

    def recurrences(layer, n, k=0):
        pad = guest if k else layer
        block = end if k else s
        raised = guest_boost if k else boost.at[layer]
        lanes = slice(n * width, (n + 1) * width)
        conv = None
        for tap in range(taps.shape[1]):
            term = taps[layer, tap : tap + 1, lanes] * xpad[
                pad, HALO - 1 + tap : HALO - 1 + tap + rows, lanes
            ]
            conv = term if conv is None else conv + term
        conv_half = conv.astype(jnp.bfloat16)
        conv = conv_half.astype(jnp.float32)
        for d in range(2):
            recur = jax.nn.sigmoid(
                jnp.dot(conv_half, blocks[layer, d, 0, n], preferred_element_type=jnp.float32)
            )
            inject = jax.nn.sigmoid(
                jnp.dot(conv_half, blocks[layer, d, 1, n], preferred_element_type=jnp.float32)
            )
            lift = jnp.sum(
                jnp.where(diagonal, raised[d : d + 1], 0.0), axis=1, keepdims=True
            )
            log_decay = rate[layer, d : d + 1, lanes] * recur + lift
            decay = jnp.exp(log_decay)
            first = (row == 0) & (block == 0) if d == 0 else (row == rows - 1) & (block == last)
            m = jnp.where(first, 1.0, jnp.sqrt(one_minus_square(log_decay, decay)))
            a, b = scanned(decay, m * inject * conv, d == 1)
            cum[k, d, :, lanes] = a
            loc[k, d, :, lanes] = b
            edge = rows - 1 if d == 0 else 0
            ends[layer, block, 2 * d : 2 * d + 1, lanes] = a[edge : edge + 1]
            ends[layer, block, 2 * d + 1 : 2 * d + 2, lanes] = b[edge : edge + 1]

    def e_copy(layer, source, d, to):
        return remote(
            ends.at[layer, source], ends.at[layer, source],
            e_send.at[layer, d], e_recv.at[layer, source], "sp", to,
        )

    def send_ends(layer):
        for d in range(1, n_sp):
            launch(e_copy(layer, s, d, lax.rem(s + d, n_sp)))

    def ends_pair(to_half):
        here = ends.at[0, pl.ds(2 * to_half, 2)]
        return remote(here, here, e_send.at[0, 0], e_recv.at[0, 0], "sp", far_mid)

    def gather_ends(layer):
        for d in range(1, n_sp):
            source = lax.rem(s + d, n_sp)
            e_copy(layer, source, d, source).wait_recv()

    def states(layer, k=0):
        block = end if k else s
        forward = jnp.zeros((1, channels), jnp.float32)
        backward = forward
        for step in range(n_sp - 1):
            forward = jnp.where(
                step < block, ends[layer, step, 0:1] * forward + ends[layer, step, 1:2], forward
            )
            back = n_sp - 1 - step
            backward = jnp.where(
                back > block, ends[layer, back, 2:3] * backward + ends[layer, back, 3:4], backward
            )
        state = loc[k, 0] + cum[k, 0] * forward + loc[k, 1] + cum[k, 1] * backward
        return (state * y_act[k]).astype(jnp.bfloat16)

    def a_copy(layer, k):
        return remote(
            a_out.at[layer, k], a_in.at[layer, k],
            a_send.at[layer, k], a_recv.at[layer, k], "tp", partner,
        )

    def b_copy(layer, p):
        return remote(
            b_out.at[layer, strip(p)], b_in.at[layer, strip(p)],
            b_send.at[layer, p], b_recv.at[layer, p], "tp", across,
        )

    def branch(layer, j):
        return jnp.dot(gated[...], g_out[layer, j], preferred_element_type=jnp.float32)

    def project_out(layer):
        chips = (1 - chip, chip)
        for k in range(2):
            a_out[layer, k] = branch(layer, 2 * chips[k] + 1 - core).astype(jnp.bfloat16)
            launch(a_copy(layer, k))
        for k in range(2):
            own[k] = branch(layer, 2 * chips[k] + core)
        if layer == 0:
            serve(14, 13)
        a_copy(layer, 0).wait_recv()
        for p in range(pieces):
            here = slice(p * part, (p + 1) * part)
            b_out[layer, here] = (
                own[0, here] + a_in[layer, 0, here].astype(jnp.float32)
            ).astype(jnp.bfloat16)
            launch(b_copy(layer, p))
        a_copy(layer, 1).wait_recv()
        own[1] += a_in[layer, 1].astype(jnp.float32)

    def project_last(layer, w):
        chips = (1 - chip, chip)
        theirs = [2 * c + 1 - core for c in chips]
        ours = [2 * c + core for c in chips]

        def give(k):
            a_out[layer, k] = branch(layer, theirs[k]).astype(jnp.bfloat16)

        def keep(k):
            own[k] = branch(layer, ours[k])

        def add():
            a_copy(layer, 0).wait_recv()
            b_out[layer] = (own[0] + a_in[layer, 0].astype(jnp.float32)).astype(jnp.bfloat16)

        for k in range(2):
            pl.when(theirs[k] != far_end)(functools.partial(give, k))
            launch(a_copy(layer, k), theirs[k] != far_end)
        for k in range(2):
            pl.when(ours[k] != far_end)(functools.partial(keep, k))
        pl.when(ours[0] != far_end)(add)
        for p in range(pieces):
            launch(b_copy(layer, p), ours[0] != far_end)
        landed(w, (2,))
        for k in range(2):
            pl.when(theirs[k] == far_end)(functools.partial(give, k))
            launch(a_copy(layer, k), theirs[k] == far_end)
        for k in range(2):
            pl.when(ours[k] == far_end)(functools.partial(keep, k))
        pl.when(ours[0] == far_end)(add)
        for p in range(pieces):
            launch(b_copy(layer, p), ours[0] == far_end)
        a_copy(layer, 1).wait_recv()
        own[1] += a_in[layer, 1].astype(jnp.float32)

    def finish(layer, p, old):
        here = slice(p * part, (p + 1) * part)
        b_copy(layer, p).wait_recv()
        new = old[here].astype(jnp.float32) + own[1, here]
        return (new + b_in[layer, here].astype(jnp.float32)).astype(jnp.bfloat16)

    launch(boost_copy(), is_end)
    send_outgoing(2)
    for p in range(pieces):
        launch(guest_copy(p), is_end)
        spread(0, p, stream, is_mid)
    send_outgoing(0)
    send_inward(2)
    for n in range(early):
        launch(own_to_near(2 + n // 2, n % 2), is_mid)
    for layer in range(layers):
        rate[layer] = -RECURRENT_WIDTH * softplus(-logit[layer])

    serve(2, 4)
    for p in range(pieces):
        hand_on(0, p, is_mid)
    for p in range(pieces):
        serve(2 + (2 * p + 1) // pieces)

        @pl.when(is_mid)
        def _():
            guest_copy(p).wait_recv()

        spread(guest, p, full.at[guest, t], is_mid)
    serve(4)

    @pl.when(is_mid)
    def _():
        gathered(0)
        normalise(0, 0, 0)

    for p in range(pieces):
        hand_on(guest, p, is_mid)
    serve(6)

    @pl.when(is_mid)
    def _():
        gathered(guest)
        normalise(0, guest, 1)

    landed(0)

    @pl.when(is_mid)
    def _():
        x = project(0, 0).astype(jnp.float32)
        xpad[0, HALO : HALO + rows] = x
        edge = jnp.zeros((HALO, channels), jnp.float32)

        @pl.when(half == 0)
        def _():
            xpad[guest, 0:HALO] = edge
            xpad[guest, HALO + rows : 2 * HALO + rows] = x[:HALO]

        @pl.when(half == 1)
        def _():
            xpad[guest, 0:HALO] = x[rows - HALO :]
            xpad[guest, HALO + rows : 2 * HALO + rows] = edge

    launch(halo_right(0), s == 1)
    launch(halo_left(0), s == 2)

    @pl.when(is_mid)
    def _():
        x = project(0, 1).astype(jnp.float32)
        xpad[guest, HALO : HALO + rows] = x

        @pl.when(half == 0)
        def _():
            xpad[0, 0:HALO] = x[rows - HALO :]

        @pl.when(half == 1)
        def _():
            xpad[0, HALO + rows : 2 * HALO + rows] = x[:HALO]

        boost_copy().wait_recv()

    serve(8, 8)
    send_outgoing(4)
    for n in range(groups):
        pl.when(is_mid)(functools.partial(recurrences, 0, n, 1))
        serve(8 + (n + 2) // 3)

    @pl.when(s == 2)
    def _():
        halo_right(0).wait_recv()

    @pl.when(s == 1)
    def _():
        halo_left(0).wait_recv()

    for n in range(groups):
        serve((9, 10, 11)[n])
        pl.when(is_mid)(functools.partial(recurrences, 0, n))
    launch(ends_pair(half), is_mid)
    landed(1)

    @pl.when(is_mid)
    def _():
        y_act[1] = jax.nn.gelu(project(1, 1).astype(jnp.float32))

    serve(12, 8)

    @pl.when(is_mid)
    def _():
        y_act[0] = jax.nn.gelu(project(1, 0).astype(jnp.float32))
        ends_pair(1 - half).wait_recv()
        x = states(0, 1)
        for n in range(groups):
            p_out[n] = x[:, n * width : (n + 1) * width]

    for n in range(groups):
        launch(p_copy(n), is_mid)

    @pl.when(is_mid)
    def _():
        gated[...] = states(0)

    serve(12, 12)

    send_outgoing(len(outgoing))

    @pl.when(is_end)
    def _():
        for n in range(groups):
            p_copy(n).wait_recv()
            gated[:, n * width : (n + 1) * width] = p_in[n]

    for layer in range(layers):
        wx, wy, wo = 3 * layer, 3 * layer + 1, 3 * layer + 2
        final = layer + 1 == layers
        if layer > 0:
            for p in range(pieces):
                hand_on(layer, p)
                if layer == 1:
                    serve((20, 20, 21, 22)[4 * p // pieces], (17, 18, 19, 20)[4 * p // pieces])
            gathered(layer)
            normalise(layer, layer, 0)
            landed(wx)
            xpad[layer, HALO : HALO + rows] = project(wx, 0).astype(jnp.float32)
            launch(halo_right(layer), s < last)
            launch(halo_left(layer), s > 0)
            if final:
                serve((24, 22)[0], (24, 22)[1])

            @pl.when(s > 0)
            def _():
                halo_right(layer).wait_recv()

            @pl.when(s == 0)
            def _():
                xpad[layer, 0:HALO] = jnp.zeros((HALO, channels), jnp.float32)

            @pl.when(s < last)
            def _():
                halo_left(layer).wait_recv()

            @pl.when(s == last)
            def _():
                xpad[layer, HALO + rows : 2 * HALO + rows] = jnp.zeros(
                    (HALO, channels), jnp.float32
                )

            for n in range(groups):
                recurrences(layer, n)
            send_ends(layer)
            if final:
                serve(4 * weights, 24)
            landed(wy)
            y_act[0] = jax.nn.gelu(project(wy, 0).astype(jnp.float32))
            gather_ends(layer)
            gated[...] = states(layer)
        if final:
            landed(wo, (0, 1))
            project_last(layer, wo)
        else:
            landed(wo)
            project_out(layer)
        for p in range(pieces):
            if layer == 0:
                serve((16, 17, 18, 19)[4 * p // pieces], (14, 15, 16, 17)[4 * p // pieces])
            new = finish(layer, p, full.at[layer, t])
            if final:
                out[p * part : (p + 1) * part] = new
            else:
                full[layer + 1, t, p * part : (p + 1) * part] = new
                spread(layer + 1, p, full.at[layer + 1, t])

    for copy, cond in started:
        if cond is None:
            copy.wait_send()
        else:
            @pl.when(cond)
            def _():
                copy.wait_send()


def folds(n_grp, n_sp, n_tp, layers, rows, ds, cs, channels):
    return (
        n_grp == 2 and n_sp == 4 and n_tp == n_sp and cs == ds
        and rows % (PIECES * TILE) == 0 and cs % (4 * TILE) == 0 and channels % (4 * TILE) == 0
    )


def solution(mesh):
    n_grp, n_sp, n_tp = mesh.shape["grp"], mesh.shape["sp"], mesh.shape["tp"]

    def local(stream, gain, conv_w, gate_w, out_w, taps, blocks, logit, boost):
        layers, cs, channels = conv_w.shape
        rows, ds = stream.shape
        width = blocks.shape[-1]
        bf, f32, dma = jnp.bfloat16, jnp.float32, pltpu.SemaphoreType.DMA
        vmem = pltpu.VMEM
        if folds(n_grp, n_sp, n_tp, layers, rows, ds, cs, channels):
            weights, groups = 3 * layers, channels // width
            return pl.pallas_call(
                functools.partial(folded_kernel, n_grp, n_sp, n_tp),
                out_shape=jax.ShapeDtypeStruct((rows, ds), bf),
                in_specs=[pl.BlockSpec(memory_space=pl.ANY)] * 9,
                out_specs=pl.BlockSpec(memory_space=vmem),
                scratch_shapes=[
                    vmem(gain.shape, f32),
                    vmem(conv_w.shape, bf),
                    vmem(gate_w.shape, bf),
                    vmem(taps.shape, f32),
                    vmem(blocks.shape, bf),
                    vmem(logit.shape, f32),
                    vmem(boost.shape, f32),
                    vmem(logit.shape, f32),
                    dma((8 + layers,)),
                    vmem((layers + 1, n_tp, rows, ds), bf),
                    vmem((2, n_sp, rows, cs), bf),
                    vmem((2 * layers, 3, cs, channels), bf),
                    vmem((layers, n_sp, channels, cs), bf),
                    vmem((layers + 1, rows + 2 * HALO, channels), f32),
                    vmem((groups, rows, width), bf),
                    vmem((groups, rows, width), bf),
                    vmem((2, rows, channels), f32),
                    vmem((2, 2, rows, channels), f32),
                    vmem((2, 2, rows, channels), f32),
                    vmem((layers, n_sp, 8, channels), f32),
                    vmem((rows, channels), bf),
                    vmem((layers, 2, rows, ds), bf),
                    vmem((layers, 2, rows, ds), bf),
                    vmem((2, rows, ds), f32),
                    vmem((layers, rows, ds), bf),
                    vmem((layers, rows, ds), bf),
                    dma((weights, 4)),
                    dma((weights, 2)),
                    dma((weights, 2)),
                    dma((weights, 2, 2)),
                    dma((weights, 3, 2)),
                    dma((weights, 3, 4)),
                    vmem((2, rows), f32),
                    dma((1,)),
                    dma((1,)),
                    dma((PIECES,)),
                    dma((PIECES,)),
                    dma((layers + 1, PIECES)),
                    dma((layers + 1, PIECES)),
                    dma((layers + 1, PIECES, 2)),
                    dma((layers + 1, PIECES, 2)),
                    dma((groups,)),
                    dma((groups,)),
                    dma((layers, 2)),
                    dma((layers, 2)),
                    dma((layers, n_sp)),
                    dma((layers, n_sp)),
                    dma((layers, 2)),
                    dma((layers, 2)),
                    dma((layers, PIECES)),
                    dma((layers, PIECES)),
                ],
                compiler_params=pltpu.CompilerParams(
                    collective_id=0, has_side_effects=True, vmem_limit_bytes=60 * 1024 * 1024
                ),
            )(stream, gain, conv_w, gate_w, out_w, taps, blocks, logit, boost)
        rate = (-RECURRENT_WIDTH * jax.nn.softplus(-logit)).reshape(-1, channels)
        boost = boost.reshape(-1, rows).T
        return pl.pallas_call(
            functools.partial(kernel, n_grp, n_sp, n_tp),
            out_shape=jax.ShapeDtypeStruct((rows, ds), bf),
            in_specs=[pl.BlockSpec(memory_space=vmem)] * 9,
            out_specs=pl.BlockSpec(memory_space=vmem),
            scratch_shapes=[
                vmem((layers, n_tp, rows, ds), bf),
                vmem((n_sp, rows, cs), bf),
                vmem((2 * layers, n_sp, cs, channels), bf),
                vmem((layers, n_sp, channels, cs), bf),
                vmem((layers, rows + 2 * HALO, channels), f32),
                vmem((rows, channels), f32),
                vmem((2, rows, channels), f32),
                vmem((2, rows, channels), f32),
                vmem((layers, n_sp, 8, channels), f32),
                vmem((rows, channels), bf),
                vmem((layers, n_tp, rows, ds), bf),
                vmem((layers, n_tp, rows, ds), bf),
                dma((3 * layers, n_sp + 1)),
                dma((3 * layers, n_sp)),
                dma((3 * layers, n_sp)),
                dma((3 * layers, n_sp)),
                dma((layers, n_tp)),
                dma((layers, n_tp)),
                dma((layers, n_tp)),
                dma((layers, n_tp)),
                dma((layers, 2)),
                dma((layers, 2)),
                dma((layers, n_sp)),
                dma((layers, n_sp)),
            ],
            compiler_params=pltpu.CompilerParams(
                collective_id=0, has_side_effects=True, vmem_limit_bytes=60 * 1024 * 1024
            ),
        )(stream, gain, conv_w, gate_w, out_w, taps, blocks, rate, boost)

    return jax.shard_map(
        local,
        mesh=mesh,
        in_specs=(
            P(("grp", "sp"), "tp"),
            P(),
            P(None, "sp", "tp"),
            P(None, "sp", "tp"),
            P(None, "tp", "sp"),
            P(None, None, "tp"),
            P(None, None, None, "tp", None, None),
            P(None, None, "tp"),
            P(None, None, ("grp", "sp")),
        ),
        out_specs=P(("grp", "sp"), "tp"),
        check_vma=False,
    )
```

```python
import functools

import jax
import jax.numpy as jnp
from jax import lax
from jax.experimental import pallas as pl
from jax.experimental.pallas import tpu as pltpu
from jax.sharding import PartitionSpec as P

EPS = 1e-06
RECURRENT_WIDTH = 8.0
TILE = 16
HALO = 8
LAG = 0
END_LAG = 0
PIECES = 4
MESH = pl.DeviceIdType.MESH


def own_share(rows, n_grp):
    if n_grp != 2:
        return rows
    return min(rows, -(-rows * 11 // (20 * TILE)) * TILE)


def one_minus_square(log_decay, decay):
    y = 2.0 * log_decay
    series = y * (1 / 720) + 1 / 120
    series = series * y + 1 / 24
    series = series * y + 1 / 6
    series = series * y + 0.5
    series = series * y + 1.0
    return jnp.where(y > -0.25, -y * series, 1.0 - decay * decay)


def scanned(a, b, reverse):
    count = a.shape[0]
    row = lax.broadcasted_iota(jnp.int32, a.shape, 0)
    step = 1
    while step < count:
        inside = row < count - step if reverse else row >= step
        shift = count - step if reverse else step
        a_near = jnp.where(inside, pltpu.roll(a, shift, 0), 1.0)
        b_near = jnp.where(inside, pltpu.roll(b, shift, 0), 0.0)
        b = a * b_near + b
        a = a * a_near
        step *= 2
    return a, b


def kernel(
    n_grp, n_sp, n_tp,
    stream, gain, conv_w, gate_w, out_w, taps, blocks, rate, boost,
    out,
    full, normed, g_in, g_out, xpad, y_act, cum, loc, ends, gated, parts, sums,
    z_send, z_recv, y_send, y_recv, f_send, f_recv, r_send, r_recv,
    h_send, h_recv, e_send, e_recv,
):
    g, s, t = lax.axis_index("grp"), lax.axis_index("sp"), lax.axis_index("tp")
    layers = conv_w.shape[0]
    rows, ds = stream.shape
    cs, channels = conv_w.shape[1], conv_w.shape[2]
    width = blocks.shape[-1]
    weights = 3 * layers

    def remote(src, dst, send, recv, axis, place):
        return pltpu.make_async_remote_copy(
            src_ref=src, dst_ref=dst, send_sem=send, recv_sem=recv,
            device_id={axis: place}, device_id_type=MESH,
        )

    barrier = pltpu.get_barrier_semaphore()
    total = 0
    for axis, me, count in (("sp", s, n_sp), ("tp", t, n_tp), ("grp", g, n_grp)):
        for d in range(1, count):
            pl.semaphore_signal(
                barrier, inc=1, device_id={axis: lax.rem(me + d, count)}, device_id_type=MESH
            )
            total += 1
    pl.semaphore_wait(barrier, total)

    def mine(w):
        return (conv_w, gate_w, out_w)[w % 3].at[w // 3]

    def hold(w, c):
        return g_out.at[w // 3, c] if w % 3 == 2 else g_in.at[w // 3 * 2 + w % 3, c]

    def depth(w):
        return channels if w % 3 == 2 else cs

    def z_rows(w):
        share = own_share(depth(w), n_grp)
        if share == depth(w):
            return pl.ds(0, share)
        return pl.ds(pl.multiple_of(g * (depth(w) - share), TILE), share)

    def y_rows(w, place):
        share = own_share(depth(w), n_grp)
        return pl.ds(pl.multiple_of(place * share, TILE), depth(w) - share)

    def z_copy(w, c, src, to, slot):
        return remote(
            src.at[z_rows(w)], hold(w, c).at[z_rows(w)],
            z_send.at[w, slot], z_recv.at[w, c], "sp", to,
        )

    shared = n_grp == 2

    def y_copy(w, c, place):
        return remote(
            hold(w, c).at[y_rows(w, place)], hold(w, c).at[y_rows(w, place)],
            y_send.at[w, c], y_recv.at[w, c], "grp", 1 - g,
        )

    def has_y(w):
        return shared and own_share(depth(w), n_grp) < depth(w)

    def start_own(w):
        @pl.when(s < n_sp - 1)
        def _():
            z_copy(w, s, mine(w), s + 1, s).start()

        @pl.when(s > 0)
        def _():
            z_copy(w, s, mine(w), s - 1, n_sp).start()

    def pass_on(w, c, onward, to, back):
        z_copy(w, c, hold(w, c), back, c).wait_recv()

        @pl.when(onward)
        def _():
            z_copy(w, c, hold(w, c), to, c).start()

        if has_y(w):
            y_copy(w, c, g).start()

    def event(w, k):
        @pl.when(s - 1 - k >= 0)
        def _():
            pass_on(w, s - 1 - k, s < n_sp - 1, s + 1, s - 1)

        @pl.when(s + 1 + k <= n_sp - 1)
        def _():
            pass_on(w, s + 1 + k, s > 0, s - 1, s + 1)

        if k == 0 and w + 2 < weights:
            start_own(w + 2)

    queue = [(w, k) for w in range(weights) for k in range(n_sp - 1)]

    def serve(count):
        for _ in range(min(count, len(queue))):
            event(*queue.pop(0))

    def serve_until(w):
        while queue and queue[0][0] <= w:
            event(*queue.pop(0))

    def landed(w):
        if has_y(w):
            for c in range(n_sp):
                @pl.when(c != s)
                def _():
                    y_copy(w, c, 1 - g).wait_recv()

    def f_copy(layer, src, source, d, to):
        return remote(
            src, full.at[layer, source], f_send.at[layer, d], f_recv.at[layer, source], "tp", to
        )

    tp_order = [d for d in range(1, n_tp)]

    def send_features(layer, src):
        for d in tp_order:
            f_copy(layer, src, t, d, lax.rem(t + d, n_tp)).start()

    send_features(0, stream)
    for w in range(min(2, weights)):
        start_own(w)
    full[0, t] = stream[...]
    for w in range(weights):
        if w % 3 == 2:
            g_out[w // 3, s] = out_w[w // 3]
        else:
            g_in[w // 3 * 2 + w % 3, s] = (conv_w, gate_w)[w % 3][w // 3]

    row = lax.broadcasted_iota(jnp.int32, (rows, 1), 0)

    for layer in range(layers):
        if layer == 0:
            serve(1)
        for d in tp_order:
            source = lax.rem(t + d, n_tp)
            f_copy(layer, full.at[layer, source], source, d, source).wait_recv()
        square = jnp.zeros((rows, 1), jnp.float32)
        for j in range(n_tp):
            x = full[layer, j].astype(jnp.float32)
            square += jnp.sum(x * x, axis=-1, keepdims=True)
        inverse = lax.rsqrt(square / (n_tp * ds) + EPS)
        piece = min(cs, ds)
        for p in range(n_tp * ds // piece):
            at = p * piece
            x = full[layer, at // ds, :, at % ds : at % ds + piece].astype(jnp.float32)
            x = x * inverse * gain[layer : layer + 1, at : at + piece]
            normed[at // cs, :, at % cs : at % cs + piece] = x.astype(jnp.bfloat16)

        def project(w):
            acc = None
            for c in range(n_sp):
                term = jnp.dot(
                    normed[c], g_in[w // 3 * 2 + w % 3, c], preferred_element_type=jnp.float32
                )
                acc = term if acc is None else acc + term
            return acc.astype(jnp.bfloat16).astype(jnp.float32)

        wx, wy, wo = 3 * layer, 3 * layer + 1, 3 * layer + 2
        serve_until(wx)
        if layer == 0:
            serve(1)
        landed(wx)
        xpad[layer, HALO : HALO + rows] = project(wx)

        def halo_right():
            return remote(
                xpad.at[layer, pl.ds(rows, HALO)], xpad.at[layer, pl.ds(0, HALO)],
                h_send.at[layer, 0], h_recv.at[layer, 0], "sp", lax.rem(s + 1, n_sp),
            )

        def halo_left():
            return remote(
                xpad.at[layer, pl.ds(HALO, HALO)], xpad.at[layer, pl.ds(HALO + rows, HALO)],
                h_send.at[layer, 1], h_recv.at[layer, 1], "sp", lax.rem(s + n_sp - 1, n_sp),
            )

        @pl.when(s < n_sp - 1)
        def _():
            halo_right().start()

        @pl.when(s > 0)
        def _():
            halo_left().start()

        serve_until(wy)
        landed(wy)
        y_act[...] = jax.nn.gelu(project(wy))

        @pl.when(s > 0)
        def _():
            halo_right().wait_recv()

        @pl.when(s == 0)
        def _():
            xpad[layer, 0:HALO] = jnp.zeros((HALO, channels), jnp.float32)

        @pl.when(s < n_sp - 1)
        def _():
            halo_left().wait_recv()

        @pl.when(s == n_sp - 1)
        def _():
            xpad[layer, HALO + rows : 2 * HALO + rows] = jnp.zeros((HALO, channels), jnp.float32)

        for n in range(channels // width):
            lanes = slice(n * width, (n + 1) * width)
            conv = None
            for k in range(taps.shape[1]):
                term = taps[layer, k : k + 1, lanes] * xpad[
                    layer, HALO - 1 + k : HALO - 1 + k + rows, lanes
                ]
                conv = term if conv is None else conv + term
            conv_half = conv.astype(jnp.bfloat16)
            conv = conv_half.astype(jnp.float32)
            for d in range(2):
                recur = jax.nn.sigmoid(
                    jnp.dot(conv_half, blocks[layer, d, 0, n], preferred_element_type=jnp.float32)
                )
                inject = jax.nn.sigmoid(
                    jnp.dot(conv_half, blocks[layer, d, 1, n], preferred_element_type=jnp.float32)
                )
                at = 2 * layer + d
                log_decay = rate[at : at + 1, lanes] * recur + boost[:, at : at + 1]
                decay = jnp.exp(log_decay)
                first = (row == 0) & (s == 0) if d == 0 else (row == rows - 1) & (s == n_sp - 1)
                m = jnp.where(first, 1.0, jnp.sqrt(one_minus_square(log_decay, decay)))
                a, b = scanned(decay, m * inject * conv, d == 1)
                cum[d, :, lanes] = a
                loc[d, :, lanes] = b
                edge = rows - 1 if d == 0 else 0
                ends[layer, s, 2 * d : 2 * d + 1, lanes] = a[edge : edge + 1]
                ends[layer, s, 2 * d + 1 : 2 * d + 2, lanes] = b[edge : edge + 1]
            serve(1)

        def e_copy(source, d, to):
            return remote(
                ends.at[layer, source], ends.at[layer, source],
                e_send.at[layer, d], e_recv.at[layer, source], "sp", to,
            )

        for d in range(1, n_sp):
            e_copy(s, d, lax.rem(s + d, n_sp)).start()
        serve_until(wo)
        for d in range(1, n_sp):
            source = lax.rem(s + d, n_sp)
            e_copy(source, d, source).wait_recv()
        forward = jnp.zeros((1, channels), jnp.float32)
        backward = forward
        for step in range(n_sp - 1):
            forward = jnp.where(
                step < s, ends[layer, step, 0:1] * forward + ends[layer, step, 1:2], forward
            )
            back = n_sp - 1 - step
            backward = jnp.where(
                back > s, ends[layer, back, 2:3] * backward + ends[layer, back, 3:4], backward
            )
        state = loc[0] + cum[0] * forward + loc[1] + cum[1] * backward
        gated[...] = (state * y_act[...]).astype(jnp.bfloat16)

        def r_copy(source, slot, to):
            return remote(
                parts.at[layer, to], sums.at[layer, source],
                r_send.at[layer, slot], r_recv.at[layer, source], "tp", to,
            )

        landed(wo)
        for c in range(n_sp):
            partial = jnp.dot(gated[...], g_out[layer, c], preferred_element_type=jnp.float32)
            partial = partial.astype(jnp.bfloat16)
            for q in range(cs // piece):
                at = c * cs + q * piece
                j = at // ds
                parts[layer, j, :, at % ds : at % ds + piece] = partial[
                    :, q * piece : (q + 1) * piece
                ]
                if (at + piece) % ds == 0:
                    @pl.when(j != t)
                    def _():
                        r_copy(t, j, j).start()

        if layer == 0:
            serve(n_sp - 1)
        new = full[layer, t].astype(jnp.float32) + parts[layer, t].astype(jnp.float32)
        for d in tp_order:
            source = lax.rem(t + d, n_tp)
            r_copy(source, source, source).wait_recv()
            new = new + sums[layer, source].astype(jnp.float32)
        new = new.astype(jnp.bfloat16)
        if layer + 1 < layers:
            full[layer + 1, t] = new
            send_features(layer + 1, full.at[layer + 1, t])
        else:
            out[...] = new

    for w in range(weights):
        @pl.when(s < n_sp - 1)
        def _():
            z_copy(w, s, mine(w), s + 1, s).wait_send()

        @pl.when(s > 0)
        def _():
            z_copy(w, s, mine(w), s - 1, n_sp).wait_send()

        for c in range(n_sp):
            @pl.when(((c < s) & (s < n_sp - 1)) | ((c > s) & (s > 0)))
            def _():
                z_copy(w, c, hold(w, c), lax.rem(s + 1, n_sp), c).wait_send()

            if has_y(w):
                @pl.when(c != s)
                def _():
                    y_copy(w, c, g).wait_send()

    for layer in range(layers):
        for d in tp_order:
            f_copy(layer, full.at[layer, t], t, d, lax.rem(t + d, n_tp)).wait_send()
        for j in range(n_tp):
            @pl.when(j != t)
            def _():
                remote(
                    parts.at[layer, j], sums.at[layer, t],
                    r_send.at[layer, j], r_recv.at[layer, t], "tp", j,
                ).wait_send()

        for d in range(1, n_sp):
            remote(
                ends.at[layer, s], ends.at[layer, s],
                e_send.at[layer, d], e_recv.at[layer, s], "sp", lax.rem(s + d, n_sp),
            ).wait_send()

        @pl.when(s < n_sp - 1)
        def _():
            remote(
                xpad.at[layer, pl.ds(rows, HALO)], xpad.at[layer, pl.ds(0, HALO)],
                h_send.at[layer, 0], h_recv.at[layer, 0], "sp", lax.rem(s + 1, n_sp),
            ).wait_send()

        @pl.when(s > 0)
        def _():
            remote(
                xpad.at[layer, pl.ds(HALO, HALO)], xpad.at[layer, pl.ds(HALO + rows, HALO)],
                h_send.at[layer, 1], h_recv.at[layer, 1], "sp", lax.rem(s + n_sp - 1, n_sp),
            ).wait_send()


def softplus(x):
    u = jnp.exp(-jnp.abs(x))
    w = u / (u + 2.0)
    square = w * w
    series = jnp.full_like(x, 1 / 19)
    for k in range(17, 0, -2):
        series = series * square + 1 / k
    return jnp.maximum(x, 0.0) + 2.0 * w * series


def folded_kernel(
    n_grp, n_sp, n_tp,
    stream_in, gain_in, conv_in, gate_in, out_in, taps_in, blocks_in, logit_in, boost_in,
    out,
    gain, conv_w, gate_w, taps, blocks, logit, boost, rate, load_sem,
    full, normed, g_in, g_out, xpad, p_out, p_in, y_act, cum, loc, ends, gated,
    a_out, a_in, own, b_out, b_in,
    own_send, mid_send, in_send, out_send, y_send, w_recv,
    guest_boost, g_send, g_recv, s_send, s_recv, x_send, x_recv, c_send, c_recv, p_send, p_recv,
    h_send, h_recv, e_send, e_recv, a_send, a_recv, b_send, b_recv,
):
    g, s, t = lax.axis_index("grp"), lax.axis_index("sp"), lax.axis_index("tp")
    layers = conv_w.shape[0]
    rows, ds = stream_in.shape
    cs, channels = conv_w.shape[1], conv_w.shape[2]
    width = blocks.shape[-1]
    groups = channels // width
    weights = 3 * layers
    last = n_sp - 1
    half = s // 2
    end, mid = last * half, 1 + half
    far_mid, far_end = last - mid, last - end
    is_end = s == end
    is_mid = s == mid
    near = end + mid - s
    chip, core = t // 2, t % 2
    across, partner = lax.rem(t + 2, n_tp), t + 1 - 2 * core
    guest = layers
    slots = (near, far_mid, far_end)

    def remote(src, dst, send, recv, axis, place):
        return pltpu.make_async_remote_copy(
            src_ref=src, dst_ref=dst, send_sem=send, recv_sem=recv,
            device_id={axis: place}, device_id_type=MESH,
        )

    stream = full.at[0, t]
    loads = [
        (stream_in, stream), (conv_in, conv_w), (gate_in, gate_w),
        *((out_in.at[layer], g_out.at[layer, s]) for layer in range(layers)),
        (logit_in, logit), (gain_in, gain), (taps_in, taps), (boost_in, boost),
        (blocks_in, blocks),
    ]
    loads = [
        pltpu.make_async_copy(src, dst, load_sem.at[i]) for i, (src, dst) in enumerate(loads)
    ]
    for load in loads:
        load.start()

    started = []

    def launch(copy, cond=None):
        started.append((copy, cond))
        if cond is None:
            copy.start()
        else:
            @pl.when(cond)
            def _():
                copy.start()

    barrier = pltpu.get_barrier_semaphore()
    total = 0
    for axis, me, count in (("sp", s, n_sp), ("tp", t, n_tp), ("grp", g, n_grp)):
        for d in range(1, count):
            pl.semaphore_signal(
                barrier, inc=1, device_id={axis: lax.rem(me + d, count)}, device_id_type=MESH
            )
            total += 1
    pl.semaphore_wait(barrier, total)
    for load in loads:
        load.wait()

    def mine(w):
        if w % 3 == 2:
            return g_out.at[w // 3, s]
        return (conv_w, gate_w)[w % 3].at[w // 3]

    def place(w, slot, chunk):
        return g_out.at[w // 3, chunk] if w % 3 == 2 else g_in.at[w // 3 * 2 + w % 3, slot]

    def quarter(w, i):
        size = (channels if w % 3 == 2 else cs) // 4
        index = 2 * g + i if i < 2 else 2 * (1 - g) + i - 2
        return pl.ds(pl.multiple_of(index * size, TILE), size)

    def whole(w):
        return w >= 1

    def own_to_near(w, i):
        q = quarter(w, i)
        return remote(
            mine(w).at[q], place(w, 0, s).at[q],
            own_send.at[w, i], w_recv.at[w, 0, i], "sp", near,
        )

    def own_to_mid(w, i):
        q = quarter(w, i)
        return remote(
            mine(w).at[q], place(w, 1, s).at[q],
            mid_send.at[w, i], w_recv.at[w, 1, i], "sp", far_mid,
        )

    def pass_in(w, i):
        q = quarter(w, i)
        return remote(
            place(w, 0, near).at[q], place(w, 2, near).at[q],
            in_send.at[w, i], w_recv.at[w, 2, i], "sp", far_mid,
        )

    def pass_out(w, slot, i):
        here = place(w, slot, slots[slot]).at[quarter(w, i)]
        return remote(
            here, here, out_send.at[w, slot - 1, i], w_recv.at[w, slot, i], "sp", near
        )

    def share(w, slot, i):
        here = place(w, slot, slots[slot]).at[quarter(w, i)]
        return remote(
            here, here, y_send.at[w, slot, i], w_recv.at[w, slot, 2 + i], "grp", 1 - g
        )

    def arrived(w, slot, i):
        here = place(w, slot, slots[slot]).at[quarter(w, i)]
        remote(
            here, here, y_send.at[w, slot, 0], w_recv.at[w, slot, i], "grp", 1 - g
        ).wait_recv()

    outgoing = [(w, i) for w in range(weights) for i in range(4 if whole(w) else 2)]

    def send_outgoing(count):
        for _ in range(min(count, len(outgoing))):
            launch(own_to_near(*outgoing.pop(0)), is_end)

    inward = [(w, i) for w in range(weights) for i in range(2)]

    def send_inward(count):
        for _ in range(min(count, len(inward))):
            launch(own_to_mid(*inward.pop(0)), is_mid)

    early = 2 * (weights - 2)

    def mid_tick(n):
        w, i = n // 4, n % 4
        slot, p = 1 + i // 2, i % 2

        @pl.when(is_mid)
        def _():
            arrived(w, slot, p)

        launch(share(w, slot, p), is_mid)
        if w >= 2:
            launch(pass_out(w, slot, p), is_mid)
        if i < 2:
            @pl.when(is_mid)
            def _():
                arrived(w, 0, p)

            launch(pass_in(w, p), is_mid)
            if not whole(w):
                launch(share(w, 0, p), is_mid)
            if i == 1:
                send_inward(2)

    def end_tick(n):
        w, i = n // 4, n % 4
        slot, p = 1 + i // 2, i % 2
        if n >= 2:
            send_outgoing(1)
        if n < early:
            @pl.when(is_end)
            def _():
                arrived(2 + n // 2, 0, n % 2)

            launch(share(2 + n // 2, 0, n % 2), is_end)
        if w >= 2:
            @pl.when(is_end)
            def _():
                arrived(w, slot, p)

            launch(share(w, slot, p), is_end)

    mid_ticks = list(range(4 * weights))
    end_ticks = list(range(4 * weights))

    def serve(mid=0, end=0):
        while mid_ticks and mid_ticks[0] < mid:
            mid_tick(mid_ticks.pop(0))
        while end_ticks and end_ticks[0] < end:
            end_tick(end_ticks.pop(0))

    def landed(w, chosen=range(3)):
        serve(4 * w + 4 + LAG, 4 * w + 4 + END_LAG if w >= 2 else 0)

        def wait_all():
            for slot in chosen:
                for i in (2, 3):
                    arrived(w, slot, i)

        if w < 2:
            pl.when(is_mid)(wait_all)
        else:
            wait_all()

    pieces = PIECES
    part = rows // pieces

    def strip(p):
        return pl.ds(p * part, part)

    def guest_copy(p):
        return remote(
            stream.at[strip(p)], full.at[guest, t, strip(p)],
            s_send.at[p], s_recv.at[p], "sp", mid,
        )

    def across_copy(k, p, src):
        return remote(
            src.at[strip(p)], full.at[k, t, strip(p)],
            x_send.at[k, p], x_recv.at[k, p], "tp", across,
        )

    def core_copy(k, p, src):
        return remote(
            src.at[strip(p)], full.at[k, t, strip(p)],
            c_send.at[k, p, 0], c_recv.at[k, p, 0], "tp", partner,
        )

    def hand_copy(k, p):
        here = full.at[k, across, strip(p)]
        return remote(here, here, c_send.at[k, p, 1], c_recv.at[k, p, 1], "tp", partner)

    def spread(k, p, src, cond=None):
        launch(across_copy(k, p, src), cond)
        launch(core_copy(k, p, src), cond)

    def hand_on(k, p, cond=None):
        copy = across_copy(k, p, full.at[k, t])
        if cond is None:
            copy.wait_recv()
        else:
            @pl.when(cond)
            def _():
                copy.wait_recv()

        launch(hand_copy(k, p), cond)

    def gathered(k):
        for p in range(pieces):
            core_copy(k, p, full.at[k, t]).wait_recv()
            hand_copy(k, p).wait_recv()

    def normalise(layer, k, slot):
        square = jnp.zeros((rows, 1), jnp.float32)
        for j in range(n_tp):
            x = full[k, j].astype(jnp.float32)
            square += jnp.sum(x * x, axis=-1, keepdims=True)
        inverse = lax.rsqrt(square / (n_tp * ds) + EPS)
        for j in range(n_tp):
            x = full[k, j].astype(jnp.float32)
            x = x * inverse * gain[layer : layer + 1, j * ds : (j + 1) * ds]
            normed[slot, j] = x.astype(jnp.bfloat16)

    def project(w, slot):
        acc = jnp.dot(
            normed[slot, s], mine(w)[...], preferred_element_type=jnp.float32
        )
        for k in range(3):
            acc += jnp.dot(
                normed[slot, slots[k]], g_in[w // 3 * 2 + w % 3, k],
                preferred_element_type=jnp.float32,
            )
        return acc.astype(jnp.bfloat16)

    def p_copy(n):
        return remote(p_out.at[n], p_in.at[n], p_send.at[n], p_recv.at[n], "sp", near)

    def boost_copy():
        return remote(
            boost.at[0], guest_boost, g_send.at[0], g_recv.at[0], "sp", mid
        )

    def halo_right(layer):
        return remote(
            xpad.at[layer, pl.ds(rows, HALO)], xpad.at[layer, pl.ds(0, HALO)],
            h_send.at[layer, 0], h_recv.at[layer, 0], "sp", lax.rem(s + 1, n_sp),
        )

    def halo_left(layer):
        return remote(
            xpad.at[layer, pl.ds(HALO, HALO)], xpad.at[layer, pl.ds(HALO + rows, HALO)],
            h_send.at[layer, 1], h_recv.at[layer, 1], "sp", lax.rem(s + n_sp - 1, n_sp),
        )

    row = lax.broadcasted_iota(jnp.int32, (rows, 1), 0)
    diagonal = lax.broadcasted_iota(jnp.int32, (rows, rows), 0) == lax.broadcasted_iota(
        jnp.int32, (rows, rows), 1
    )

    def recurrences(layer, n, k=0):
        pad = guest if k else layer
        block = end if k else s
        raised = guest_boost if k else boost.at[layer]
        lanes = slice(n * width, (n + 1) * width)
        conv = None
        for tap in range(taps.shape[1]):
            term = taps[layer, tap : tap + 1, lanes] * xpad[
                pad, HALO - 1 + tap : HALO - 1 + tap + rows, lanes
            ]
            conv = term if conv is None else conv + term
        conv_half = conv.astype(jnp.bfloat16)
        conv = conv_half.astype(jnp.float32)
        for d in range(2):
            recur = jax.nn.sigmoid(
                jnp.dot(conv_half, blocks[layer, d, 0, n], preferred_element_type=jnp.float32)
            )
            inject = jax.nn.sigmoid(
                jnp.dot(conv_half, blocks[layer, d, 1, n], preferred_element_type=jnp.float32)
            )
            lift = jnp.sum(
                jnp.where(diagonal, raised[d : d + 1], 0.0), axis=1, keepdims=True
            )
            log_decay = rate[layer, d : d + 1, lanes] * recur + lift
            decay = jnp.exp(log_decay)
            first = (row == 0) & (block == 0) if d == 0 else (row == rows - 1) & (block == last)
            m = jnp.where(first, 1.0, jnp.sqrt(one_minus_square(log_decay, decay)))
            a, b = scanned(decay, m * inject * conv, d == 1)
            cum[k, d, :, lanes] = a
            loc[k, d, :, lanes] = b
            edge = rows - 1 if d == 0 else 0
            ends[layer, block, 2 * d : 2 * d + 1, lanes] = a[edge : edge + 1]
            ends[layer, block, 2 * d + 1 : 2 * d + 2, lanes] = b[edge : edge + 1]

    def e_copy(layer, source, d, to):
        return remote(
            ends.at[layer, source], ends.at[layer, source],
            e_send.at[layer, d], e_recv.at[layer, source], "sp", to,
        )

    def send_ends(layer):
        for d in range(1, n_sp):
            launch(e_copy(layer, s, d, lax.rem(s + d, n_sp)))

    def ends_pair(to_half):
        here = ends.at[0, pl.ds(2 * to_half, 2)]
        return remote(here, here, e_send.at[0, 0], e_recv.at[0, 0], "sp", far_mid)

    def gather_ends(layer):
        for d in range(1, n_sp):
            source = lax.rem(s + d, n_sp)
            e_copy(layer, source, d, source).wait_recv()

    def states(layer, k=0):
        block = end if k else s
        forward = jnp.zeros((1, channels), jnp.float32)
        backward = forward
        for step in range(n_sp - 1):
            forward = jnp.where(
                step < block, ends[layer, step, 0:1] * forward + ends[layer, step, 1:2], forward
            )
            back = n_sp - 1 - step
            backward = jnp.where(
                back > block, ends[layer, back, 2:3] * backward + ends[layer, back, 3:4], backward
            )
        state = loc[k, 0] + cum[k, 0] * forward + loc[k, 1] + cum[k, 1] * backward
        return (state * y_act[k]).astype(jnp.bfloat16)

    def a_copy(layer, k):
        return remote(
            a_out.at[layer, k], a_in.at[layer, k],
            a_send.at[layer, k], a_recv.at[layer, k], "tp", partner,
        )

    def b_copy(layer, p):
        return remote(
            b_out.at[layer, strip(p)], b_in.at[layer, strip(p)],
            b_send.at[layer, p], b_recv.at[layer, p], "tp", across,
        )

    def branch(layer, j):
        return jnp.dot(gated[...], g_out[layer, j], preferred_element_type=jnp.float32)

    def project_out(layer):
        chips = (1 - chip, chip)
        for k in range(2):
            a_out[layer, k] = branch(layer, 2 * chips[k] + 1 - core).astype(jnp.bfloat16)
            launch(a_copy(layer, k))
        for k in range(2):
            own[k] = branch(layer, 2 * chips[k] + core)
        if layer == 0:
            serve(14, 13)
        a_copy(layer, 0).wait_recv()
        for p in range(pieces):
            here = slice(p * part, (p + 1) * part)
            b_out[layer, here] = (
                own[0, here] + a_in[layer, 0, here].astype(jnp.float32)
            ).astype(jnp.bfloat16)
            launch(b_copy(layer, p))
        a_copy(layer, 1).wait_recv()
        own[1] += a_in[layer, 1].astype(jnp.float32)

    def project_last(layer, w):
        chips = (1 - chip, chip)
        theirs = [2 * c + 1 - core for c in chips]
        ours = [2 * c + core for c in chips]

        def give(k):
            a_out[layer, k] = branch(layer, theirs[k]).astype(jnp.bfloat16)

        def keep(k):
            own[k] = branch(layer, ours[k])

        def add():
            a_copy(layer, 0).wait_recv()
            b_out[layer] = (own[0] + a_in[layer, 0].astype(jnp.float32)).astype(jnp.bfloat16)

        for k in range(2):
            pl.when(theirs[k] != far_end)(functools.partial(give, k))
            launch(a_copy(layer, k), theirs[k] != far_end)
        for k in range(2):
            pl.when(ours[k] != far_end)(functools.partial(keep, k))
        pl.when(ours[0] != far_end)(add)
        for p in range(pieces):
            launch(b_copy(layer, p), ours[0] != far_end)
        landed(w, (2,))
        for k in range(2):
            pl.when(theirs[k] == far_end)(functools.partial(give, k))
            launch(a_copy(layer, k), theirs[k] == far_end)
        for k in range(2):
            pl.when(ours[k] == far_end)(functools.partial(keep, k))
        pl.when(ours[0] == far_end)(add)
        for p in range(pieces):
            launch(b_copy(layer, p), ours[0] == far_end)
        if layer + 1 < layers:
            serve(14, 13)
        a_copy(layer, 1).wait_recv()
        own[1] += a_in[layer, 1].astype(jnp.float32)

    def finish(layer, p, old):
        here = slice(p * part, (p + 1) * part)
        b_copy(layer, p).wait_recv()
        new = old[here].astype(jnp.float32) + own[1, here]
        return (new + b_in[layer, here].astype(jnp.float32)).astype(jnp.bfloat16)

    launch(boost_copy(), is_end)
    send_outgoing(2)
    for p in range(pieces):
        launch(guest_copy(p), is_end)
        spread(0, p, stream, is_mid)
    send_outgoing(0)
    send_inward(2)
    for n in range(early):
        launch(own_to_near(2 + n // 2, n % 2), is_mid)
    for layer in range(layers):
        rate[layer] = -RECURRENT_WIDTH * softplus(-logit[layer])

    serve(2, 4)
    for p in range(pieces):
        hand_on(0, p, is_mid)
    for p in range(pieces):
        serve(2 + (2 * p + 1) // pieces)

        @pl.when(is_mid)
        def _():
            guest_copy(p).wait_recv()

        spread(guest, p, full.at[guest, t], is_mid)
    serve(4)

    @pl.when(is_mid)
    def _():
        gathered(0)
        normalise(0, 0, 0)

    for p in range(pieces):
        hand_on(guest, p, is_mid)
    serve(6)

    @pl.when(is_mid)
    def _():
        gathered(guest)
        normalise(0, guest, 1)

    landed(0)

    @pl.when(is_mid)
    def _():
        x = project(0, 0).astype(jnp.float32)
        xpad[0, HALO : HALO + rows] = x
        edge = jnp.zeros((HALO, channels), jnp.float32)

        @pl.when(half == 0)
        def _():
            xpad[guest, 0:HALO] = edge
            xpad[guest, HALO + rows : 2 * HALO + rows] = x[:HALO]

        @pl.when(half == 1)
        def _():
            xpad[guest, 0:HALO] = x[rows - HALO :]
            xpad[guest, HALO + rows : 2 * HALO + rows] = edge

    launch(halo_right(0), s == 1)
    launch(halo_left(0), s == 2)

    @pl.when(is_mid)
    def _():
        x = project(0, 1).astype(jnp.float32)
        xpad[guest, HALO : HALO + rows] = x

        @pl.when(half == 0)
        def _():
            xpad[0, 0:HALO] = x[rows - HALO :]

        @pl.when(half == 1)
        def _():
            xpad[0, HALO + rows : 2 * HALO + rows] = x[:HALO]

        boost_copy().wait_recv()

    serve(8, 8)
    send_outgoing(4)
    for n in range(groups):
        pl.when(is_mid)(functools.partial(recurrences, 0, n, 1))
        serve(8 + (n + 2) // 3)

    @pl.when(s == 2)
    def _():
        halo_right(0).wait_recv()

    @pl.when(s == 1)
    def _():
        halo_left(0).wait_recv()

    for n in range(groups):
        serve((9, 10, 11)[n])
        pl.when(is_mid)(functools.partial(recurrences, 0, n))
    launch(ends_pair(half), is_mid)
    landed(1)

    @pl.when(is_mid)
    def _():
        y_act[1] = jax.nn.gelu(project(1, 1).astype(jnp.float32))

    serve(12, 8)

    @pl.when(is_mid)
    def _():
        y_act[0] = jax.nn.gelu(project(1, 0).astype(jnp.float32))
        ends_pair(1 - half).wait_recv()
        x = states(0, 1)
        for n in range(groups):
            p_out[n] = x[:, n * width : (n + 1) * width]

    for n in range(groups):
        launch(p_copy(n), is_mid)

    @pl.when(is_mid)
    def _():
        gated[...] = states(0)

    serve(12, 12)

    send_outgoing(len(outgoing))

    @pl.when(is_end)
    def _():
        for n in range(groups):
            p_copy(n).wait_recv()
            gated[:, n * width : (n + 1) * width] = p_in[n]

    for layer in range(layers):
        wx, wy, wo = 3 * layer, 3 * layer + 1, 3 * layer + 2
        final = layer + 1 == layers
        if layer > 0:
            for p in range(pieces):
                hand_on(layer, p)
                if layer == 1:
                    serve((20, 20, 21, 22)[4 * p // pieces], (17, 18, 19, 20)[4 * p // pieces])
            gathered(layer)
            normalise(layer, layer, 0)
            landed(wx)
            xpad[layer, HALO : HALO + rows] = project(wx, 0).astype(jnp.float32)
            launch(halo_right(layer), s < last)
            launch(halo_left(layer), s > 0)
            if final:
                serve((24, 22)[0], (24, 22)[1])

            @pl.when(s > 0)
            def _():
                halo_right(layer).wait_recv()

            @pl.when(s == 0)
            def _():
                xpad[layer, 0:HALO] = jnp.zeros((HALO, channels), jnp.float32)

            @pl.when(s < last)
            def _():
                halo_left(layer).wait_recv()

            @pl.when(s == last)
            def _():
                xpad[layer, HALO + rows : 2 * HALO + rows] = jnp.zeros(
                    (HALO, channels), jnp.float32
                )

            for n in range(groups):
                recurrences(layer, n)
            send_ends(layer)
            if final:
                serve(4 * weights, 24)
            landed(wy)
            y_act[0] = jax.nn.gelu(project(wy, 0).astype(jnp.float32))
            gather_ends(layer)
            gated[...] = states(layer)
        landed(wo, (0, 1))
        project_last(layer, wo)
        for p in range(pieces):
            if layer == 0:
                serve((16, 17, 18, 19)[4 * p // pieces], (14, 15, 16, 17)[4 * p // pieces])
            new = finish(layer, p, full.at[layer, t])
            if final:
                out[p * part : (p + 1) * part] = new
            else:
                full[layer + 1, t, p * part : (p + 1) * part] = new
                spread(layer + 1, p, full.at[layer + 1, t])

    for copy, cond in started:
        if cond is None:
            copy.wait_send()
        else:
            @pl.when(cond)
            def _():
                copy.wait_send()


def folds(n_grp, n_sp, n_tp, layers, rows, ds, cs, channels):
    return (
        n_grp == 2 and n_sp == 4 and n_tp == n_sp and cs == ds
        and rows % (PIECES * TILE) == 0 and cs % (4 * TILE) == 0 and channels % (4 * TILE) == 0
    )


def solution(mesh):
    n_grp, n_sp, n_tp = mesh.shape["grp"], mesh.shape["sp"], mesh.shape["tp"]

    def local(stream, gain, conv_w, gate_w, out_w, taps, blocks, logit, boost):
        layers, cs, channels = conv_w.shape
        rows, ds = stream.shape
        width = blocks.shape[-1]
        bf, f32, dma = jnp.bfloat16, jnp.float32, pltpu.SemaphoreType.DMA
        vmem = pltpu.VMEM
        if folds(n_grp, n_sp, n_tp, layers, rows, ds, cs, channels):
            weights, groups = 3 * layers, channels // width
            return pl.pallas_call(
                functools.partial(folded_kernel, n_grp, n_sp, n_tp),
                out_shape=jax.ShapeDtypeStruct((rows, ds), bf),
                in_specs=[pl.BlockSpec(memory_space=pl.ANY)] * 9,
                out_specs=pl.BlockSpec(memory_space=vmem),
                scratch_shapes=[
                    vmem(gain.shape, f32),
                    vmem(conv_w.shape, bf),
                    vmem(gate_w.shape, bf),
                    vmem(taps.shape, f32),
                    vmem(blocks.shape, bf),
                    vmem(logit.shape, f32),
                    vmem(boost.shape, f32),
                    vmem(logit.shape, f32),
                    dma((8 + layers,)),
                    vmem((layers + 1, n_tp, rows, ds), bf),
                    vmem((2, n_sp, rows, cs), bf),
                    vmem((2 * layers, 3, cs, channels), bf),
                    vmem((layers, n_sp, channels, cs), bf),
                    vmem((layers + 1, rows + 2 * HALO, channels), f32),
                    vmem((groups, rows, width), bf),
                    vmem((groups, rows, width), bf),
                    vmem((2, rows, channels), f32),
                    vmem((2, 2, rows, channels), f32),
                    vmem((2, 2, rows, channels), f32),
                    vmem((layers, n_sp, 8, channels), f32),
                    vmem((rows, channels), bf),
                    vmem((layers, 2, rows, ds), bf),
                    vmem((layers, 2, rows, ds), bf),
                    vmem((2, rows, ds), f32),
                    vmem((layers, rows, ds), bf),
                    vmem((layers, rows, ds), bf),
                    dma((weights, 4)),
                    dma((weights, 2)),
                    dma((weights, 2)),
                    dma((weights, 2, 2)),
                    dma((weights, 3, 2)),
                    dma((weights, 3, 4)),
                    vmem((2, rows), f32),
                    dma((1,)),
                    dma((1,)),
                    dma((PIECES,)),
                    dma((PIECES,)),
                    dma((layers + 1, PIECES)),
                    dma((layers + 1, PIECES)),
                    dma((layers + 1, PIECES, 2)),
                    dma((layers + 1, PIECES, 2)),
                    dma((groups,)),
                    dma((groups,)),
                    dma((layers, 2)),
                    dma((layers, 2)),
                    dma((layers, n_sp)),
                    dma((layers, n_sp)),
                    dma((layers, 2)),
                    dma((layers, 2)),
                    dma((layers, PIECES)),
                    dma((layers, PIECES)),
                ],
                compiler_params=pltpu.CompilerParams(
                    collective_id=0, has_side_effects=True, vmem_limit_bytes=60 * 1024 * 1024
                ),
            )(stream, gain, conv_w, gate_w, out_w, taps, blocks, logit, boost)
        rate = (-RECURRENT_WIDTH * jax.nn.softplus(-logit)).reshape(-1, channels)
        boost = boost.reshape(-1, rows).T
        return pl.pallas_call(
            functools.partial(kernel, n_grp, n_sp, n_tp),
            out_shape=jax.ShapeDtypeStruct((rows, ds), bf),
            in_specs=[pl.BlockSpec(memory_space=vmem)] * 9,
            out_specs=pl.BlockSpec(memory_space=vmem),
            scratch_shapes=[
                vmem((layers, n_tp, rows, ds), bf),
                vmem((n_sp, rows, cs), bf),
                vmem((2 * layers, n_sp, cs, channels), bf),
                vmem((layers, n_sp, channels, cs), bf),
                vmem((layers, rows + 2 * HALO, channels), f32),
                vmem((rows, channels), f32),
                vmem((2, rows, channels), f32),
                vmem((2, rows, channels), f32),
                vmem((layers, n_sp, 8, channels), f32),
                vmem((rows, channels), bf),
                vmem((layers, n_tp, rows, ds), bf),
                vmem((layers, n_tp, rows, ds), bf),
                dma((3 * layers, n_sp + 1)),
                dma((3 * layers, n_sp)),
                dma((3 * layers, n_sp)),
                dma((3 * layers, n_sp)),
                dma((layers, n_tp)),
                dma((layers, n_tp)),
                dma((layers, n_tp)),
                dma((layers, n_tp)),
                dma((layers, 2)),
                dma((layers, 2)),
                dma((layers, n_sp)),
                dma((layers, n_sp)),
            ],
            compiler_params=pltpu.CompilerParams(
                collective_id=0, has_side_effects=True, vmem_limit_bytes=60 * 1024 * 1024
            ),
        )(stream, gain, conv_w, gate_w, out_w, taps, blocks, rate, boost)

    return jax.shard_map(
        local,
        mesh=mesh,
        in_specs=(
            P(("grp", "sp"), "tp"),
            P(),
            P(None, "sp", "tp"),
            P(None, "sp", "tp"),
            P(None, "tp", "sp"),
            P(None, None, "tp"),
            P(None, None, None, "tp", None, None),
            P(None, None, "tp"),
            P(None, None, ("grp", "sp")),
        ),
        out_specs=P(("grp", "sp"), "tp"),
        check_vma=False,
    )
```
